512 devices in a mesh: sp: 64 (over z, y), tp: 8 (over x, core).
Axes of the slice: x: 4, y: 4, z: 16, core: 2. Of those that a mesh axis runs over, the one named last changes fastest.
Arguments:
- tokens: bfloat16 [6144, 4, 1024], P(('sp', 'tp')), may hold values from -6 to 6
- in_gain: float32 [1024], replicated, may hold values from 0.1 to 1.9
- w_query: bfloat16 [1024, 1024], P('sp', 'tp'), may hold values from -0.1875 to 0.1875
- w_key: bfloat16 [1024, 1024], P('sp', 'tp'), may hold values from -0.1875 to 0.1875
- w_value: bfloat16 [1024, 1024], P('sp', 'tp'), may hold values from -0.1875 to 0.1875
- w_gate: bfloat16 [1024, 1024], P('sp', 'tp'), may hold values from -0.1875 to 0.1875
- w_beta: bfloat16 [1024, 8], P('sp', 'tp'), may hold values from -0.1875 to 0.1875
- conv_query: bfloat16 [4, 1024], P(None, 'tp'), may hold values from -3 to 3
- conv_key: bfloat16 [4, 1024], P(None, 'tp'), may hold values from -3 to 3
- conv_value: bfloat16 [4, 1024], P(None, 'tp'), may hold values from -3 to 3
- decay_rate: float32 [8], P('tp'), may hold values from 0.1 to 3
- out_gain: float32 [128], replicated, may hold values from 0.1 to 1.9
- w_out: bfloat16 [1024, 1024], P('tp', 'sp'), may hold values from -0.1875 to 0.1875
Outputs:
- mixed: bfloat16 [6144, 4, 1024], P(('sp', 'tp'))
The draws below stay inside these ranges and needn't reach their ends.
All inputs are finite; a program needn't handle non-finite values.
Results may differ from the reference program's by a relative error of at most 0.02.
Values may be sent and summed in bfloat16 or wider, within the bound.
A program may use at most 64 MiB of HBM per device.

```python
import math
import jax
import jax.numpy as jnp
from jax import lax

D = 1024
HEADS = 8
DK = 128
CONV_K = 4
BLOCK = 32
SEQS = 4
TOKENS = 6144


def shard_levels(own_key, extent, shards, low, top_value):
    level, own = 1.0, jax.random.fold_in(own_key, 6)
    for dim, parts in shards:
        heights = jnp.exp(jax.random.uniform(jax.random.fold_in(own, dim), (parts,), jnp.float32, low / len(shards), top_value / len(shards)))
        level = level * jnp.repeat(heights, extent[dim] // parts).reshape([-1 if axis == dim else 1 for axis in range(len(extent))])
    return level


def normal_values(stream_key, shape, spread, limit, shards=(), held_as=jnp.bfloat16):
    values = spread * jax.random.normal(stream_key, shape, jnp.float32)
    if shards:
        values = values * shard_levels(stream_key, shape, shards, -0.22, 0.18)
    return jnp.clip(values, -limit, limit).astype(held_as)


def setup_inputs(seed: int = 0) -> dict:
    key_of = jax.random.split(jax.random.key(seed), 14)
    tokens = normal_values(key_of[0], (TOKENS, SEQS, D), 1.0, 6.0, ((0, 512),))
    in_gain = jnp.clip(1.0 + 0.18 * jax.random.normal(key_of[1], (D,), jnp.float32), 0.1, 1.9)
    w_query = normal_values(key_of[2], (D, HEADS * DK), D ** -0.5, 0.1875, ((0, 64), (1, 8)))
    w_key = normal_values(key_of[3], (D, HEADS * DK), D ** -0.5, 0.1875, ((0, 64), (1, 8)))
    w_value = normal_values(key_of[4], (D, HEADS * DK), D ** -0.5, 0.1875, ((0, 64), (1, 8)))
    w_gate = normal_values(key_of[5], (D, HEADS * DK), D ** -0.5, 0.1875, ((0, 64), (1, 8)))
    w_beta = normal_values(key_of[6], (D, HEADS), D ** -0.5, 0.1875, ((0, 64), (1, 8)))
    conv_query = normal_values(key_of[7], (CONV_K, HEADS * DK), CONV_K ** -0.5, 3.0, ((1, 8),))
    conv_key = normal_values(key_of[8], (CONV_K, HEADS * DK), CONV_K ** -0.5, 3.0, ((1, 8),))
    conv_value = normal_values(key_of[9], (CONV_K, HEADS * DK), CONV_K ** -0.5, 3.0, ((1, 8),))
    decay_rate = jnp.clip(jnp.exp(math.log(3.0) - 3.4011974 * jax.random.uniform(key_of[10], (HEADS,), jnp.float32) ** shard_levels(key_of[10], (HEADS,), ((0, 8),), -0.2, 0.2)), 0.1, 3.0)
    out_gain = jnp.clip(1.0 + 0.18 * jax.random.normal(key_of[11], (DK,), jnp.float32), 0.1, 1.9)
    w_out = normal_values(key_of[12], (HEADS * DK, D), (HEADS * DK) ** -0.5, 0.1875, ((0, 8), (1, 64)))
    return {"tokens": tokens, "in_gain": in_gain, "w_query": w_query, "w_key": w_key, "w_value": w_value, "w_gate": w_gate, "w_beta": w_beta, "conv_query": conv_query, "conv_key": conv_key, "conv_value": conv_value, "decay_rate": decay_rate, "out_gain": out_gain, "w_out": w_out}


epsilon = 1e-06
out_epsilon = 1e-10
highest = lax.Precision.HIGHEST

def unit_inverse(lower):
    size = lower.shape[-1]
    inverse = jnp.eye(size, dtype=jnp.float32) - lower
    power = jnp.matmul(lower, lower, precision=highest)
    span = 2
    while span < size:
        inverse = inverse + jnp.matmul(inverse, power, precision=highest)
        power = jnp.matmul(power, power, precision=highest)
        span = span * 2
    return inverse

def make_terms(query, keys, values, beta, rate_col):
    size = query.shape[-2]
    steps = jnp.arange(1, size + 1).astype(jnp.float32)
    cumulative = -rate_col * steps
    lower_mask = jnp.tril(jnp.ones((size, size), bool))
    strict_mask = jnp.tril(jnp.ones((size, size), bool), -1)
    decay = jnp.where(lower_mask, jnp.exp(cumulative[..., :, None] - cumulative[..., None, :]), 0.0)
    weighted = keys * beta[..., None]
    lower = jnp.where(strict_mask, jnp.einsum('...cd,...sd->...cs', weighted, keys, precision=highest) * decay, 0.0)
    inverse = unit_inverse(lower)
    update = jnp.einsum('...cs,...sv->...cv', inverse, values * beta[..., None], precision=highest)
    erase = jnp.einsum('...cs,...sd->...cd', inverse, weighted * jnp.exp(cumulative)[..., None], precision=highest)
    scores = jnp.einsum('...cd,...sd->...cs', query, keys, precision=highest) * decay
    query_decayed = query * jnp.exp(cumulative)[..., None]
    final = cumulative[..., -1:]
    keys_decayed = keys * jnp.exp(final - cumulative)[..., None]
    return (query_decayed, keys_decayed, update, erase, scores, jnp.exp(final))

def apply_block(state, terms):
    query_decayed, keys_decayed, update, erase, scores, kept = terms
    fresh = update - jnp.einsum('...cd,...dv->...cv', erase, state, precision=highest)
    output = jnp.einsum('...cd,...dv->...cv', query_decayed, state, precision=highest)
    output = output + jnp.einsum('...cs,...sv->...cv', scores, fresh, precision=highest)
    state = state * kept[..., None] + jnp.einsum('...cd,...cv->...dv', keys_decayed, fresh, precision=highest)
    return (state, output)

def causal_conv(pre, conv_taps, history):
    width = conv_taps.shape[0]
    extended = jnp.concatenate([history, pre], axis=0).astype(jnp.float32)
    length = pre.shape[0]
    total = jnp.zeros(pre.shape, jnp.float32)
    for tap in range(width):
        total = total + extended[tap:tap + length] * conv_taps[tap].astype(jnp.float32)
    return total

def rms_scale(values_in, gain):
    values = values_in.astype(jnp.float32)
    scaled = values * lax.rsqrt(lax.optimization_barrier(jnp.mean(values * values, axis=-1, keepdims=True)) + epsilon)
    return (scaled * gain).astype(jnp.bfloat16)

def l2_normalize(array):
    return array * lax.rsqrt(lax.optimization_barrier(jnp.sum(array * array, axis=-1, keepdims=True)) + epsilon)

def finish(outputs, out_gain, gate_pre):
    normed = outputs * lax.rsqrt(lax.optimization_barrier(jnp.mean(outputs * outputs, axis=-1, keepdims=True)) + out_epsilon) * out_gain
    gate = jax.nn.silu(gate_pre.astype(jnp.float32)).reshape(outputs.shape)
    return (normed * gate).astype(jnp.bfloat16).reshape(outputs.shape[0], outputs.shape[1], -1)

def reference(tokens, in_gain, w_query, w_key, w_value, w_gate, w_beta, conv_query, conv_key, conv_value, decay_rate, out_gain, w_out):
    width = tokens.shape[2]
    head_width = HEADS * DK
    normed = rms_scale(tokens, in_gain)
    flat = normed.reshape(-1, width)

    def project(weight):
        return jnp.dot(flat, weight, preferred_element_type=jnp.float32).astype(jnp.bfloat16).reshape(TOKENS, SEQS, -1)
    mixed_pre = jnp.concatenate([project(w_query), project(w_key), project(w_value)], axis=2)
    gate_pre = project(w_gate)
    beta_pre = project(w_beta)
    history = jnp.zeros((CONV_K - 1, SEQS, 3 * head_width), jnp.bfloat16)
    conv_taps = jnp.concatenate([conv_query, conv_key, conv_value], axis=1)
    convolved = jax.nn.silu(causal_conv(mixed_pre, conv_taps, history))

    def split_heads(array):
        return array.reshape(TOKENS, SEQS, HEADS, DK)
    query = l2_normalize(split_heads(convolved[:, :, :head_width])) * DK ** (-0.5)
    keys = l2_normalize(split_heads(convolved[:, :, head_width:2 * head_width]))
    values = split_heads(convolved[:, :, 2 * head_width:])
    beta = jax.nn.sigmoid(beta_pre.astype(jnp.float32) + math.log(DK / (4.0 * TOKENS)))
    rate_col = (decay_rate / TOKENS)[:, None]
    blocks = TOKENS // BLOCK

    def to_blocks(array):
        return jnp.moveaxis(array.reshape(blocks, BLOCK, SEQS, HEADS, DK), 1, 3)
    beta_blocks = jnp.moveaxis(beta.reshape(blocks, BLOCK, SEQS, HEADS), 1, 3)

    def advance(state, inputs):
        query_block, key_block, value_block, beta_block = inputs
        return apply_block(state, make_terms(query_block, key_block, value_block, beta_block, rate_col))
    initial = jnp.zeros((SEQS, HEADS, DK, DK), jnp.float32)
    _, outputs = lax.scan(advance, initial, (to_blocks(query), to_blocks(keys), to_blocks(values), beta_blocks))
    outputs = jnp.moveaxis(outputs, 3, 1).reshape(TOKENS, SEQS, HEADS, DK)
    gated = finish(outputs, out_gain, gate_pre)
    mixed = jnp.dot(gated.reshape(-1, head_width), w_out, preferred_element_type=jnp.float32).astype(jnp.bfloat16)
    return mixed.reshape(TOKENS, SEQS, width)
```

```python
import functools
import math

import jax
import jax.numpy as jnp
from jax import lax
from jax.experimental import pallas as pl
from jax.experimental.pallas import tpu as pltpu
from jax.sharding import PartitionSpec as P

MESH = pl.DeviceIdType.MESH
PAD = 16
CHUNKS = 3
epsilon = 1e-06
out_epsilon = 1e-10
f32 = jnp.float32
bf16 = jnp.bfloat16
NN, NT, TN = ((1,), (0,)), ((1,), (1,)), ((0,), (0,))


def dot(a, b, dims=NN):
    return lax.dot_general(
        a.astype(bf16), b.astype(bf16), (dims, ((), ())), preferred_element_type=f32
    )


def iota(shape, axis):
    return lax.broadcasted_iota(jnp.int32, shape, axis)


def l2_normalize(array):
    return array * lax.rsqrt(jnp.sum(array * array, axis=-1, keepdims=True) + epsilon)


def unit_inverses(lowers, row, col):
    size = row.shape[0]
    near = ((row >> 1) == (col >> 1)) & (row != col)
    eye = jnp.where(row == col, 1.0, 0.0)
    inverses = [eye - jnp.where(near, lower, 0.0) for lower in lowers]
    level = 1
    while (1 << level) < size:
        mask = ((row >> (level + 1)) == (col >> (level + 1))) & ((row >> level) != (col >> level))
        inner = [dot(jnp.where(mask, l, 0.0), v) for l, v in zip(lowers, inverses)]
        inverses = [v - dot(v, w) for v, w in zip(inverses, inner)]
        level += 1
    return inverses


def compose(first, kept_first, second, kept_second):
    depth = first[0].shape[0]
    cross = dot(second[1], jnp.concatenate(first, axis=1))
    value = kept_second * first[0] + second[0] - cross[:, :depth]
    erase = kept_second * first[1] + kept_first * second[1] - cross[:, depth:]
    return value, erase


def mixer_kernel(
    sizes,
    tokens_ref,
    in_gain_ref,
    wq_ref,
    wk_ref,
    wv_ref,
    wg_ref,
    wb_ref,
    taps_ref,
    rate_ref,
    out_gain_ref,
    wo_ref,
    out_ref,
    weights,
    spread,
    strips,
    rows_buf,
    conv_buf,
    maps,
    parts,
    landed,
    w_send_y,
    w_send_z,
    w_recv,
    a_send,
    a_recv,
    b_send,
    b_recv,
    h_send,
    h_recv,
    m_send,
    m_recv,
    o_send,
    o_recv,
):
    depth, seqs, group, hops, here_rows, width = sizes
    total_tokens = hops * seqs * group * here_rows
    strip = seqs * here_rows
    span = group * strip
    size = span // CHUNKS
    sp, tp = lax.axis_index("sp"), lax.axis_index("tp")
    z, y = sp // seqs, sp % seqs
    up, down = (z + 1) % hops, (z + hops - 1) % hops

    def at(zz, yy, tt):
        return {"sp": zz * seqs + yy, "tp": tt}

    def copy(src, dst, send, recv, device):
        return pltpu.make_async_remote_copy(
            src_ref=src,
            dst_ref=dst,
            send_sem=send,
            recv_sem=recv,
            device_id=device,
            device_id_type=MESH,
        )

    me = at(z, y, tp)
    neighbours = [at(up, y, tp), at(down, y, tp)]
    far = [hops // 2, (hops - 1) // 2]
    source = [lambda d: (z + hops - d) % hops, lambda d: (z + d) % hops]
    pending = []

    def launch(*args):
        one = copy(*args)
        one.start()
        pending.append(one)

    barrier = pltpu.get_barrier_semaphore()

    def greet(device):
        pl.semaphore_signal(barrier, inc=1, device_id=device, device_id_type=MESH)

    for side in range(2):
        greet(neighbours[side])
    for dy in range(seqs):
        for dt in range(group):
            if dy or dt:
                greet(at(z, (y + dy) % seqs, (tp + dt) % group))

    block = sp
    weights[block, :, 0 * depth : 1 * depth] = wq_ref[...]
    weights[block, :, 1 * depth : 2 * depth] = wk_ref[...]
    weights[block, :, 2 * depth : 3 * depth] = wv_ref[...]
    weights[block, :, 3 * depth : 4 * depth] = wg_ref[...]
    weights[block, :, 4 * depth : 5 * depth] = jnp.broadcast_to(
        wb_ref[...].astype(f32), (wb_ref.shape[0], depth)
    ).astype(bf16)
    small = wo_ref.shape[1]
    unit = jnp.where(iota((small, small), 0) == iota((small, small), 1), 1.0, 0.0)
    weights[block, :, 5 * depth : 6 * depth] = dot(unit, wo_ref[...], NT).astype(bf16)

    pl.semaphore_wait(barrier, 2 + seqs * group - 1)

    for dy in range(1, seqs):
        launch(
            weights.at[block],
            weights.at[block],
            w_send_y.at[dy],
            w_recv.at[0, 0, seqs - dy],
            at(z, (y + dy) % seqs, tp),
        )

    zeros = jnp.zeros((PAD - here_rows, width), f32)
    for seq in range(seqs):
        values = tokens_ref[:, seq, :].astype(f32)
        scaled = values * lax.rsqrt(jnp.mean(values * values, axis=-1, keepdims=True) + epsilon)
        spread[seq] = jnp.concatenate([scaled * in_gain_ref[...], zeros], axis=0).astype(bf16)
    for dy in range(1, seqs):
        to = (y + dy) % seqs
        launch(spread.at[to], strips.at[y], a_send.at[dy], a_recv.at[seqs - dy], at(z, to, tp))
    strips[y] = spread[y]

    def w_copy(side, hop, place, zz, yy):
        one = weights.at[zz * seqs + yy]
        return copy(one, one, w_send_z.at[side, hop, place], w_recv.at[side, hop, place], neighbours[side])

    def w_forward(side, hop, place):
        if hop <= far[side]:
            zz = z if hop == 1 else source[side](hop - 1)
            one = w_copy(side, hop, place, zz, (y + place) % seqs)
            one.start()
            pending.append(one)

    for side in range(2):
        w_forward(side, 1, 0)
    for dy in range(1, seqs):
        yy = (y + dy) % seqs
        slot = weights.at[z * seqs + yy]
        copy(slot, slot, w_send_y.at[dy], w_recv.at[0, 0, dy], me).wait_recv()
        for side in range(2):
            w_forward(side, 1, dy)

    for dy in range(1, seqs):
        slot = strips.at[(y + dy) % seqs]
        copy(slot, slot, a_send.at[dy], a_recv.at[dy], me).wait_recv()
    own_rows = pl.ds(pl.multiple_of(PAD + tp * strip, PAD), strip)
    rows_buf[own_rows, :] = jnp.concatenate(
        [strips[yy].astype(f32)[:here_rows] for yy in range(seqs)], axis=0
    ).astype(bf16)
    for dt in range(1, group):
        launch(
            rows_buf.at[own_rows],
            rows_buf.at[own_rows],
            b_send.at[dt],
            b_recv.at[group - dt],
            at(z, y, (tp + dt) % group),
        )

    def w_hop(hop):
        for place in range(seqs):
            for side in range(2):
                if hop <= far[side]:
                    w_copy(side, hop, place, source[side](hop), (y + place) % seqs).wait_recv()
                    w_forward(side, hop + 1, place)

    middle = max(far) // 2
    for hop in range(1, middle + 1):
        w_hop(hop)
    for dt in range(1, group):
        rows = pl.ds(pl.multiple_of(PAD + (tp + dt) % group * strip, PAD), strip)
        one = rows_buf.at[rows]
        copy(one, one, b_send.at[dt], b_recv.at[dt], me).wait_recv()
    history = copy(
        rows_buf.at[pl.ds(span, PAD)], rows_buf.at[pl.ds(0, PAD)], h_send, h_recv, neighbours[0]
    )
    history.start()
    pending.append(history)
    for hop in range(middle + 1, max(far) + 1):
        w_hop(hop)
    history.wait_recv()

    full = PAD + span
    pre = dot(rows_buf[...], weights[:, :, : 5 * depth].reshape(width, 5 * depth)).astype(bf16)
    row, col = iota((full, full), 0), iota((full, full), 1)
    token, place = row - PAD, col - PAD
    t_of, y_of, i_of = place // strip, place % strip // here_rows, place % here_rows
    match = (token == y_of * (group * here_rows) + t_of * here_rows + i_of) & (place >= 0) & (token >= 0)
    match = match | ((row == col) & (row < PAD) & (z > 0))
    pre = dot(jnp.where(match, 1.0, 0.0), pre)
    conv_buf[...] = pre[:, : 3 * depth]
    gate_pre = pre[PAD:, 3 * depth : 4 * depth]
    shift = math.log(depth / (4.0 * total_tokens))
    beta = jax.nn.sigmoid(pre[PAD:, 4 * depth :] + shift)

    width_taps = taps_ref.shape[0]

    def conv(part, begin):
        columns = slice(part * depth, (part + 1) * depth)
        total = jnp.zeros((size, depth), f32)
        for tap in range(width_taps):
            first = PAD + begin - (width_taps - 1) + tap
            total = total + conv_buf[first : first + size, columns] * taps_ref[tap : tap + 1, columns]
        return total * jax.nn.sigmoid(total)

    rate = rate_ref[0] / total_tokens
    row, col = iota((size, size), 0), iota((size, size), 1)
    decay = jnp.exp(-rate * jnp.maximum(row - col, 0).astype(f32))
    step = iota((size, depth), 0).astype(f32)
    kept = jnp.exp(-rate * (step + 1.0))
    rest = jnp.exp(-rate * (size - 1.0 - step))
    queries, keys, values, betas = [], [], [], []
    for chunk in range(CHUNKS):
        begin = chunk * size
        queries.append(l2_normalize(conv(0, begin)) * depth ** (-0.5))
        keys.append(l2_normalize(conv(1, begin)))
        values.append(conv(2, begin))
        betas.append(beta[begin : begin + size])
    weighted = [k * b for k, b in zip(keys, betas)]
    products = [
        dot(jnp.concatenate([w, q], axis=0), k, NT) for w, q, k in zip(weighted, queries, keys)
    ]
    lowers = [jnp.where(row > col, p[:size] * decay, 0.0) for p in products]
    scores = [jnp.where(row >= col, p[size:] * decay, 0.0) for p in products]
    inverses = unit_inverses(lowers, row, col)
    both = [
        dot(inv, jnp.concatenate([v * b, w * kept], axis=1))
        for inv, v, b, w in zip(inverses, values, betas, weighted)
    ]
    moved = [dot(k * rest, b, TN) for k, b in zip(keys, both)]
    chunk_maps = [(m[:, :depth], m[:, depth:]) for m in moved]
    chunk_kept = jnp.exp(-rate * jnp.full((1, depth), float(size), f32))
    before, before_kept = [], []
    running, running_kept = chunk_maps[0], chunk_kept
    for chunk in range(1, CHUNKS):
        before.append(running)
        before_kept.append(running_kept)
        running = compose(running, running_kept, chunk_maps[chunk], chunk_kept)
        running_kept = running_kept * chunk_kept
    for part in range(2):
        maps[z, part] = running[part].astype(bf16)

    def m_copy(side, hop, part, zz):
        one = maps.at[zz, part]
        return copy(one, one, m_send.at[side, hop, part], m_recv.at[side, hop, part], neighbours[side])

    def m_forward(side, hop, part):
        if hop <= far[side]:
            one = m_copy(side, hop, part, z if hop == 1 else source[side](hop - 1))
            one.start()
            pending.append(one)

    for part in range(2):
        for side in range(2):
            m_forward(side, 1, part)

    reads, locals_ = [], []
    for chunk in range(CHUNKS):
        seen = dot(scores[chunk], both[chunk])
        read = queries[chunk] * kept - seen[:, depth:]
        local = seen[:, :depth]
        if chunk:
            value, erase = before[chunk - 1]
            shifted = dot(read, jnp.concatenate([value, erase], axis=1))
            local = local + shifted[:, :depth]
            read = before_kept[chunk - 1] * read - shifted[:, depth:]
        reads.append(read.astype(bf16))
        locals_.append(local)

    stretch = running_kept
    late, late_kept, early = None, None, jnp.zeros((depth, depth), f32)
    for hop in range(1, max(far) + 1):
        for part in range(2):
            for side in range(2):
                if hop <= far[side]:
                    m_copy(side, hop, part, source[side](hop)).wait_recv()
                    m_forward(side, hop + 1, part)
        zz = source[0](hop)
        value = jnp.where(z >= hop, maps[zz, 0].astype(f32), 0.0)
        erase = maps[zz, 1].astype(f32)
        if late is None:
            late, late_kept = (value, erase), stretch
        else:
            late = compose((value, erase), stretch, late, late_kept)
            late_kept = late_kept * stretch
        if hop <= far[1]:
            zz = source[1](hop)
            new = stretch * early + maps[zz, 0].astype(f32) - dot(maps[zz, 1], early)
            early = jnp.where(z + hop >= hops, new, 0.0)
    state = late[0] + late_kept * early - dot(late[1], early)

    out = jnp.concatenate(locals_, axis=0) + dot(jnp.concatenate(reads, axis=0), state)
    out = out * lax.rsqrt(jnp.mean(out * out, axis=-1, keepdims=True) + out_epsilon)
    gated = (out * out_gain_ref[...] * (gate_pre * jax.nn.sigmoid(gate_pre))).astype(bf16)

    owners = seqs * group
    row, col = iota((owners * PAD, span), 0), iota((owners * PAD, span), 1)
    match = (col == row // PAD * here_rows + row % PAD) & (row % PAD < here_rows)
    gated = dot(jnp.where(match, 1.0, 0.0), gated)
    full_out = weights[:, :, 5 * depth :].reshape(width, depth)
    partial = dot(gated, full_out, NT).astype(bf16)
    parts[...] = partial.reshape(owners, PAD, width)
    mine = y * group + tp
    for dy in range(seqs):
        for dt in range(group):
            if dy or dt:
                yy, tt = (y + dy) % seqs, (tp + dt) % group
                back = (seqs - dy) % seqs * group + (group - dt) % group
                launch(
                    parts.at[yy * group + tt],
                    landed.at[mine],
                    o_send.at[dy * group + dt],
                    o_recv.at[back],
                    at(z, yy, tt),
                )
    landed[mine] = parts[mine]
    for dy in range(seqs):
        for dt in range(group):
            if dy or dt:
                slot = landed.at[(y + dy) % seqs * group + (tp + dt) % group]
                index = dy * group + dt
                copy(slot, slot, o_send.at[index], o_recv.at[index], me).wait_recv()
    for seq in range(seqs):
        total = landed[seq * group].astype(f32)
        for head in range(1, group):
            total = total + landed[seq * group + head].astype(f32)
        out_ref[:, seq, :] = total[:here_rows].astype(bf16)
    for one in pending:
        one.wait_send()


def body(
    tokens,
    in_gain,
    w_query,
    w_key,
    w_value,
    w_gate,
    w_beta,
    conv_query,
    conv_key,
    conv_value,
    decay_rate,
    out_gain,
    w_out,
):
    here_rows, seqs, width = tokens.shape
    depth = w_query.shape[1]
    group, length = lax.axis_size("tp"), lax.axis_size("sp")
    hops = length // seqs
    owners = seqs * group
    span = owners * here_rows
    block = w_query.shape[0]
    taps = jnp.concatenate([conv_query, conv_key, conv_value], axis=1).astype(f32)
    sizes = (depth, seqs, group, hops, here_rows, width)
    vmem = pl.BlockSpec(memory_space=pltpu.VMEM)
    dma = pltpu.SemaphoreType.DMA
    far = hops // 2 + 1
    return pl.pallas_call(
        functools.partial(mixer_kernel, sizes),
        out_shape=jax.ShapeDtypeStruct(tokens.shape, bf16),
        in_specs=[vmem] * 8 + [pl.BlockSpec(memory_space=pltpu.SMEM)] + [vmem] * 2,
        out_specs=vmem,
        scratch_shapes=[
            pltpu.VMEM((length, block, 6 * depth), bf16),
            pltpu.VMEM((seqs, PAD, width), bf16),
            pltpu.VMEM((seqs, PAD, width), bf16),
            pltpu.VMEM((PAD + span, width), bf16),
            pltpu.VMEM((PAD + span, 3 * depth), f32),
            pltpu.VMEM((hops, 2, depth, depth), bf16),
            pltpu.VMEM((owners, PAD, width), bf16),
            pltpu.VMEM((owners, PAD, width), bf16),
            dma((seqs,)),
            dma((2, far, seqs)),
            dma((2, far, seqs)),
            dma((seqs,)),
            dma((seqs,)),
            dma((group,)),
            dma((group,)),
            dma,
            dma,
            dma((2, far, 2)),
            dma((2, far, 2)),
            dma((owners,)),
            dma((owners,)),
        ],
        compiler_params=pltpu.CompilerParams(
            collective_id=0, has_side_effects=True, vmem_limit_bytes=48 * 1024 * 1024
        ),
    )(
        tokens,
        in_gain[None],
        w_query,
        w_key,
        w_value,
        w_gate,
        w_beta,
        taps,
        decay_rate,
        out_gain[None],
        w_out,
    )


def solution(mesh):
    placed = (
        P(("sp", "tp"), None, None),
        P(),
        P("sp", "tp"),
        P("sp", "tp"),
        P("sp", "tp"),
        P("sp", "tp"),
        P("sp", "tp"),
        P(None, "tp"),
        P(None, "tp"),
        P(None, "tp"),
        P("tp"),
        P(),
        P("tp", "sp"),
    )
    return jax.shard_map(
        body, mesh=mesh, in_specs=placed, out_specs=P(("sp", "tp"), None, None), check_vma=False
    )
```

```python
import functools
import math

import jax
import jax.numpy as jnp
from jax import lax
from jax.experimental import pallas as pl
from jax.experimental.pallas import tpu as pltpu
from jax.sharding import PartitionSpec as P

MESH = pl.DeviceIdType.MESH
PAD = 16
CHUNKS = 3
CORES = 2
REACH = 4
epsilon = 1e-06
out_epsilon = 1e-10
f32 = jnp.float32
bf16 = jnp.bfloat16
NN, NT, TN = ((1,), (0,)), ((1,), (1,)), ((0,), (0,))


def dot(a, b, dims=NN):
    return lax.dot_general(
        a.astype(bf16), b.astype(bf16), (dims, ((), ())), preferred_element_type=f32
    )


def iota(shape, axis):
    return lax.broadcasted_iota(jnp.int32, shape, axis)


def l2_normalize(array):
    return array * lax.rsqrt(jnp.sum(array * array, axis=-1, keepdims=True) + epsilon)


def unit_inverses(lowers, row, col):
    size = row.shape[0]
    near = ((row >> 1) == (col >> 1)) & (row != col)
    eye = jnp.where(row == col, 1.0, 0.0)
    inverses = [eye - jnp.where(near, lower, 0.0) for lower in lowers]
    level = 1
    while (1 << level) < size:
        mask = ((row >> (level + 1)) == (col >> (level + 1))) & ((row >> level) != (col >> level))
        inner = [dot(jnp.where(mask, l, 0.0), v) for l, v in zip(lowers, inverses)]
        inverses = [v - dot(v, w) for v, w in zip(inverses, inner)]
        level += 1
    return inverses


def compose(first, kept_first, second, kept_second):
    depth = first[0].shape[0]
    cross = dot(second[1], jnp.concatenate(first, axis=1))
    value = kept_second * first[0] + second[0] - cross[:, :depth]
    erase = kept_second * first[1] + kept_first * second[1] - cross[:, depth:]
    return value, erase


def mixer_kernel(
    sizes,
    tokens_hbm,
    in_gain_hbm,
    wq_hbm,
    wk_hbm,
    wv_hbm,
    wg_hbm,
    wb_hbm,
    cq_hbm,
    ck_hbm,
    cv_hbm,
    rate_ref,
    out_gain_hbm,
    wo_hbm,
    out_ref,
    tokens_ref,
    in_gain_ref,
    beta_ref,
    cq_ref,
    ck_ref,
    cv_ref,
    out_gain_ref,
    first_half,
    second_half,
    spread,
    rows_buf,
    conv_buf,
    maps,
    swap_out,
    swap_in,
    parts,
    landed,
    load,
    z_send,
    z_recv,
    y_send,
    y_recv,
    q_send,
    q_recv,
    t_send,
    t_recv,
    c_send,
    c_recv,
    h_send,
    h_recv,
    m_send,
    m_recv,
    s_send,
    s_recv,
    o_send,
    o_recv,
):
    depth, seqs, group, hops, here_rows, width = sizes
    chips = group // CORES
    total_tokens = hops * seqs * group * here_rows
    span = seqs * group * here_rows
    size = span // CHUNKS
    sp, tp = lax.axis_index("sp"), lax.axis_index("tp")
    z, y = sp // seqs, sp % seqs
    x, core = tp // CORES, tp % CORES
    far = [hops // 2, (hops - 1) // 2]
    halves = [first_half, second_half]
    pending = []

    def at(dz, dy, dx, dc=0):
        return {
            "sp": (z + dz) % hops * seqs + (y + dy) % seqs,
            "tp": (x + dx) % chips * CORES + (core + dc) % CORES,
        }

    def copy(src, dst, send, recv, device):
        return pltpu.make_async_remote_copy(
            src_ref=src,
            dst_ref=dst,
            send_sem=send,
            recv_sem=recv,
            device_id=device,
            device_id_type=MESH,
        )

    me = {"sp": sp, "tp": tp}
    partner = at(0, 0, 0, 1)

    def launch(*args):
        one = copy(*args)
        one.start()
        pending.append(one)

    barrier = pltpu.get_barrier_semaphore()
    plane = [(dy, dx) for dy in range(seqs) for dx in range(chips) if dy or dx]
    reach = [d for d in range(1, REACH + 1) if d <= far[0]]
    reach_back = [d for d in range(1, REACH + 1) if d <= far[1]]
    friends = [partner] + [at(0, dy, dx) for dy, dx in plane]
    friends += [at(d, 0, 0) for d in reach] + [at(hops - d, 0, 0) for d in reach]
    for device in friends:
        pl.semaphore_signal(barrier, inc=1, device_id=device, device_id_type=MESH)

    def own(half, part):
        return halves[half].at[z, y, :, pl.ds(part * depth, depth)]

    loads = [
        (tokens_hbm, tokens_ref),
        (in_gain_hbm, in_gain_ref),
        (wk_hbm, own(0, 0)),
        (wv_hbm, own(0, 1)),
        (wb_hbm, beta_ref),
        (wq_hbm, own(1, 0)),
        (wg_hbm, own(1, 1)),
        (wo_hbm, own(1, 2)),
        (cq_hbm, cq_ref),
        (ck_hbm, ck_ref),
        (cv_hbm, cv_ref),
        (out_gain_hbm, out_gain_ref),
    ]
    loads = [pltpu.make_async_copy(a, b, load.at[i]) for i, (a, b) in enumerate(loads)]
    for one in loads:
        one.start()
    for one in loads:
        one.wait()

    block = wk_hbm.shape[0]
    unit = jnp.where(iota((block, block), 0) == iota((block, block), 1), 1.0, 0.0)
    column = jnp.broadcast_to(beta_ref[...].astype(f32), (depth, block))
    first_half[z, y, :, 2 * depth :] = dot(unit, column, NT).astype(bf16)

    pad_rows = jnp.zeros((PAD - here_rows, width), f32)
    for seq in range(seqs):
        values = tokens_ref[:, seq, :].astype(f32)
        scaled = values * lax.rsqrt(jnp.mean(values * values, axis=-1, keepdims=True) + epsilon)
        spread[seq] = jnp.concatenate([scaled * in_gain_ref[...], pad_rows], axis=0).astype(bf16)

    pl.semaphore_wait(barrier, len(friends))

    def z_copy(half, index, offset, device):
        one = halves[half].at[(z + offset) % hops, y]
        return copy(one, one, z_send.at[half, index], z_recv.at[half, index], device)

    def z_launch(half, index, offset, device):
        one = z_copy(half, index, offset, device)
        one.start()
        pending.append(one)

    def offset_of(index):
        return hops - index if index <= far[0] else index - far[0]

    def z_first(half):
        for d in reversed(reach):
            z_launch(half, d, 0, at(d, 0, 0))
            if d in reach_back:
                z_launch(half, far[0] + d, 0, at(hops - d, 0, 0))

    def z_arrived(half, index):
        z_copy(half, index, offset_of(index), me).wait_recv()

    def z_relay(half):
        for further in range(far[0] - REACH):
            if further == 0:
                z_arrived(half, REACH)
            index = far[0] - further
            z_launch(half, index, hops - REACH, at(index - REACH, 0, 0))
        for further in range(far[1] - REACH):
            if further == 0:
                z_arrived(half, far[0] + REACH)
            d = far[1] - further
            z_launch(half, far[0] + d, REACH, at(hops - (d - REACH), 0, 0))

    def y_copy(index, dy, offset, yy, device, back=None):
        one = first_half.at[(z + offset) % hops, yy]
        back = dy if back is None else back
        return copy(one, one, y_send.at[index, dy], y_recv.at[index, back], device)

    def y_fan(index):
        offset = offset_of(index) if index else 0
        for dy in (2, 1, 3):
            one = y_copy(index, dy, offset, y, at(0, dy, 0), seqs - dy)
            one.start()
            pending.append(one)

    def t_slot(yy, xx, cc):
        return rows_buf.at[1 + (yy * chips + xx) * CORES + cc]

    relayed = far[0] > REACH
    z_first(0)
    for index, (dy, dx) in enumerate(plane):
        launch(
            spread.at[(y + dy) % seqs],
            t_slot(y, x, core),
            t_send.at[index],
            t_recv.at[(seqs - dy) % seqs * chips + (chips - dx) % chips],
            at(0, dy, dx),
        )
    y_fan(0)
    launch(spread.at[y], t_slot(y, x, core), c_send.at[0], c_recv.at[0], partner)
    rows_buf[1 + (y * chips + x) * CORES + core] = spread[y]
    z_first(1)

    if relayed:
        z_relay(0)
        y_fan(REACH)
        y_fan(far[0] + REACH)
    for d in range(1, REACH if relayed else REACH + 1):
        for index in [d, far[0] + d]:
            if d <= far[index > far[0]]:
                z_arrived(0, index)
                y_fan(index)
    for dy, dx in plane:
        index = dy * chips + dx
        slot = t_slot((y + dy) % seqs, (x + dx) % chips, core)
        copy(slot, slot, t_send.at[0], t_recv.at[index], me).wait_recv()
        launch(slot, slot, c_send.at[index], c_recv.at[index], partner)
    if relayed:
        for d in range(REACH + 1, far[0] + 1):
            for index in [d, far[0] + d]:
                if d <= far[index > far[0]]:
                    z_arrived(0, index)
                    y_fan(index)
        z_relay(1)
    for dy, dx in [(0, 0)] + plane:
        index = dy * chips + dx
        slot = t_slot((y + dy) % seqs, (x + dx) % chips, (core + 1) % CORES)
        copy(slot, slot, c_send.at[0], c_recv.at[index], me).wait_recv()
    history = copy(rows_buf.at[seqs * group], rows_buf.at[0], h_send, h_recv, at(1, 0, 0))
    history.start()
    pending.append(history)
    for d in range(1, far[0] + 1):
        for index in [d, far[0] + d]:
            if d <= far[index > far[0]] and not (relayed and d == REACH):
                z_arrived(1, index)
    for dy in (2, 1, 3):
        one = second_half.at[:, y]
        launch(one, one, q_send.at[dy], q_recv.at[seqs - dy], at(0, dy, 0))
    for index in range(far[0] + far[1] + 1):
        offset = offset_of(index) if index else 0
        for dy in (1, 3, 2):
            y_copy(index, dy, offset, (y + dy) % seqs, me).wait_recv()
    history.wait_recv()

    full = PAD + span
    padded = (1 + seqs * group) * PAD
    row, col = iota((full, padded), 0), iota((full, padded), 1)
    place, inside = col // PAD, col % PAD
    select = (row == PAD + (place - 1) * here_rows + inside) & (inside < here_rows)
    select = jnp.where(select & ((place > 0) | (z > 0)), 1.0, 0.0).astype(bf16)

    def project(half, columns):
        weights = half[:, :, :, :columns].reshape(width, columns)
        pre = dot(rows_buf[...].reshape(padded, width), weights).astype(bf16)
        return dot(select, pre)

    pre = project(first_half, 3 * depth)
    conv_buf[:, : 2 * depth] = pre[:, : 2 * depth]
    shift = math.log(depth / (4.0 * total_tokens))
    beta = jax.nn.sigmoid(pre[PAD:, 2 * depth :] + shift)
    width_taps = cq_ref.shape[0]

    def conv(part, taps_ref, begin):
        columns = slice(part * depth, (part + 1) * depth)
        total = jnp.zeros((size, depth), f32)
        for tap in range(width_taps):
            first = PAD + begin - (width_taps - 1) + tap
            taps = taps_ref[tap : tap + 1, :].astype(f32)
            total = total + conv_buf[first : first + size, columns] * taps
        return total * jax.nn.sigmoid(total)

    rate = rate_ref[0] / total_tokens
    row, col = iota((size, size), 0), iota((size, size), 1)
    decay = jnp.exp(-rate * jnp.maximum(row - col, 0).astype(f32))
    step = iota((size, depth), 0).astype(f32)
    kept = jnp.exp(-rate * (step + 1.0))
    rest = jnp.exp(-rate * (size - 1.0 - step))
    keys, values, betas = [], [], []
    for chunk in range(CHUNKS):
        begin = chunk * size
        keys.append(l2_normalize(conv(0, ck_ref, begin)))
        values.append(conv(1, cv_ref, begin))
        betas.append(beta[begin : begin + size])
    weighted = [k * b for k, b in zip(keys, betas)]
    lowers = [
        jnp.where(row > col, dot(w, k, NT) * decay, 0.0) for w, k in zip(weighted, keys)
    ]
    inverses = unit_inverses(lowers, row, col)
    both = [
        dot(inv, jnp.concatenate([v * b, w * kept], axis=1))
        for inv, v, b, w in zip(inverses, values, betas, weighted)
    ]
    moved = [dot(k * rest, b, TN) for k, b in zip(keys, both)]
    chunk_maps = [(m[:, :depth], m[:, depth:]) for m in moved]
    chunk_kept = jnp.exp(-rate * jnp.full((1, depth), float(size), f32))
    before, before_kept = [], []
    running, running_kept = chunk_maps[0], chunk_kept
    for chunk in range(1, CHUNKS):
        before.append(running)
        before_kept.append(running_kept)
        running = compose(running, running_kept, chunk_maps[chunk], chunk_kept)
        running_kept = running_kept * chunk_kept
    for part in range(2):
        maps[z, part] = running[part].astype(bf16)

    source = [lambda d: (z + hops - d) % hops, lambda d: (z + d) % hops]
    neighbours = [at(1, 0, 0), at(hops - 1, 0, 0)]

    def m_copy(side, hop, part, zz):
        one = maps.at[zz, part]
        return copy(one, one, m_send.at[side, hop, part], m_recv.at[side, hop, part], neighbours[side])

    def m_forward(side, hop, part):
        if hop <= far[side]:
            one = m_copy(side, hop, part, z if hop == 1 else source[side](hop - 1))
            one.start()
            pending.append(one)

    for part in range(2):
        for side in range(2):
            m_forward(side, 1, part)

    late_work = {}

    def project_second():
        for dy in (1, 3, 2):
            one = second_half.at[:, (y + dy) % seqs]
            copy(one, one, q_send.at[dy], q_recv.at[dy], me).wait_recv()
        pre = project(second_half, 2 * depth)
        conv_buf[:, : depth] = pre[:, :depth]
        gate_pre = pre[PAD:, depth:]
        late_work["gate"] = gate_pre * jax.nn.sigmoid(gate_pre)

    def queries_and_scores():
        queries = [
            l2_normalize(conv(0, cq_ref, chunk * size)) * depth ** (-0.5) for chunk in range(CHUNKS)
        ]
        late_work["queries"] = queries
        late_work["scores"] = [
            jnp.where(row >= col, dot(q, k, NT) * decay, 0.0) for q, k in zip(queries, keys)
        ]

    def reads_and_locals():
        reads, locals_ = [], []
        for chunk in range(CHUNKS):
            seen = dot(late_work["scores"][chunk], both[chunk])
            read = late_work["queries"][chunk] * kept - seen[:, depth:]
            local = seen[:, :depth]
            if chunk:
                value, erase = before[chunk - 1]
                shifted = dot(read, jnp.concatenate([value, erase], axis=1))
                local = local + shifted[:, :depth]
                read = before_kept[chunk - 1] * read - shifted[:, depth:]
            reads.append(read.astype(bf16))
            locals_.append(local)
        late_work["reads"], late_work["locals"] = reads, locals_

    beside = [project_second, queries_and_scores, reads_and_locals]
    first_beside = max(1, far[0] - 3)

    stretch = running_kept
    late, late_kept, early = None, None, jnp.zeros((depth, depth), f32)
    for hop in range(1, far[0] + 1):
        for part in range(2):
            for side in range(2):
                if hop <= far[side]:
                    m_copy(side, hop, part, source[side](hop)).wait_recv()
                    m_forward(side, hop + 1, part)
        zz = source[0](hop)
        value = jnp.where(z >= hop, maps[zz, 0].astype(f32), 0.0)
        erase = maps[zz, 1].astype(f32)
        if late is None:
            late, late_kept = (value, erase), stretch
        else:
            late = compose((value, erase), stretch, late, late_kept)
            late_kept = late_kept * stretch
        if hop <= far[1]:
            zz = source[1](hop)
            new = stretch * early + maps[zz, 0].astype(f32) - dot(maps[zz, 1], early)
            early = jnp.where(z + hop >= hops, new, 0.0)
        if hop >= first_beside and beside:
            beside.pop(0)()
    for one in beside:
        one()
    state = late[0] + late_kept * early - dot(late[1], early)

    out = jnp.concatenate(late_work["locals"], axis=0)
    out = out + dot(jnp.concatenate(late_work["reads"], axis=0), state)
    out = out * lax.rsqrt(jnp.mean(out * out, axis=-1, keepdims=True) + out_epsilon)
    gated = (out * out_gain_ref[...] * late_work["gate"]).astype(bf16)

    full_out = second_half[:, :, :, 2 * depth :].reshape(width, depth)
    order = [2, 1, 3, 0]
    batch = chips * PAD
    row, col = iota((batch, span), 0), iota((batch, span), 1)

    def owned_by(dy, cc):
        owner = ((y + dy) % seqs * chips + row // PAD) * CORES + cc
        match = (col == owner * here_rows + row % PAD) & (row % PAD < here_rows)
        return jnp.where(match, 1.0, 0.0)

    def products(cc):
        rows = dot(jnp.concatenate([owned_by(dy, cc) for dy in order], axis=0), gated)
        return dot(rows, full_out, NT)

    theirs = products(1 - core).astype(bf16)
    for i in range(seqs):
        swap_out[i] = theirs[i * batch : (i + 1) * batch].reshape(chips, PAD, width)
        launch(swap_out.at[i], swap_in.at[i], s_send.at[i], s_recv.at[i], partner)
    mine = products(core)
    for i, dy in enumerate(order):
        copy(swap_in.at[i], swap_in.at[i], s_send.at[i], s_recv.at[i], me).wait_recv()
        total = mine[i * batch : (i + 1) * batch].reshape(chips, PAD, width) + swap_in[i].astype(f32)
        parts[i] = total.astype(bf16)
        for dx in range(chips):
            if dy or dx:
                launch(
                    parts.at[i, (x + dx) % chips],
                    landed.at[y * chips + x],
                    o_send.at[dy * chips + dx],
                    o_recv.at[(seqs - dy) % seqs * chips + (chips - dx) % chips],
                    at(0, dy, dx),
                )
    landed[y * chips + x] = parts[seqs - 1, x]
    for dy, dx in plane:
        slot = landed.at[(y + dy) % seqs * chips + (x + dx) % chips]
        index = dy * chips + dx
        copy(slot, slot, o_send.at[index], o_recv.at[index], me).wait_recv()
    for seq in range(seqs):
        total = landed[seq * chips].astype(f32)
        for chip in range(1, chips):
            total = total + landed[seq * chips + chip].astype(f32)
        out_ref[:, seq, :] = total[:here_rows].astype(bf16)
    for one in pending:
        one.wait_send()


def body(
    tokens,
    in_gain,
    w_query,
    w_key,
    w_value,
    w_gate,
    w_beta,
    conv_query,
    conv_key,
    conv_value,
    decay_rate,
    out_gain,
    w_out,
):
    here_rows, seqs, width = tokens.shape
    depth = w_query.shape[1]
    group, length = lax.axis_size("tp"), lax.axis_size("sp")
    hops = length // seqs
    chips = group // CORES
    owners = seqs * group
    span = owners * here_rows
    block = w_query.shape[0]
    sizes = (depth, seqs, group, hops, here_rows, width)
    anywhere = pl.BlockSpec(memory_space=pl.ANY)
    dma = pltpu.SemaphoreType.DMA
    vmem = pltpu.VMEM
    far = hops // 2 + 1
    return pl.pallas_call(
        functools.partial(mixer_kernel, sizes),
        out_shape=jax.ShapeDtypeStruct(tokens.shape, bf16),
        in_specs=[anywhere] * 10 + [pl.BlockSpec(memory_space=pltpu.SMEM)] + [anywhere] * 2,
        out_specs=pl.BlockSpec(memory_space=vmem),
        scratch_shapes=[
            vmem(tokens.shape, bf16),
            vmem((1, width), f32),
            vmem((1, block), bf16),
            vmem(conv_query.shape, bf16),
            vmem(conv_query.shape, bf16),
            vmem(conv_query.shape, bf16),
            vmem((1, depth), f32),
            vmem((hops, seqs, block, 3 * depth), bf16),
            vmem((hops, seqs, block, 3 * depth), bf16),
            vmem((seqs, PAD, width), bf16),
            vmem((1 + owners, PAD, width), bf16),
            vmem((PAD + span, 2 * depth), f32),
            vmem((hops, 2, depth, depth), bf16),
            vmem((seqs, chips, PAD, width), bf16),
            vmem((seqs, chips, PAD, width), bf16),
            vmem((seqs, chips, PAD, width), bf16),
            vmem((seqs * chips, PAD, width), bf16),
            dma((12,)),
            dma((2, hops)),
            dma((2, hops)),
            dma((hops, seqs)),
            dma((hops, seqs)),
            dma((seqs,)),
            dma((seqs,)),
            dma((seqs * chips,)),
            dma((seqs * chips,)),
            dma((seqs * chips,)),
            dma((seqs * chips,)),
            dma,
            dma,
            dma((2, far, 2)),
            dma((2, far, 2)),
            dma((seqs,)),
            dma((seqs,)),
            dma((seqs * chips,)),
            dma((seqs * chips,)),
        ],
        compiler_params=pltpu.CompilerParams(
            collective_id=0, has_side_effects=True, vmem_limit_bytes=56 * 1024 * 1024
        ),
    )(
        tokens,
        in_gain[None],
        w_query,
        w_key,
        w_value,
        w_gate,
        w_beta.T,
        conv_query,
        conv_key,
        conv_value,
        decay_rate,
        out_gain[None],
        w_out.T,
    )


def solution(mesh):
    placed = (
        P(("sp", "tp"), None, None),
        P(),
        P("sp", "tp"),
        P("sp", "tp"),
        P("sp", "tp"),
        P("sp", "tp"),
        P("sp", "tp"),
        P(None, "tp"),
        P(None, "tp"),
        P(None, "tp"),
        P("tp"),
        P(),
        P("tp", "sp"),
    )
    return jax.shard_map(
        body, mesh=mesh, in_specs=placed, out_specs=P(("sp", "tp"), None, None), check_vma=False
    )
```

```python
import functools
import math

import jax
import jax.numpy as jnp
from jax import lax
from jax.experimental import pallas as pl
from jax.experimental.pallas import tpu as pltpu
from jax.sharding import PartitionSpec as P

MESH = pl.DeviceIdType.MESH
PAD = 16
CHUNKS = 3
CORES = 2
REACH = 4
FIRST_BESIDE = 4
epsilon = 1e-06
out_epsilon = 1e-10
f32 = jnp.float32
bf16 = jnp.bfloat16
NN, NT, TN = ((1,), (0,)), ((1,), (1,)), ((0,), (0,))


def dot(a, b, dims=NN):
    return lax.dot_general(
        a.astype(bf16), b.astype(bf16), (dims, ((), ())), preferred_element_type=f32
    )


def iota(shape, axis):
    return lax.broadcasted_iota(jnp.int32, shape, axis)


def l2_normalize(array):
    return array * lax.rsqrt(jnp.sum(array * array, axis=-1, keepdims=True) + epsilon)


def unit_inverses(lowers, row, col):
    size = row.shape[0]
    near = ((row >> 1) == (col >> 1)) & (row != col)
    eye = jnp.where(row == col, 1.0, 0.0)
    inverses = [eye - jnp.where(near, lower, 0.0) for lower in lowers]
    level = 1
    while (1 << level) < size:
        mask = ((row >> (level + 1)) == (col >> (level + 1))) & ((row >> level) != (col >> level))
        inner = [dot(jnp.where(mask, l, 0.0), v) for l, v in zip(lowers, inverses)]
        inverses = [v - dot(v, w) for v, w in zip(inverses, inner)]
        level += 1
    return inverses


def compose(first, kept_first, second, kept_second):
    depth = first[0].shape[0]
    cross = dot(second[1], jnp.concatenate(first, axis=1))
    value = kept_second * first[0] + second[0] - cross[:, :depth]
    erase = kept_second * first[1] + kept_first * second[1] - cross[:, depth:]
    return value, erase


def mixer_kernel(
    sizes,
    tokens_hbm,
    in_gain_hbm,
    wq_hbm,
    wk_hbm,
    wv_hbm,
    wg_hbm,
    wb_hbm,
    cq_hbm,
    ck_hbm,
    cv_hbm,
    rate_ref,
    out_gain_hbm,
    wo_hbm,
    out_ref,
    tokens_ref,
    in_gain_ref,
    beta_ref,
    cq_ref,
    ck_ref,
    cv_ref,
    out_gain_ref,
    first_half,
    second_half,
    spread,
    rows_buf,
    conv_buf,
    maps,
    swap_out,
    swap_in,
    parts,
    landed,
    load,
    z_send,
    z_recv,
    y_send,
    y_recv,
    q_send,
    q_recv,
    t_send,
    t_recv,
    c_send,
    c_recv,
    h_send,
    h_recv,
    m_send,
    m_recv,
    s_send,
    s_recv,
    o_send,
    o_recv,
):
    depth, seqs, group, hops, here_rows, width = sizes
    chips = group // CORES
    total_tokens = hops * seqs * group * here_rows
    span = seqs * group * here_rows
    size = span // CHUNKS
    sp, tp = lax.axis_index("sp"), lax.axis_index("tp")
    z, y = sp // seqs, sp % seqs
    x, core = tp // CORES, tp % CORES
    far = [hops // 2, (hops - 1) // 2]
    halves = [first_half, second_half]
    pending = []

    def at(dz, dy, dx, dc=0):
        return {
            "sp": (z + dz) % hops * seqs + (y + dy) % seqs,
            "tp": (x + dx) % chips * CORES + (core + dc) % CORES,
        }

    def copy(src, dst, send, recv, device):
        return pltpu.make_async_remote_copy(
            src_ref=src,
            dst_ref=dst,
            send_sem=send,
            recv_sem=recv,
            device_id=device,
            device_id_type=MESH,
        )

    me = {"sp": sp, "tp": tp}
    partner = at(0, 0, 0, 1)

    def launch(*args):
        one = copy(*args)
        one.start()
        pending.append(one)

    barrier = pltpu.get_barrier_semaphore()
    plane = [(dy, dx) for dy in range(seqs) for dx in range(chips) if dy or dx]
    reach = [d for d in range(1, REACH + 1) if d <= far[0]]
    reach_back = [d for d in range(1, REACH + 1) if d <= far[1]]
    friends = [partner] + [at(0, dy, dx) for dy, dx in plane]
    friends += [at(d, 0, 0) for d in reach] + [at(hops - d, 0, 0) for d in reach]
    for device in friends:
        pl.semaphore_signal(barrier, inc=1, device_id=device, device_id_type=MESH)

    def own(half, part):
        return halves[half].at[z, y, :, pl.ds(part * depth, depth)]

    loads = [
        (tokens_hbm, tokens_ref),
        (in_gain_hbm, in_gain_ref),
        (wk_hbm, own(0, 0)),
        (wv_hbm, own(0, 1)),
        (wb_hbm, beta_ref),
        (wq_hbm, own(1, 0)),
        (wg_hbm, own(1, 1)),
        (wo_hbm, own(1, 2)),
        (cq_hbm, cq_ref),
        (ck_hbm, ck_ref),
        (cv_hbm, cv_ref),
        (out_gain_hbm, out_gain_ref),
    ]
    loads = [pltpu.make_async_copy(a, b, load.at[i]) for i, (a, b) in enumerate(loads)]
    for one in loads:
        one.start()
    for one in loads:
        one.wait()

    block = wk_hbm.shape[0]
    unit = jnp.where(iota((block, block), 0) == iota((block, block), 1), 1.0, 0.0)
    column = jnp.broadcast_to(beta_ref[...].astype(f32), (depth, block))
    first_half[z, y, :, 2 * depth :] = dot(unit, column, NT).astype(bf16)

    pad_rows = jnp.zeros((PAD - here_rows, width), f32)
    for seq in range(seqs):
        values = tokens_ref[:, seq, :].astype(f32)
        scaled = values * lax.rsqrt(jnp.mean(values * values, axis=-1, keepdims=True) + epsilon)
        spread[seq] = jnp.concatenate([scaled * in_gain_ref[...], pad_rows], axis=0).astype(bf16)

    pl.semaphore_wait(barrier, len(friends))

    def z_copy(half, index, offset, device):
        one = halves[half].at[(z + offset) % hops, y]
        return copy(one, one, z_send.at[half, index], z_recv.at[half, index], device)

    def z_launch(half, index, offset, device):
        one = z_copy(half, index, offset, device)
        one.start()
        pending.append(one)

    def offset_of(index):
        return hops - index if index <= far[0] else index - far[0]

    def z_first(half):
        for d in reversed(reach):
            z_launch(half, d, 0, at(d, 0, 0))
            if d in reach_back:
                z_launch(half, far[0] + d, 0, at(hops - d, 0, 0))

    def z_arrived(half, index):
        z_copy(half, index, offset_of(index), me).wait_recv()

    def z_relay(half):
        for further in range(far[0] - REACH):
            if further == 0:
                z_arrived(half, REACH)
            index = far[0] - further
            z_launch(half, index, hops - REACH, at(index - REACH, 0, 0))
        for further in range(far[1] - REACH):
            if further == 0:
                z_arrived(half, far[0] + REACH)
            d = far[1] - further
            z_launch(half, far[0] + d, REACH, at(hops - (d - REACH), 0, 0))

    def y_copy(index, dy, offset, yy, device, back=None):
        one = first_half.at[(z + offset) % hops, yy]
        back = dy if back is None else back
        return copy(one, one, y_send.at[index, dy], y_recv.at[index, back], device)

    def y_fan(index):
        offset = offset_of(index) if index else 0
        for dy in (2, 1, 3):
            one = y_copy(index, dy, offset, y, at(0, dy, 0), seqs - dy)
            one.start()
            pending.append(one)

    def t_slot(yy, xx, cc):
        return rows_buf.at[1 + (yy * chips + xx) * CORES + cc]

    relayed = far[0] > REACH
    z_first(0)
    for index, (dy, dx) in enumerate(plane):
        launch(
            spread.at[(y + dy) % seqs],
            t_slot(y, x, core),
            t_send.at[index],
            t_recv.at[(seqs - dy) % seqs * chips + (chips - dx) % chips],
            at(0, dy, dx),
        )
    y_fan(0)
    launch(spread.at[y], t_slot(y, x, core), c_send.at[0], c_recv.at[0], partner)
    rows_buf[1 + (y * chips + x) * CORES + core] = spread[y]
    z_first(1)

    if relayed:
        z_relay(0)
        y_fan(REACH)
        y_fan(far[0] + REACH)
    for d in range(1, REACH if relayed else REACH + 1):
        for index in [d, far[0] + d]:
            if d <= far[index > far[0]]:
                z_arrived(0, index)
                y_fan(index)
    for dy, dx in plane:
        index = dy * chips + dx
        slot = t_slot((y + dy) % seqs, (x + dx) % chips, core)
        copy(slot, slot, t_send.at[0], t_recv.at[index], me).wait_recv()
        launch(slot, slot, c_send.at[index], c_recv.at[index], partner)
    if relayed:
        for d in range(REACH + 1, far[0] + 1):
            for index in [d, far[0] + d]:
                if d <= far[index > far[0]]:
                    z_arrived(0, index)
                    y_fan(index)
        z_relay(1)
    for dy, dx in [(0, 0)] + plane:
        index = dy * chips + dx
        slot = t_slot((y + dy) % seqs, (x + dx) % chips, (core + 1) % CORES)
        copy(slot, slot, c_send.at[0], c_recv.at[index], me).wait_recv()
    history = copy(rows_buf.at[seqs * group], rows_buf.at[0], h_send, h_recv, at(1, 0, 0))
    history.start()
    pending.append(history)
    for index in range(far[0] + far[1] + 1):
        offset = offset_of(index) if index else 0
        for dy in (1, 3, 2):
            y_copy(index, dy, offset, (y + dy) % seqs, me).wait_recv()
    history.wait_recv()

    full = PAD + span
    padded = (1 + seqs * group) * PAD
    row, col = iota((full, padded), 0), iota((full, padded), 1)
    place, inside = col // PAD, col % PAD
    select = (row == PAD + (place - 1) * here_rows + inside) & (inside < here_rows)
    select = jnp.where(select & ((place > 0) | (z > 0)), 1.0, 0.0).astype(bf16)

    def project(half, columns):
        weights = half[:, :, :, :columns].reshape(width, columns)
        pre = dot(rows_buf[...].reshape(padded, width), weights).astype(bf16)
        return dot(select, pre)

    pre = project(first_half, 3 * depth)
    conv_buf[:, : 2 * depth] = pre[:, : 2 * depth]
    shift = math.log(depth / (4.0 * total_tokens))
    beta = jax.nn.sigmoid(pre[PAD:, 2 * depth :] + shift)
    width_taps = cq_ref.shape[0]

    def conv(part, taps_ref, begin):
        columns = slice(part * depth, (part + 1) * depth)
        total = jnp.zeros((size, depth), f32)
        for tap in range(width_taps):
            first = PAD + begin - (width_taps - 1) + tap
            taps = taps_ref[tap : tap + 1, :].astype(f32)
            total = total + conv_buf[first : first + size, columns] * taps
        return total * jax.nn.sigmoid(total)

    rate = rate_ref[0] / total_tokens
    row, col = iota((size, size), 0), iota((size, size), 1)
    decay = jnp.exp(-rate * jnp.maximum(row - col, 0).astype(f32))
    step = iota((size, depth), 0).astype(f32)
    kept = jnp.exp(-rate * (step + 1.0))
    rest = jnp.exp(-rate * (size - 1.0 - step))
    keys, values, betas = [], [], []
    for chunk in range(CHUNKS):
        begin = chunk * size
        keys.append(l2_normalize(conv(0, ck_ref, begin)))
        values.append(conv(1, cv_ref, begin))
        betas.append(beta[begin : begin + size])
    weighted = [k * b for k, b in zip(keys, betas)]
    lowers = [
        jnp.where(row > col, dot(w, k, NT) * decay, 0.0) for w, k in zip(weighted, keys)
    ]
    inverses = unit_inverses(lowers, row, col)
    both = [
        dot(inv, jnp.concatenate([v * b, w * kept], axis=1))
        for inv, v, b, w in zip(inverses, values, betas, weighted)
    ]
    moved = [dot(k * rest, b, TN) for k, b in zip(keys, both)]
    chunk_maps = [(m[:, :depth], m[:, depth:]) for m in moved]
    chunk_kept = jnp.exp(-rate * jnp.full((1, depth), float(size), f32))
    before, before_kept = [], []
    running, running_kept = chunk_maps[0], chunk_kept
    for chunk in range(1, CHUNKS):
        before.append(running)
        before_kept.append(running_kept)
        running = compose(running, running_kept, chunk_maps[chunk], chunk_kept)
        running_kept = running_kept * chunk_kept
    for part in range(2):
        maps[z, part] = running[part].astype(bf16)

    source = [lambda d: (z + hops - d) % hops, lambda d: (z + d) % hops]

    def m_copy(side, hop, part, offset, device):
        one = maps.at[source[side](offset), part]
        return copy(one, one, m_send.at[side, hop, part], m_recv.at[side, hop, part], device)

    def m_forward(behind):
        for step in (2, 1):
            for part in range(2):
                for side in range(2):
                    if behind + step <= far[side]:
                        device = at(step if side == 0 else hops - step, 0, 0)
                        one = m_copy(side, behind + step, part, behind, device)
                        one.start()
                        pending.append(one)

    def m_arrived(hop):
        for part in range(2):
            for side in range(2):
                if hop <= far[side]:
                    m_copy(side, hop, part, hop, me).wait_recv()

    m_forward(0)

    for d in range(1, far[0] + 1):
        for index in [d, far[0] + d]:
            if d <= far[index > far[0]] and not (relayed and d == REACH):
                z_arrived(1, index)
    for dy in (2, 1, 3):
        one = second_half.at[:, y]
        launch(one, one, q_send.at[dy], q_recv.at[seqs - dy], at(0, dy, 0))

    late_work = {}

    def project_second():
        for dy in (1, 3, 2):
            one = second_half.at[:, (y + dy) % seqs]
            copy(one, one, q_send.at[dy], q_recv.at[dy], me).wait_recv()
        pre = project(second_half, 2 * depth)
        conv_buf[:, : depth] = pre[:, :depth]
        gate_pre = pre[PAD:, depth:]
        late_work["gate"] = gate_pre * jax.nn.sigmoid(gate_pre)

    def queries_and_scores():
        queries = [
            l2_normalize(conv(0, cq_ref, chunk * size)) * depth ** (-0.5) for chunk in range(CHUNKS)
        ]
        late_work["queries"] = queries
        late_work["scores"] = [
            jnp.where(row >= col, dot(q, k, NT) * decay, 0.0) for q, k in zip(queries, keys)
        ]

    def reads_and_locals():
        reads, locals_ = [], []
        for chunk in range(CHUNKS):
            seen = dot(late_work["scores"][chunk], both[chunk])
            read = late_work["queries"][chunk] * kept - seen[:, depth:]
            local = seen[:, :depth]
            if chunk:
                value, erase = before[chunk - 1]
                shifted = dot(read, jnp.concatenate([value, erase], axis=1))
                local = local + shifted[:, :depth]
                read = before_kept[chunk - 1] * read - shifted[:, depth:]
            reads.append(read.astype(bf16))
            locals_.append(local)
        late_work["reads"], late_work["locals"] = reads, locals_

    beside = [project_second, queries_and_scores, reads_and_locals]
    stretch = running_kept
    late, late_kept, early = None, None, jnp.zeros((depth, depth), f32)
    for stage in range(2, far[0] + 2, 2):
        if stage <= far[0]:
            m_arrived(stage)
            m_forward(stage)
        for hop in (stage - 1, stage):
            if hop > far[0]:
                continue
            if hop < stage:
                m_arrived(hop)
            zz = source[0](hop)
            value = jnp.where(z >= hop, maps[zz, 0].astype(f32), 0.0)
            erase = maps[zz, 1].astype(f32)
            if late is None:
                late, late_kept = (value, erase), stretch
            else:
                late = compose((value, erase), stretch, late, late_kept)
                late_kept = late_kept * stretch
            if hop <= far[1]:
                zz = source[1](hop)
                new = stretch * early + maps[zz, 0].astype(f32) - dot(maps[zz, 1], early)
                early = jnp.where(z + hop >= hops, new, 0.0)
        if stage >= FIRST_BESIDE and beside:
            beside.pop(0)()
    for one in beside:
        one()
    state = late[0] + late_kept * early - dot(late[1], early)

    out = jnp.concatenate(late_work["locals"], axis=0)
    out = out + dot(jnp.concatenate(late_work["reads"], axis=0), state)
    out = out * lax.rsqrt(jnp.mean(out * out, axis=-1, keepdims=True) + out_epsilon)
    gated = (out * out_gain_ref[...] * late_work["gate"]).astype(bf16)

    full_out = second_half[:, :, :, 2 * depth :].reshape(width, depth)
    order = [2, 1, 3, 0]
    batch = chips * PAD
    row, col = iota((batch, span), 0), iota((batch, span), 1)

    def owned_by(dy, cc):
        owner = ((y + dy) % seqs * chips + row // PAD) * CORES + cc
        match = (col == owner * here_rows + row % PAD) & (row % PAD < here_rows)
        return jnp.where(match, 1.0, 0.0)

    def products(cc):
        rows = dot(jnp.concatenate([owned_by(dy, cc) for dy in order], axis=0), gated)
        return dot(rows, full_out, NT)

    theirs = products(1 - core).astype(bf16)
    for i in range(seqs):
        swap_out[i] = theirs[i * batch : (i + 1) * batch].reshape(chips, PAD, width)
        launch(swap_out.at[i], swap_in.at[i], s_send.at[i], s_recv.at[i], partner)
    mine = products(core)
    for i, dy in enumerate(order):
        copy(swap_in.at[i], swap_in.at[i], s_send.at[i], s_recv.at[i], me).wait_recv()
        total = mine[i * batch : (i + 1) * batch].reshape(chips, PAD, width) + swap_in[i].astype(f32)
        parts[i] = total.astype(bf16)
        for dx in range(chips):
            if dy or dx:
                launch(
                    parts.at[i, (x + dx) % chips],
                    landed.at[y * chips + x],
                    o_send.at[dy * chips + dx],
                    o_recv.at[(seqs - dy) % seqs * chips + (chips - dx) % chips],
                    at(0, dy, dx),
                )
    landed[y * chips + x] = parts[seqs - 1, x]
    for dy, dx in plane:
        slot = landed.at[(y + dy) % seqs * chips + (x + dx) % chips]
        index = dy * chips + dx
        copy(slot, slot, o_send.at[index], o_recv.at[index], me).wait_recv()
    for seq in range(seqs):
        total = landed[seq * chips].astype(f32)
        for chip in range(1, chips):
            total = total + landed[seq * chips + chip].astype(f32)
        out_ref[:, seq, :] = total[:here_rows].astype(bf16)
    for one in pending:
        one.wait_send()


def body(
    tokens,
    in_gain,
    w_query,
    w_key,
    w_value,
    w_gate,
    w_beta,
    conv_query,
    conv_key,
    conv_value,
    decay_rate,
    out_gain,
    w_out,
):
    here_rows, seqs, width = tokens.shape
    depth = w_query.shape[1]
    group, length = lax.axis_size("tp"), lax.axis_size("sp")
    hops = length // seqs
    chips = group // CORES
    owners = seqs * group
    span = owners * here_rows
    block = w_query.shape[0]
    sizes = (depth, seqs, group, hops, here_rows, width)
    anywhere = pl.BlockSpec(memory_space=pl.ANY)
    dma = pltpu.SemaphoreType.DMA
    vmem = pltpu.VMEM
    far = hops // 2 + 1
    return pl.pallas_call(
        functools.partial(mixer_kernel, sizes),
        out_shape=jax.ShapeDtypeStruct(tokens.shape, bf16),
        in_specs=[anywhere] * 10 + [pl.BlockSpec(memory_space=pltpu.SMEM)] + [anywhere] * 2,
        out_specs=pl.BlockSpec(memory_space=vmem),
        scratch_shapes=[
            vmem(tokens.shape, bf16),
            vmem((1, width), f32),
            vmem((1, block), bf16),
            vmem(conv_query.shape, bf16),
            vmem(conv_query.shape, bf16),
            vmem(conv_query.shape, bf16),
            vmem((1, depth), f32),
            vmem((hops, seqs, block, 3 * depth), bf16),
            vmem((hops, seqs, block, 3 * depth), bf16),
            vmem((seqs, PAD, width), bf16),
            vmem((1 + owners, PAD, width), bf16),
            vmem((PAD + span, 2 * depth), f32),
            vmem((hops, 2, depth, depth), bf16),
            vmem((seqs, chips, PAD, width), bf16),
            vmem((seqs, chips, PAD, width), bf16),
            vmem((seqs, chips, PAD, width), bf16),
            vmem((seqs * chips, PAD, width), bf16),
            dma((12,)),
            dma((2, hops)),
            dma((2, hops)),
            dma((hops, seqs)),
            dma((hops, seqs)),
            dma((seqs,)),
            dma((seqs,)),
            dma((seqs * chips,)),
            dma((seqs * chips,)),
            dma((seqs * chips,)),
            dma((seqs * chips,)),
            dma,
            dma,
            dma((2, far, 2)),
            dma((2, far, 2)),
            dma((seqs,)),
            dma((seqs,)),
            dma((seqs * chips,)),
            dma((seqs * chips,)),
        ],
        compiler_params=pltpu.CompilerParams(
            collective_id=0, has_side_effects=True, vmem_limit_bytes=56 * 1024 * 1024
        ),
    )(
        tokens,
        in_gain[None],
        w_query,
        w_key,
        w_value,
        w_gate,
        w_beta.T,
        conv_query,
        conv_key,
        conv_value,
        decay_rate,
        out_gain[None],
        w_out.T,
    )


def solution(mesh):
    placed = (
        P(("sp", "tp"), None, None),
        P(),
        P("sp", "tp"),
        P("sp", "tp"),
        P("sp", "tp"),
        P("sp", "tp"),
        P("sp", "tp"),
        P(None, "tp"),
        P(None, "tp"),
        P(None, "tp"),
        P("tp"),
        P(),
        P("tp", "sp"),
    )
    return jax.shard_map(
        body, mesh=mesh, in_specs=placed, out_specs=P(("sp", "tp"), None, None), check_vma=False
    )
```

```python
import functools
import math

import jax
import jax.numpy as jnp
from jax import lax
from jax.experimental import pallas as pl
from jax.experimental.pallas import tpu as pltpu
from jax.sharding import PartitionSpec as P

MESH = pl.DeviceIdType.MESH
PAD = 16
CHUNKS = 3
CORES = 2
REACH = 4
FIRST_BESIDE = 4
FOLD = 4
epsilon = 1e-06
out_epsilon = 1e-10
f32 = jnp.float32
bf16 = jnp.bfloat16
NN, NT, TN = ((1,), (0,)), ((1,), (1,)), ((0,), (0,))


def dot(a, b, dims=NN):
    return lax.dot_general(
        a.astype(bf16), b.astype(bf16), (dims, ((), ())), preferred_element_type=f32
    )


def iota(shape, axis):
    return lax.broadcasted_iota(jnp.int32, shape, axis)


def l2_normalize(array):
    return array * lax.rsqrt(jnp.sum(array * array, axis=-1, keepdims=True) + epsilon)


def unit_inverses(lowers, row, col):
    size = row.shape[0]
    near = ((row >> 1) == (col >> 1)) & (row != col)
    eye = jnp.where(row == col, 1.0, 0.0)
    inverses = [eye - jnp.where(near, lower, 0.0) for lower in lowers]
    level = 1
    while (1 << level) < size:
        mask = ((row >> (level + 1)) == (col >> (level + 1))) & ((row >> level) != (col >> level))
        inner = [dot(jnp.where(mask, l, 0.0), v) for l, v in zip(lowers, inverses)]
        inverses = [v - dot(v, w) for v, w in zip(inverses, inner)]
        level += 1
    return inverses


def compose(first, kept_first, second, kept_second):
    depth = first[0].shape[0]
    cross = dot(second[1], jnp.concatenate(first, axis=1))
    value = kept_second * first[0] + second[0] - cross[:, :depth]
    erase = kept_second * first[1] + kept_first * second[1] - cross[:, depth:]
    return value, erase


def mixer_kernel(
    sizes,
    tokens_hbm,
    in_gain_hbm,
    wq_hbm,
    wk_hbm,
    wv_hbm,
    wg_hbm,
    wb_hbm,
    cq_hbm,
    ck_hbm,
    cv_hbm,
    rate_ref,
    out_gain_hbm,
    wo_hbm,
    out_ref,
    tokens_ref,
    in_gain_ref,
    beta_ref,
    cq_ref,
    ck_ref,
    cv_ref,
    out_gain_ref,
    first_half,
    second_half,
    strengths,
    spread,
    tail_out,
    tail_in,
    select_buf,
    owned_buf,
    out_weights,
    rows_buf,
    conv_buf,
    maps,
    swap_out,
    swap_in,
    parts,
    landed,
    load,
    z_send,
    z_recv,
    y_send,
    y_recv,
    g_send,
    g_recv,
    q_send,
    q_recv,
    t_send,
    t_recv,
    c_send,
    c_recv,
    h_send,
    h_recv,
    m_send,
    m_recv,
    s_send,
    s_recv,
    o_send,
    o_recv,
):
    depth, seqs, group, hops, here_rows, width = sizes
    chips = group // CORES
    total_tokens = hops * seqs * group * here_rows
    span = seqs * group * here_rows
    size = span // CHUNKS
    sp, tp = lax.axis_index("sp"), lax.axis_index("tp")
    z, y = sp // seqs, sp % seqs
    x, core = tp // CORES, tp % CORES
    far = [hops // 2, (hops - 1) // 2]
    last = (y == seqs - 1) & (tp == group - 1)
    pending = []

    def at(dz, dy, dx, dc=0):
        return {
            "sp": (z + dz) % hops * seqs + (y + dy) % seqs,
            "tp": (x + dx) % chips * CORES + (core + dc) % CORES,
        }

    def copy(src, dst, send, recv, device):
        return pltpu.make_async_remote_copy(
            src_ref=src,
            dst_ref=dst,
            send_sem=send,
            recv_sem=recv,
            device_id=device,
            device_id_type=MESH,
        )

    me = {"sp": sp, "tp": tp}
    partner = at(0, 0, 0, 1)

    def launch(*args):
        one = copy(*args)
        one.start()
        pending.append(one)

    barrier = pltpu.get_barrier_semaphore()
    plane = [(dy, dx) for dy in range(seqs) for dx in range(chips) if dy or dx]
    reach = [d for d in range(1, REACH + 1) if d <= far[0]]
    reach_back = [d for d in range(1, REACH + 1) if d <= far[1]]
    friends = [partner] + [at(0, dy, dx) for dy, dx in plane]
    friends += [at(d, 0, 0) for d in reach] + [at(hops - d, 0, 0) for d in reach]
    for device in friends:
        pl.semaphore_signal(barrier, inc=1, device_id=device, device_id_type=MESH)

    def own(half, part):
        return (first_half, second_half)[half].at[z, y, :, pl.ds(part * depth, depth)]

    loads = [
        (wk_hbm, own(0, 0)),
        (wv_hbm, own(0, 1)),
        (wb_hbm, beta_ref),
        (tokens_hbm, tokens_ref),
        (in_gain_hbm, in_gain_ref),
        (wq_hbm, own(1, 0)),
        (wg_hbm, own(1, 1)),
        (wo_hbm, own(1, 2)),
        (cq_hbm, cq_ref),
        (ck_hbm, ck_ref),
        (cv_hbm, cv_ref),
        (out_gain_hbm, out_gain_ref),
    ]
    loads = [pltpu.make_async_copy(a, b, load.at[i]) for i, (a, b) in enumerate(loads)]
    for one in loads:
        one.start()

    full = PAD + span
    padded = seqs * group * PAD
    row, col = iota((full, padded), 0), iota((full, padded), 1)
    place, inside = col // PAD, col % PAD
    select = (row == PAD + place * here_rows + inside) & (inside < here_rows)
    select = select | ((col - row == padded - PAD) & (inside >= here_rows) & (row < PAD))
    select_buf[...] = jnp.where(select, 1.0, 0.0).astype(bf16)

    order = [2, 1, 3, 0]
    folded = FOLD * here_rows
    batch = chips * folded
    row = iota((batch, 1), 0).astype(f32) + 0.5
    chip_of = jnp.floor(row / folded)
    fold_of = jnp.floor(row / here_rows) - FOLD * chip_of
    inside = row - 0.5 - here_rows * (FOLD * chip_of + fold_of)
    first = (CORES * here_rows * chip_of + inside).astype(jnp.int32)
    col = iota((batch, span), 1)
    for cc in range(CORES):
        for i, dy in enumerate(order):
            begin = ((y + dy) % seqs * chips * CORES + cc) * here_rows
            owned_buf[cc, i * batch : (i + 1) * batch, :] = jnp.where(
                col == first + begin, 1.0, 0.0
            ).astype(bf16)

    for one in loads:
        one.wait()

    block = wk_hbm.shape[0]
    strengths[z, y] = jnp.concatenate(
        [beta_ref[...].astype(f32), jnp.zeros((1, depth - block), f32)], axis=1
    )

    pl.semaphore_wait(barrier, len(friends))

    def z_copy(half, index, offset, device):
        zz = (z + offset) % hops
        one = strengths.at[zz] if half == 2 else (first_half, second_half)[half].at[zz, y]
        return copy(one, one, z_send.at[half, index], z_recv.at[half, index], device)

    def z_launch(half, index, offset, device):
        one = z_copy(half, index, offset, device)
        one.start()
        pending.append(one)

    def offset_of(index):
        return hops - index if index <= far[0] else index - far[0]

    def z_first(half):
        for d in reversed(reach):
            z_launch(half, d, 0, at(d, 0, 0))
            if d in reach_back:
                z_launch(half, far[0] + d, 0, at(hops - d, 0, 0))

    def z_arrived(half, index):
        z_copy(half, index, offset_of(index), me).wait_recv()

    def z_relay(half):
        for further in range(far[0] - REACH):
            if further == 0:
                z_arrived(half, REACH)
            index = far[0] - further
            z_launch(half, index, hops - REACH, at(index - REACH, 0, 0))
        for further in range(far[1] - REACH):
            if further == 0:
                z_arrived(half, far[0] + REACH)
            d = far[1] - further
            z_launch(half, far[0] + d, REACH, at(hops - (d - REACH), 0, 0))

    def y_copy(index, dy, offset, yy, device, back=None):
        one = first_half.at[(z + offset) % hops, yy]
        back = dy if back is None else back
        return copy(one, one, y_send.at[index, dy], y_recv.at[index, back], device)

    def y_fan(index):
        offset = offset_of(index) if index else 0
        for dy in (2, 1, 3):
            one = y_copy(index, dy, offset, y, at(0, dy, 0), seqs - dy)
            one.start()
            pending.append(one)

    def t_slot(yy, xx, cc):
        return rows_buf.at[(yy * chips + xx) * CORES + cc]

    relayed = far[0] > REACH
    z_first(0)
    for dy in (2, 1, 3):
        one = strengths.at[z, y]
        launch(one, one, g_send.at[dy], g_recv.at[seqs - dy], at(0, dy, 0))
    y_fan(0)

    pad_rows = jnp.zeros((PAD - here_rows, width), f32)
    tail_rows = PAD - here_rows
    for seq in range(seqs):
        values = tokens_ref[:, seq, :].astype(f32)
        scaled = values * lax.rsqrt(jnp.mean(values * values, axis=-1, keepdims=True) + epsilon)
        spread[seq] = jnp.concatenate([scaled * in_gain_ref[...], pad_rows], axis=0).astype(bf16)

    tail = copy(tail_out, tail_in, h_send, h_recv, at(1, 0, 0))

    @pl.when(last)
    def _():
        ends = [spread[seq].astype(f32)[here_rows - tail_rows : here_rows] for seq in range(seqs)]
        tail_out[...] = jnp.concatenate(ends, axis=0).astype(bf16)
        tail.start()
        tail.wait_recv()
        before = jnp.where(z > 0, tail_in[...].astype(f32), 0.0)
        for seq in range(seqs):
            rows = [
                spread[seq].astype(f32)[:here_rows],
                before[seq * tail_rows : (seq + 1) * tail_rows],
            ]
            spread[seq] = jnp.concatenate(rows, axis=0).astype(bf16)

    for index, (dy, dx) in enumerate(plane):
        launch(
            spread.at[(y + dy) % seqs],
            t_slot(y, x, core),
            t_send.at[index],
            t_recv.at[(seqs - dy) % seqs * chips + (chips - dx) % chips],
            at(0, dy, dx),
        )
    launch(spread.at[y], t_slot(y, x, core), c_send.at[0], c_recv.at[0], partner)
    rows_buf[(y * chips + x) * CORES + core] = spread[y]
    for dy in (1, 3, 2):
        one = strengths.at[z, (y + dy) % seqs]
        copy(one, one, g_send.at[dy], g_recv.at[dy], me).wait_recv()
    z_first(2)
    z_first(1)

    if relayed:
        z_relay(0)
        y_fan(REACH)
        y_fan(far[0] + REACH)
    for d in range(1, REACH if relayed else REACH + 1):
        for index in [d, far[0] + d]:
            if d <= far[index > far[0]]:
                z_arrived(0, index)
                y_fan(index)
    for dy, dx in plane:
        index = dy * chips + dx
        slot = t_slot((y + dy) % seqs, (x + dx) % chips, core)
        copy(slot, slot, t_send.at[0], t_recv.at[index], me).wait_recv()
        launch(slot, slot, c_send.at[index], c_recv.at[index], partner)
    if relayed:
        z_relay(2)
        for d in range(REACH + 1, far[0] + 1):
            for index in [d, far[0] + d]:
                if d <= far[index > far[0]]:
                    z_arrived(0, index)
                    y_fan(index)
        z_relay(1)
    for d in range(1, far[0] + 1):
        for index in [d, far[0] + d]:
            if d <= far[index > far[0]] and not (relayed and d == REACH):
                z_arrived(2, index)
    for dy, dx in [(0, 0)] + plane:
        index = dy * chips + dx
        slot = t_slot((y + dy) % seqs, (x + dx) % chips, (core + 1) % CORES)
        copy(slot, slot, c_send.at[0], c_recv.at[index], me).wait_recv()
    for index in range(far[0] + far[1] + 1):
        offset = offset_of(index) if index else 0
        for dy in (1, 3, 2):
            y_copy(index, dy, offset, (y + dy) % seqs, me).wait_recv()

    def project(weights):
        pre = dot(rows_buf[...].reshape(padded, width), weights).astype(bf16)
        return dot(select_buf[...], pre)

    devices = hops * seqs
    pick = iota((width, devices), 0) // block == iota((width, devices), 1)
    column = dot(jnp.where(pick, 1.0, 0.0), strengths[...].reshape(devices, depth))
    column = jnp.where(iota((width, depth), 0) % block == iota((width, depth), 1), column, 0.0)
    column = dot(column, jnp.ones((depth, depth), f32)).astype(bf16)
    weights = first_half[...].reshape(width, 2 * depth)
    pre = project(jnp.concatenate([weights, column], axis=1))
    conv_buf[...] = pre[:, : 2 * depth]
    shift = math.log(depth / (4.0 * total_tokens))
    beta = jax.nn.sigmoid(pre[PAD:, 2 * depth :] + shift)
    width_taps = cq_ref.shape[0]

    def conv(part, taps_ref, begin):
        columns = slice(part * depth, (part + 1) * depth)
        total = jnp.zeros((size, depth), f32)
        for tap in range(width_taps):
            first = PAD + begin - (width_taps - 1) + tap
            taps = taps_ref[tap : tap + 1, :].astype(f32)
            total = total + conv_buf[first : first + size, columns] * taps
        return total * jax.nn.sigmoid(total)

    rate = rate_ref[0] / total_tokens
    row, col = iota((size, size), 0), iota((size, size), 1)
    decay = jnp.exp(-rate * jnp.maximum(row - col, 0).astype(f32))
    step = iota((size, depth), 0).astype(f32)
    kept = jnp.exp(-rate * (step + 1.0))
    rest = jnp.exp(-rate * (size - 1.0 - step))
    keys, values, betas = [], [], []
    for chunk in range(CHUNKS):
        begin = chunk * size
        keys.append(l2_normalize(conv(0, ck_ref, begin)))
        values.append(conv(1, cv_ref, begin))
        betas.append(beta[begin : begin + size])
    weighted = [k * b for k, b in zip(keys, betas)]
    lowers = [
        jnp.where(row > col, dot(w, k, NT) * decay, 0.0) for w, k in zip(weighted, keys)
    ]
    inverses = unit_inverses(lowers, row, col)
    both = [
        dot(inv, jnp.concatenate([v * b, w * kept], axis=1))
        for inv, v, b, w in zip(inverses, values, betas, weighted)
    ]
    moved = [dot(k * rest, b, TN) for k, b in zip(keys, both)]
    chunk_maps = [(m[:, :depth], m[:, depth:]) for m in moved]
    chunk_kept = jnp.exp(-rate * jnp.full((1, depth), float(size), f32))
    before, before_kept = [], []
    running, running_kept = chunk_maps[0], chunk_kept
    for chunk in range(1, CHUNKS):
        before.append(running)
        before_kept.append(running_kept)
        running = compose(running, running_kept, chunk_maps[chunk], chunk_kept)
        running_kept = running_kept * chunk_kept
    for part in range(2):
        maps[z, part] = running[part].astype(bf16)

    source = [lambda d: (z + hops - d) % hops, lambda d: (z + d) % hops]

    def m_copy(side, hop, part, offset, device):
        one = maps.at[source[side](offset), part]
        return copy(one, one, m_send.at[side, hop, part], m_recv.at[side, hop, part], device)

    def m_forward(behind):
        for step in (2, 1):
            for part in range(2):
                for side in range(2):
                    if behind + step <= far[side]:
                        device = at(step if side == 0 else hops - step, 0, 0)
                        one = m_copy(side, behind + step, part, behind, device)
                        one.start()
                        pending.append(one)

    def m_arrived(hop):
        for part in range(2):
            for side in range(2):
                if hop <= far[side]:
                    m_copy(side, hop, part, hop, me).wait_recv()

    m_forward(0)

    for d in range(1, far[0] + 1):
        for index in [d, far[0] + d]:
            if d <= far[index > far[0]] and not (relayed and d == REACH):
                z_arrived(1, index)
    for dy in (2, 1, 3):
        one = second_half.at[:, y]
        launch(one, one, q_send.at[dy], q_recv.at[seqs - dy], at(0, dy, 0))

    late_work = {}

    def project_second():
        for dy in (1, 3, 2):
            one = second_half.at[:, (y + dy) % seqs]
            copy(one, one, q_send.at[dy], q_recv.at[dy], me).wait_recv()
        pre = project(second_half[:, :, :, : 2 * depth].reshape(width, 2 * depth))
        full_out = second_half[:, :, :, 2 * depth :].reshape(FOLD, width // FOLD, depth)
        for fold in range(FOLD):
            out_weights[:, fold * depth : (fold + 1) * depth] = full_out[fold]
        conv_buf[:, : depth] = pre[:, :depth]
        gate_pre = pre[PAD:, depth:]
        late_work["gate"] = gate_pre * jax.nn.sigmoid(gate_pre)

    def queries_and_scores():
        queries = [
            l2_normalize(conv(0, cq_ref, chunk * size)) * depth ** (-0.5) for chunk in range(CHUNKS)
        ]
        late_work["queries"] = queries
        late_work["scores"] = [
            jnp.where(row >= col, dot(q, k, NT) * decay, 0.0) for q, k in zip(queries, keys)
        ]

    def reads_and_locals():
        reads, locals_ = [], []
        for chunk in range(CHUNKS):
            seen = dot(late_work["scores"][chunk], both[chunk])
            read = late_work["queries"][chunk] * kept - seen[:, depth:]
            local = seen[:, :depth]
            if chunk:
                value, erase = before[chunk - 1]
                shifted = dot(read, jnp.concatenate([value, erase], axis=1))
                local = local + shifted[:, :depth]
                read = before_kept[chunk - 1] * read - shifted[:, depth:]
            reads.append(read.astype(bf16))
            locals_.append(local)
        late_work["reads"], late_work["locals"] = reads, locals_

    beside = [project_second, queries_and_scores, reads_and_locals]
    stretch = running_kept
    late, late_kept, early = None, None, jnp.zeros((depth, depth), f32)
    for stage in range(2, far[0] + 2, 2):
        if stage <= far[0]:
            m_arrived(stage)
            m_forward(stage)
        for hop in (stage - 1, stage):
            if hop > far[0]:
                continue
            if hop < stage:
                m_arrived(hop)
            zz = source[0](hop)
            value = jnp.where(z >= hop, maps[zz, 0].astype(f32), 0.0)
            erase = maps[zz, 1].astype(f32)
            if late is None:
                late, late_kept = (value, erase), stretch
            else:
                late = compose((value, erase), stretch, late, late_kept)
                late_kept = late_kept * stretch
            if hop <= far[1]:
                zz = source[1](hop)
                new = stretch * early + maps[zz, 0].astype(f32) - dot(maps[zz, 1], early)
                early = jnp.where(z + hop >= hops, new, 0.0)
        if stage >= FIRST_BESIDE and beside:
            beside.pop(0)()
    for one in beside:
        one()
    state = late[0] + late_kept * early - dot(late[1], early)

    out = jnp.concatenate(late_work["locals"], axis=0)
    out = out + dot(jnp.concatenate(late_work["reads"], axis=0), state)
    out = out * lax.rsqrt(jnp.mean(out * out, axis=-1, keepdims=True) + out_epsilon)
    gated = (out * out_gain_ref[...] * late_work["gate"]).astype(bf16)

    fold_row = fold_of.astype(jnp.int32)

    def products(cc):
        rows = dot(owned_buf[cc], gated)
        folds = jnp.concatenate([fold_row] * seqs, axis=0)
        wide = [jnp.where(folds == fold, rows, 0.0).astype(bf16) for fold in range(FOLD)]
        return dot(jnp.concatenate(wide, axis=1), out_weights[...], NT)

    theirs = products(1 - core).astype(bf16)
    for i in range(seqs):
        swap_out[i] = theirs[i * batch : (i + 1) * batch].reshape(chips, folded, -1)
        launch(swap_out.at[i], swap_in.at[i], s_send.at[i], s_recv.at[i], partner)
    mine = products(core)
    for i, dy in enumerate(order):
        copy(swap_in.at[i], swap_in.at[i], s_send.at[i], s_recv.at[i], me).wait_recv()
        total = mine[i * batch : (i + 1) * batch].reshape(chips, folded, -1) + swap_in[i].astype(f32)
        parts[i] = total.astype(bf16)
        for dx in range(chips):
            if dy or dx:
                launch(
                    parts.at[i, (x + dx) % chips],
                    landed.at[y * chips + x],
                    o_send.at[dy * chips + dx],
                    o_recv.at[(seqs - dy) % seqs * chips + (chips - dx) % chips],
                    at(0, dy, dx),
                )
    landed[y * chips + x] = parts[seqs - 1, x]
    for dy, dx in plane:
        slot = landed.at[(y + dy) % seqs * chips + (x + dx) % chips]
        index = dy * chips + dx
        copy(slot, slot, o_send.at[index], o_recv.at[index], me).wait_recv()
    for seq in range(seqs):
        total = landed[seq * chips].astype(f32)
        for chip in range(1, chips):
            total = total + landed[seq * chips + chip].astype(f32)
        rows = [total[fold * here_rows : (fold + 1) * here_rows] for fold in range(FOLD)]
        out_ref[:, seq, :] = jnp.concatenate(rows, axis=1).astype(bf16)
    for one in pending:
        one.wait_send()

    @pl.when(last)
    def _():
        tail.wait_send()


def body(
    tokens,
    in_gain,
    w_query,
    w_key,
    w_value,
    w_gate,
    w_beta,
    conv_query,
    conv_key,
    conv_value,
    decay_rate,
    out_gain,
    w_out,
):
    here_rows, seqs, width = tokens.shape
    depth = w_query.shape[1]
    group, length = lax.axis_size("tp"), lax.axis_size("sp")
    hops = length // seqs
    chips = group // CORES
    owners = seqs * group
    span = owners * here_rows
    block = w_query.shape[0]
    sizes = (depth, seqs, group, hops, here_rows, width)
    anywhere = pl.BlockSpec(memory_space=pl.ANY)
    dma = pltpu.SemaphoreType.DMA
    vmem = pltpu.VMEM
    far = hops // 2 + 1
    return pl.pallas_call(
        functools.partial(mixer_kernel, sizes),
        out_shape=jax.ShapeDtypeStruct(tokens.shape, bf16),
        in_specs=[anywhere] * 10 + [pl.BlockSpec(memory_space=pltpu.SMEM)] + [anywhere] * 2,
        out_specs=pl.BlockSpec(memory_space=vmem),
        scratch_shapes=[
            vmem(tokens.shape, bf16),
            vmem((1, width), f32),
            vmem((1, block), bf16),
            vmem(conv_query.shape, bf16),
            vmem(conv_query.shape, bf16),
            vmem(conv_query.shape, bf16),
            vmem((1, depth), f32),
            vmem((hops, seqs, block, 2 * depth), bf16),
            vmem((hops, seqs, block, 3 * depth), bf16),
            vmem((hops, seqs, 1, depth), f32),
            vmem((seqs, PAD, width), bf16),
            vmem((PAD, width), bf16),
            vmem((PAD, width), bf16),
            vmem((PAD + span, owners * PAD), bf16),
            vmem((CORES, owners // CORES * FOLD * here_rows, span), bf16),
            vmem((width // FOLD, FOLD * depth), bf16),
            vmem((owners, PAD, width), bf16),
            vmem((PAD + span, 2 * depth), f32),
            vmem((hops, 2, depth, depth), bf16),
            vmem((seqs, chips, FOLD * here_rows, width // FOLD), bf16),
            vmem((seqs, chips, FOLD * here_rows, width // FOLD), bf16),
            vmem((seqs, chips, FOLD * here_rows, width // FOLD), bf16),
            vmem((seqs * chips, FOLD * here_rows, width // FOLD), bf16),
            dma((12,)),
            dma((3, hops)),
            dma((3, hops)),
            dma((hops, seqs)),
            dma((hops, seqs)),
            dma((seqs,)),
            dma((seqs,)),
            dma((seqs,)),
            dma((seqs,)),
            dma((seqs * chips,)),
            dma((seqs * chips,)),
            dma((seqs * chips,)),
            dma((seqs * chips,)),
            dma,
            dma,
            dma((2, far, 2)),
            dma((2, far, 2)),
            dma((seqs,)),
            dma((seqs,)),
            dma((seqs * chips,)),
            dma((seqs * chips,)),
        ],
        compiler_params=pltpu.CompilerParams(
            collective_id=0, has_side_effects=True, vmem_limit_bytes=56 * 1024 * 1024
        ),
    )(
        tokens,
        in_gain[None],
        w_query,
        w_key,
        w_value,
        w_gate,
        w_beta.T,
        conv_query,
        conv_key,
        conv_value,
        decay_rate,
        out_gain[None],
        w_out.T,
    )


def solution(mesh):
    placed = (
        P(("sp", "tp"), None, None),
        P(),
        P("sp", "tp"),
        P("sp", "tp"),
        P("sp", "tp"),
        P("sp", "tp"),
        P("sp", "tp"),
        P(None, "tp"),
        P(None, "tp"),
        P(None, "tp"),
        P("tp"),
        P(),
        P("tp", "sp"),
    )
    return jax.shard_map(
        body, mesh=mesh, in_specs=placed, out_specs=P(("sp", "tp"), None, None), check_vma=False
    )
```

```python
import functools
import math

import jax
import jax.numpy as jnp
from jax import lax
from jax.experimental import pallas as pl
from jax.experimental.pallas import tpu as pltpu
from jax.sharding import PartitionSpec as P

MESH = pl.DeviceIdType.MESH
PAD = 16
CHUNKS = 3
CORES = 2
REACH = 4
FIRST_BESIDE = 4
FOLD = 4
epsilon = 1e-06
out_epsilon = 1e-10
f32 = jnp.float32
bf16 = jnp.bfloat16
NN, NT, TN = ((1,), (0,)), ((1,), (1,)), ((0,), (0,))


def dot(a, b, dims=NN):
    return lax.dot_general(
        a.astype(bf16), b.astype(bf16), (dims, ((), ())), preferred_element_type=f32
    )


def iota(shape, axis):
    return lax.broadcasted_iota(jnp.int32, shape, axis)


def l2_normalize(array):
    return array * lax.rsqrt(jnp.sum(array * array, axis=-1, keepdims=True) + epsilon)


def unit_inverses(lowers, row, col):
    size = row.shape[0]
    near = ((row >> 1) == (col >> 1)) & (row != col)
    eye = jnp.where(row == col, 1.0, 0.0)
    inverses = [eye - jnp.where(near, lower, 0.0) for lower in lowers]
    level = 1
    while (1 << level) < size:
        mask = ((row >> (level + 1)) == (col >> (level + 1))) & ((row >> level) != (col >> level))
        inner = [dot(jnp.where(mask, l, 0.0), v) for l, v in zip(lowers, inverses)]
        inverses = [v - dot(v, w) for v, w in zip(inverses, inner)]
        level += 1
    return inverses


def compose(first, kept_first, second, kept_second):
    depth = first[0].shape[0]
    cross = dot(second[1], jnp.concatenate(first, axis=1))
    value = kept_second * first[0] + second[0] - cross[:, :depth]
    erase = kept_second * first[1] + kept_first * second[1] - cross[:, depth:]
    return value, erase


def mixer_kernel(
    sizes,
    tokens_hbm,
    in_gain_hbm,
    wq_hbm,
    wk_hbm,
    wv_hbm,
    wg_hbm,
    wb_hbm,
    cq_hbm,
    ck_hbm,
    cv_hbm,
    rate_ref,
    out_gain_hbm,
    wo_hbm,
    out_ref,
    tokens_ref,
    in_gain_ref,
    beta_ref,
    cq_ref,
    ck_ref,
    cv_ref,
    out_gain_ref,
    first_half,
    second_half,
    strengths,
    spread,
    tail_out,
    tail_in,
    select_buf,
    owned_buf,
    reads_buf,
    locals_buf,
    gate_buf,
    out_weights,
    rows_buf,
    conv_buf,
    maps,
    swap_out,
    swap_in,
    parts,
    landed,
    load,
    z_send,
    z_recv,
    y_send,
    y_recv,
    g_send,
    g_recv,
    q_send,
    q_recv,
    t_send,
    t_recv,
    c_send,
    c_recv,
    h_send,
    h_recv,
    m_send,
    m_recv,
    s_send,
    s_recv,
    o_send,
    o_recv,
):
    depth, seqs, group, hops, here_rows, width = sizes
    chips = group // CORES
    total_tokens = hops * seqs * group * here_rows
    span = seqs * group * here_rows
    size = span // CHUNKS
    sp, tp = lax.axis_index("sp"), lax.axis_index("tp")
    z, y = sp // seqs, sp % seqs
    x, core = tp // CORES, tp % CORES
    far = [hops // 2, (hops - 1) // 2]
    last = (y == seqs - 1) & (tp == group - 1)
    pending = []

    def at(dz, dy, dx, dc=0):
        return {
            "sp": (z + dz) % hops * seqs + (y + dy) % seqs,
            "tp": (x + dx) % chips * CORES + (core + dc) % CORES,
        }

    def copy(src, dst, send, recv, device):
        return pltpu.make_async_remote_copy(
            src_ref=src,
            dst_ref=dst,
            send_sem=send,
            recv_sem=recv,
            device_id=device,
            device_id_type=MESH,
        )

    me = {"sp": sp, "tp": tp}
    partner = at(0, 0, 0, 1)

    def launch(*args):
        one = copy(*args)
        one.start()
        pending.append(one)

    barrier = pltpu.get_barrier_semaphore()
    plane = [(dy, dx) for dy in range(seqs) for dx in range(chips) if dy or dx]
    reach = [d for d in range(1, REACH + 1) if d <= far[0]]
    reach_back = [d for d in range(1, REACH + 1) if d <= far[1]]
    friends = [partner] + [at(0, dy, dx) for dy, dx in plane]
    friends += [at(d, 0, 0) for d in reach] + [at(hops - d, 0, 0) for d in reach]
    for device in friends:
        pl.semaphore_signal(barrier, inc=1, device_id=device, device_id_type=MESH)

    def own(half, part):
        return (first_half, second_half)[half].at[z, y, :, pl.ds(part * depth, depth)]

    loads = [
        (tokens_hbm, tokens_ref),
        (in_gain_hbm, in_gain_ref),
        (wk_hbm, own(0, 0)),
        (wv_hbm, own(0, 1)),
        (wb_hbm, beta_ref),
        (wq_hbm, own(1, 0)),
        (wg_hbm, own(1, 1)),
        (wo_hbm, own(1, 2)),
        (cq_hbm, cq_ref),
        (ck_hbm, ck_ref),
        (cv_hbm, cv_ref),
        (out_gain_hbm, out_gain_ref),
    ]
    loads = [pltpu.make_async_copy(a, b, load.at[i]) for i, (a, b) in enumerate(loads)]
    for one in loads:
        one.start()

    for one in loads[:2]:
        one.wait()

    pad_rows = jnp.zeros((PAD - here_rows, width), f32)
    tail_rows = PAD - here_rows
    for seq in range(seqs):
        values = tokens_ref[:, seq, :].astype(f32)
        scaled = values * lax.rsqrt(jnp.mean(values * values, axis=-1, keepdims=True) + epsilon)
        spread[seq] = jnp.concatenate([scaled * in_gain_ref[...], pad_rows], axis=0).astype(bf16)

    for one in loads[2:]:
        one.wait()

    block = wk_hbm.shape[0]
    strengths[z, y] = jnp.concatenate(
        [beta_ref[...].astype(f32), jnp.zeros((1, depth - block), f32)], axis=1
    )

    pl.semaphore_wait(barrier, len(friends))

    def z_copy(half, index, offset, device):
        zz = (z + offset) % hops
        one = strengths.at[zz] if half == 2 else (first_half, second_half)[half].at[zz, y]
        return copy(one, one, z_send.at[half, index], z_recv.at[half, index], device)

    def z_launch(half, index, offset, device):
        one = z_copy(half, index, offset, device)
        one.start()
        pending.append(one)

    def offset_of(index):
        return hops - index if index <= far[0] else index - far[0]

    def z_first(half):
        for d in reversed(reach):
            z_launch(half, d, 0, at(d, 0, 0))
            if d in reach_back:
                z_launch(half, far[0] + d, 0, at(hops - d, 0, 0))

    def z_arrived(half, index):
        z_copy(half, index, offset_of(index), me).wait_recv()

    def z_relay(half):
        for further in range(far[0] - REACH):
            if further == 0:
                z_arrived(half, REACH)
            index = far[0] - further
            z_launch(half, index, hops - REACH, at(index - REACH, 0, 0))
        for further in range(far[1] - REACH):
            if further == 0:
                z_arrived(half, far[0] + REACH)
            d = far[1] - further
            z_launch(half, far[0] + d, REACH, at(hops - (d - REACH), 0, 0))

    def y_copy(index, dy, offset, yy, device, back=None):
        one = first_half.at[(z + offset) % hops, yy]
        back = dy if back is None else back
        return copy(one, one, y_send.at[index, dy], y_recv.at[index, back], device)

    def y_fan(index):
        offset = offset_of(index) if index else 0
        for dy in (2, 1, 3):
            one = y_copy(index, dy, offset, y, at(0, dy, 0), seqs - dy)
            one.start()
            pending.append(one)

    def t_slot(yy, xx, cc):
        return rows_buf.at[(yy * chips + xx) * CORES + cc]

    relayed = far[0] > REACH
    tail = copy(tail_out, tail_in, h_send, h_recv, at(1, 0, 0))

    @pl.when(last)
    def _():
        ends = [spread[seq].astype(f32)[here_rows - tail_rows : here_rows] for seq in range(seqs)]
        tail_out[...] = jnp.concatenate(ends, axis=0).astype(bf16)
        tail.start()

    z_first(0)
    for dy in (2, 1, 3):
        one = strengths.at[z, y]
        launch(one, one, g_send.at[dy], g_recv.at[seqs - dy], at(0, dy, 0))
    y_fan(0)

    token_copies = [
        copy(
            spread.at[(y + dy) % seqs],
            t_slot(y, x, core),
            t_send.at[dy * chips + dx],
            t_recv.at[(seqs - dy) % seqs * chips + (chips - dx) % chips],
            at(0, dy, dx),
        )
        for dy, dx in plane
    ]
    token_copies.append(
        copy(spread.at[y], t_slot(y, x, core), c_send.at[0], c_recv.at[0], partner)
    )
    pending.extend(token_copies)

    def send_tokens():
        for one in token_copies:
            one.start()
        rows_buf[(y * chips + x) * CORES + core] = spread[y]

    @pl.when(jnp.logical_not(last))
    def _():
        send_tokens()

    full = PAD + span
    padded = seqs * group * PAD
    row, col = iota((full, padded), 0), iota((full, padded), 1)
    place, inside = col // PAD, col % PAD
    select = (row == PAD + place * here_rows + inside) & (inside < here_rows)
    select = select | ((col - row == padded - PAD) & (inside >= here_rows) & (row < PAD))
    select_buf[...] = jnp.where(select, 1.0, 0.0).astype(bf16)

    order = [2, 1, 3, 0]
    share = span // seqs
    folded = FOLD * here_rows
    batch = chips * folded
    row = iota((batch, 1), 0).astype(f32) + 0.5
    chip_of = jnp.floor(row / folded)
    fold_of = jnp.floor(row / here_rows) - FOLD * chip_of
    inside = row - 0.5 - here_rows * (FOLD * chip_of + fold_of)
    first = (CORES * here_rows * chip_of + inside).astype(jnp.int32)
    col = iota((batch, share), 1)
    for cc in range(CORES):
        owned_buf[cc] = jnp.where(col == first + cc * here_rows, 1.0, 0.0).astype(bf16)

    for dy in (1, 3, 2):
        one = strengths.at[z, (y + dy) % seqs]
        copy(one, one, g_send.at[dy], g_recv.at[dy], me).wait_recv()
    z_first(2)

    @pl.when(last)
    def _():
        tail.wait_recv()
        before = jnp.where(z > 0, tail_in[...].astype(f32), 0.0)
        for seq in range(seqs):
            rows = [
                spread[seq].astype(f32)[:here_rows],
                before[seq * tail_rows : (seq + 1) * tail_rows],
            ]
            spread[seq] = jnp.concatenate(rows, axis=0).astype(bf16)
        send_tokens()

    z_first(1)

    if relayed:
        z_relay(0)
        y_fan(REACH)
        y_fan(far[0] + REACH)
    for d in range(1, REACH if relayed else REACH + 1):
        for index in [d, far[0] + d]:
            if d <= far[index > far[0]]:
                z_arrived(0, index)
                y_fan(index)
    if relayed:
        z_relay(2)
        for d in range(REACH + 1, far[0] + 1):
            for index in [d, far[0] + d]:
                if d <= far[index > far[0]]:
                    z_arrived(0, index)
                    y_fan(index)
    for dy, dx in plane:
        index = dy * chips + dx
        slot = t_slot((y + dy) % seqs, (x + dx) % chips, core)
        copy(slot, slot, t_send.at[0], t_recv.at[index], me).wait_recv()
        launch(slot, slot, c_send.at[index], c_recv.at[index], partner)
    if relayed:
        z_relay(1)
    for d in range(1, far[0] + 1):
        for index in [d, far[0] + d]:
            if d <= far[index > far[0]] and not (relayed and d == REACH):
                z_arrived(2, index)
    for dy, dx in [(0, 0)] + plane:
        index = dy * chips + dx
        slot = t_slot((y + dy) % seqs, (x + dx) % chips, (core + 1) % CORES)
        copy(slot, slot, c_send.at[0], c_recv.at[index], me).wait_recv()
    for index in range(far[0] + far[1] + 1):
        offset = offset_of(index) if index else 0
        for dy in (1, 3, 2):
            y_copy(index, dy, offset, (y + dy) % seqs, me).wait_recv()

    def project(weights):
        pre = dot(rows_buf[...].reshape(padded, width), weights).astype(bf16)
        return dot(select_buf[...], pre)

    devices = hops * seqs
    pick = iota((width, devices), 0) // block == iota((width, devices), 1)
    column = dot(jnp.where(pick, 1.0, 0.0), strengths[...].reshape(devices, depth))
    column = jnp.where(iota((width, depth), 0) % block == iota((width, depth), 1), column, 0.0)
    column = dot(column, jnp.ones((depth, depth), f32)).astype(bf16)
    weights = first_half[...].reshape(width, 2 * depth)
    pre = project(jnp.concatenate([weights, column], axis=1))
    conv_buf[...] = pre[:, : 2 * depth]
    shift = math.log(depth / (4.0 * total_tokens))
    beta = jax.nn.sigmoid(pre[PAD:, 2 * depth :] + shift)
    width_taps = cq_ref.shape[0]

    def conv(part, taps_ref, begin):
        columns = slice(part * depth, (part + 1) * depth)
        total = jnp.zeros((size, depth), f32)
        for tap in range(width_taps):
            first = PAD + begin - (width_taps - 1) + tap
            taps = taps_ref[tap : tap + 1, :].astype(f32)
            total = total + conv_buf[first : first + size, columns] * taps
        return total * jax.nn.sigmoid(total)

    rate = rate_ref[0] / total_tokens
    row, col = iota((size, size), 0), iota((size, size), 1)
    decay = jnp.exp(-rate * jnp.maximum(row - col, 0).astype(f32))
    step = iota((size, depth), 0).astype(f32)
    kept = jnp.exp(-rate * (step + 1.0))
    rest = jnp.exp(-rate * (size - 1.0 - step))
    keys, values, betas = [], [], []
    for chunk in range(CHUNKS):
        begin = chunk * size
        keys.append(l2_normalize(conv(0, ck_ref, begin)))
        values.append(conv(1, cv_ref, begin))
        betas.append(beta[begin : begin + size])
    weighted = [k * b for k, b in zip(keys, betas)]
    lowers = [
        jnp.where(row > col, dot(w, k, NT) * decay, 0.0) for w, k in zip(weighted, keys)
    ]
    inverses = unit_inverses(lowers, row, col)
    both = [
        dot(inv, jnp.concatenate([v * b, w * kept], axis=1))
        for inv, v, b, w in zip(inverses, values, betas, weighted)
    ]
    moved = [dot(k * rest, b, TN) for k, b in zip(keys, both)]
    chunk_maps = [(m[:, :depth], m[:, depth:]) for m in moved]
    chunk_kept = jnp.exp(-rate * jnp.full((1, depth), float(size), f32))
    before, before_kept = [], []
    running, running_kept = chunk_maps[0], chunk_kept
    for chunk in range(1, CHUNKS):
        before.append(running)
        before_kept.append(running_kept)
        running = compose(running, running_kept, chunk_maps[chunk], chunk_kept)
        running_kept = running_kept * chunk_kept
    for part in range(2):
        maps[z, part] = running[part].astype(bf16)

    source = [lambda d: (z + hops - d) % hops, lambda d: (z + d) % hops]

    def m_copy(side, hop, part, offset, device):
        one = maps.at[source[side](offset), part]
        return copy(one, one, m_send.at[side, hop, part], m_recv.at[side, hop, part], device)

    def m_forward(behind):
        for step in (2, 1):
            for part in range(2):
                for side in range(2):
                    if behind + step <= far[side]:
                        device = at(step if side == 0 else hops - step, 0, 0)
                        one = m_copy(side, behind + step, part, behind, device)
                        one.start()
                        pending.append(one)

    def m_arrived(hop):
        for part in range(2):
            for side in range(2):
                if hop <= far[side]:
                    m_copy(side, hop, part, hop, me).wait_recv()

    m_forward(0)

    for d in range(1, far[0] + 1):
        for index in [d, far[0] + d]:
            if d <= far[index > far[0]] and not (relayed and d == REACH):
                z_arrived(1, index)
    for dy in (2, 1, 3):
        one = second_half.at[:, y]
        launch(one, one, q_send.at[dy], q_recv.at[seqs - dy], at(0, dy, 0))

    late_work = {}

    def project_second():
        for dy in (1, 3, 2):
            one = second_half.at[:, (y + dy) % seqs]
            copy(one, one, q_send.at[dy], q_recv.at[dy], me).wait_recv()
        pre = project(second_half[:, :, :, : 2 * depth].reshape(width, 2 * depth))
        full_out = second_half[:, :, :, 2 * depth :].reshape(FOLD, width // FOLD, depth)
        for fold in range(FOLD):
            out_weights[:, fold * depth : (fold + 1) * depth] = full_out[fold]
        conv_buf[:, : depth] = pre[:, :depth]
        gate_pre = pre[PAD:, depth:]
        gate_buf[...] = out_gain_ref[...] * gate_pre * jax.nn.sigmoid(gate_pre)

    def queries_and_scores():
        queries = [
            l2_normalize(conv(0, cq_ref, chunk * size)) * depth ** (-0.5) for chunk in range(CHUNKS)
        ]
        late_work["queries"] = queries
        late_work["scores"] = [
            jnp.where(row >= col, dot(q, k, NT) * decay, 0.0) for q, k in zip(queries, keys)
        ]

    def reads_and_locals():
        for chunk in range(CHUNKS):
            seen = dot(late_work["scores"][chunk], both[chunk])
            read = late_work["queries"][chunk] * kept - seen[:, depth:]
            local = seen[:, :depth]
            if chunk:
                value, erase = before[chunk - 1]
                shifted = dot(read, jnp.concatenate([value, erase], axis=1))
                local = local + shifted[:, :depth]
                read = before_kept[chunk - 1] * read - shifted[:, depth:]
            rows = slice(chunk * size, (chunk + 1) * size)
            reads_buf[rows, :] = read.astype(bf16)
            locals_buf[rows, :] = local

    beside = [project_second, queries_and_scores, reads_and_locals]
    stretch = running_kept
    late, late_kept, early = None, None, jnp.zeros((depth, depth), f32)
    for stage in range(2, far[0] + 2, 2):
        if stage <= far[0]:
            m_arrived(stage)
            m_forward(stage)
        for hop in (stage - 1, stage):
            if hop > far[0]:
                continue
            if hop < stage:
                m_arrived(hop)
            zz = source[0](hop)
            value = jnp.where(z >= hop, maps[zz, 0].astype(f32), 0.0)
            erase = maps[zz, 1].astype(f32)
            if late is None:
                late, late_kept = (value, erase), stretch
            else:
                late = compose((value, erase), stretch, late, late_kept)
                late_kept = late_kept * stretch
            if hop <= far[1]:
                zz = source[1](hop)
                new = stretch * early + maps[zz, 0].astype(f32) - dot(maps[zz, 1], early)
                early = jnp.where(z + hop >= hops, new, 0.0)
        if stage >= FIRST_BESIDE and beside:
            beside.pop(0)()
    for one in beside:
        one()
    state = late[0] + late_kept * early - dot(late[1], early)

    state = state.astype(bf16)

    fold_row = fold_of.astype(jnp.int32)

    def products(rows_of, cc):
        rows = dot(owned_buf[cc], rows_of)
        wide = [jnp.where(fold_row == fold, rows, 0.0).astype(bf16) for fold in range(FOLD)]
        return dot(jnp.concatenate(wide, axis=1), out_weights[...], NT).reshape(chips, folded, -1)

    gated = []
    for i, dy in enumerate(order):
        rows = pl.ds(pl.multiple_of((y + dy) % seqs * share, PAD), share)
        out = locals_buf[rows, :] + dot(reads_buf[rows, :], state)
        out = out * lax.rsqrt(jnp.mean(out * out, axis=-1, keepdims=True) + out_epsilon)
        gated.append((out * gate_buf[rows, :]).astype(bf16))
        swap_out[i] = products(gated[i], 1 - core).astype(bf16)
        launch(swap_out.at[i], swap_in.at[i], s_send.at[i], s_recv.at[i], partner)
    for i, dy in enumerate(order):
        mine = products(gated[i], core)
        copy(swap_in.at[i], swap_in.at[i], s_send.at[i], s_recv.at[i], me).wait_recv()
        parts[i] = (mine + swap_in[i].astype(f32)).astype(bf16)
        for dx in (2, 1, 3, 0) if chips == 4 else range(chips):
            if dy or dx:
                launch(
                    parts.at[i, (x + dx) % chips],
                    landed.at[y * chips + x],
                    o_send.at[dy * chips + dx],
                    o_recv.at[(seqs - dy) % seqs * chips + (chips - dx) % chips],
                    at(0, dy, dx),
                )
    landed[y * chips + x] = parts[seqs - 1, x]
    for dy, dx in plane:
        slot = landed.at[(y + dy) % seqs * chips + (x + dx) % chips]
        index = dy * chips + dx
        copy(slot, slot, o_send.at[index], o_recv.at[index], me).wait_recv()
    for seq in range(seqs):
        total = landed[seq * chips].astype(f32)
        for chip in range(1, chips):
            total = total + landed[seq * chips + chip].astype(f32)
        rows = [total[fold * here_rows : (fold + 1) * here_rows] for fold in range(FOLD)]
        out_ref[:, seq, :] = jnp.concatenate(rows, axis=1).astype(bf16)
    for one in pending:
        one.wait_send()

    @pl.when(last)
    def _():
        tail.wait_send()


def body(
    tokens,
    in_gain,
    w_query,
    w_key,
    w_value,
    w_gate,
    w_beta,
    conv_query,
    conv_key,
    conv_value,
    decay_rate,
    out_gain,
    w_out,
):
    here_rows, seqs, width = tokens.shape
    depth = w_query.shape[1]
    group, length = lax.axis_size("tp"), lax.axis_size("sp")
    hops = length // seqs
    chips = group // CORES
    owners = seqs * group
    span = owners * here_rows
    block = w_query.shape[0]
    sizes = (depth, seqs, group, hops, here_rows, width)
    anywhere = pl.BlockSpec(memory_space=pl.ANY)
    dma = pltpu.SemaphoreType.DMA
    vmem = pltpu.VMEM
    far = hops // 2 + 1
    return pl.pallas_call(
        functools.partial(mixer_kernel, sizes),
        out_shape=jax.ShapeDtypeStruct(tokens.shape, bf16),
        in_specs=[anywhere] * 10 + [pl.BlockSpec(memory_space=pltpu.SMEM)] + [anywhere] * 2,
        out_specs=pl.BlockSpec(memory_space=vmem),
        scratch_shapes=[
            vmem(tokens.shape, bf16),
            vmem((1, width), f32),
            vmem((1, block), bf16),
            vmem(conv_query.shape, bf16),
            vmem(conv_query.shape, bf16),
            vmem(conv_query.shape, bf16),
            vmem((1, depth), f32),
            vmem((hops, seqs, block, 2 * depth), bf16),
            vmem((hops, seqs, block, 3 * depth), bf16),
            vmem((hops, seqs, 1, depth), f32),
            vmem((seqs, PAD, width), bf16),
            vmem((PAD, width), bf16),
            vmem((PAD, width), bf16),
            vmem((PAD + span, owners * PAD), bf16),
            vmem((CORES, chips * FOLD * here_rows, span // seqs), bf16),
            vmem((span, depth), bf16),
            vmem((span, depth), f32),
            vmem((span, depth), f32),
            vmem((width // FOLD, FOLD * depth), bf16),
            vmem((owners, PAD, width), bf16),
            vmem((PAD + span, 2 * depth), f32),
            vmem((hops, 2, depth, depth), bf16),
            vmem((seqs, chips, FOLD * here_rows, width // FOLD), bf16),
            vmem((seqs, chips, FOLD * here_rows, width // FOLD), bf16),
            vmem((seqs, chips, FOLD * here_rows, width // FOLD), bf16),
            vmem((seqs * chips, FOLD * here_rows, width // FOLD), bf16),
            dma((12,)),
            dma((3, hops)),
            dma((3, hops)),
            dma((hops, seqs)),
            dma((hops, seqs)),
            dma((seqs,)),
            dma((seqs,)),
            dma((seqs,)),
            dma((seqs,)),
            dma((seqs * chips,)),
            dma((seqs * chips,)),
            dma((seqs * chips,)),
            dma((seqs * chips,)),
            dma,
            dma,
            dma((2, far, 2)),
            dma((2, far, 2)),
            dma((seqs,)),
            dma((seqs,)),
            dma((seqs * chips,)),
            dma((seqs * chips,)),
        ],
        compiler_params=pltpu.CompilerParams(
            collective_id=0, has_side_effects=True, vmem_limit_bytes=56 * 1024 * 1024
        ),
    )(
        tokens,
        in_gain[None],
        w_query,
        w_key,
        w_value,
        w_gate,
        w_beta.T,
        conv_query,
        conv_key,
        conv_value,
        decay_rate,
        out_gain[None],
        w_out.T,
    )


def solution(mesh):
    placed = (
        P(("sp", "tp"), None, None),
        P(),
        P("sp", "tp"),
        P("sp", "tp"),
        P("sp", "tp"),
        P("sp", "tp"),
        P("sp", "tp"),
        P(None, "tp"),
        P(None, "tp"),
        P(None, "tp"),
        P("tp"),
        P(),
        P("tp", "sp"),
    )
    return jax.shard_map(
        body, mesh=mesh, in_specs=placed, out_specs=P(("sp", "tp"), None, None), check_vma=False
    )
```

```python
import functools
import math

import jax
import jax.numpy as jnp
from jax import lax
from jax.experimental import pallas as pl
from jax.experimental.pallas import tpu as pltpu
from jax.sharding import PartitionSpec as P

MESH = pl.DeviceIdType.MESH
PAD = 16
CHUNKS = 3
CORES = 2
REACH = 4
FIRST_BESIDE = 4
FOLD = 4
epsilon = 1e-06
out_epsilon = 1e-10
f32 = jnp.float32
bf16 = jnp.bfloat16
NN, NT, TN = ((1,), (0,)), ((1,), (1,)), ((0,), (0,))


def dot(a, b, dims=NN):
    return lax.dot_general(
        a.astype(bf16), b.astype(bf16), (dims, ((), ())), preferred_element_type=f32
    )


def iota(shape, axis):
    return lax.broadcasted_iota(jnp.int32, shape, axis)


def l2_normalize(array):
    return array * lax.rsqrt(jnp.sum(array * array, axis=-1, keepdims=True) + epsilon)


def unit_inverses(lowers, row, col):
    size = row.shape[0]
    near = ((row >> 1) == (col >> 1)) & (row != col)
    eye = jnp.where(row == col, 1.0, 0.0)
    inverses = [eye - jnp.where(near, lower, 0.0) for lower in lowers]
    level = 1
    while (1 << level) < size:
        mask = ((row >> (level + 1)) == (col >> (level + 1))) & ((row >> level) != (col >> level))
        inner = [dot(jnp.where(mask, l, 0.0), v) for l, v in zip(lowers, inverses)]
        inverses = [v - dot(v, w) for v, w in zip(inverses, inner)]
        level += 1
    return inverses


def compose(first, kept_first, second, kept_second):
    depth = first[0].shape[0]
    cross = dot(second[1], jnp.concatenate(first, axis=1))
    value = kept_second * first[0] + second[0] - cross[:, :depth]
    erase = kept_second * first[1] + kept_first * second[1] - cross[:, depth:]
    return value, erase


def mixer_kernel(
    sizes,
    tokens_hbm,
    in_gain_hbm,
    wq_hbm,
    wk_hbm,
    wv_hbm,
    wg_hbm,
    wb_hbm,
    cq_hbm,
    ck_hbm,
    cv_hbm,
    rate_ref,
    out_gain_hbm,
    wo_hbm,
    out_ref,
    tokens_ref,
    in_gain_ref,
    beta_ref,
    cq_ref,
    ck_ref,
    cv_ref,
    out_gain_ref,
    first_half,
    second_half,
    strengths,
    spread,
    tail_out,
    tail_in,
    select_buf,
    owned_buf,
    reads_buf,
    locals_buf,
    gate_buf,
    out_weights,
    rows_buf,
    conv_buf,
    maps,
    swap_out,
    swap_in,
    parts,
    landed,
    load,
    z_send,
    z_recv,
    y_send,
    y_recv,
    g_send,
    g_recv,
    q_send,
    q_recv,
    t_send,
    t_recv,
    c_send,
    c_recv,
    h_send,
    h_recv,
    m_send,
    m_recv,
    s_send,
    s_recv,
    o_send,
    o_recv,
):
    depth, seqs, group, hops, here_rows, width = sizes
    chips = group // CORES
    total_tokens = hops * seqs * group * here_rows
    span = seqs * group * here_rows
    size = span // CHUNKS
    sp, tp = lax.axis_index("sp"), lax.axis_index("tp")
    z, y = sp // seqs, sp % seqs
    x, core = tp // CORES, tp % CORES
    far = [hops // 2, (hops - 1) // 2]
    last = (y == seqs - 1) & (tp == group - 1)
    pending = []

    def at(dz, dy, dx, dc=0):
        return {
            "sp": (z + dz) % hops * seqs + (y + dy) % seqs,
            "tp": (x + dx) % chips * CORES + (core + dc) % CORES,
        }

    def copy(src, dst, send, recv, device):
        return pltpu.make_async_remote_copy(
            src_ref=src,
            dst_ref=dst,
            send_sem=send,
            recv_sem=recv,
            device_id=device,
            device_id_type=MESH,
        )

    me = {"sp": sp, "tp": tp}
    partner = at(0, 0, 0, 1)

    def launch(*args):
        one = copy(*args)
        one.start()
        pending.append(one)

    barrier = pltpu.get_barrier_semaphore()
    plane = [(dy, dx) for dy in range(seqs) for dx in range(chips) if dy or dx]
    reach = [d for d in range(1, REACH + 1) if d <= far[0]]
    reach_back = [d for d in range(1, REACH + 1) if d <= far[1]]
    friends = [partner] + [at(0, dy, dx) for dy, dx in plane]
    friends += [at(d, 0, 0) for d in reach] + [at(hops - d, 0, 0) for d in reach]
    for device in friends:
        pl.semaphore_signal(barrier, inc=1, device_id=device, device_id_type=MESH)

    def own(half, part):
        return (first_half, second_half)[half].at[z, y, :, pl.ds(part * depth, depth)]

    loads = [
        (tokens_hbm, tokens_ref),
        (in_gain_hbm, in_gain_ref),
        (wk_hbm, own(0, 0)),
        (wv_hbm, own(0, 1)),
        (wb_hbm, beta_ref),
        (wq_hbm, own(1, 0)),
        (wg_hbm, own(1, 1)),
        (wo_hbm, own(1, 2)),
        (cq_hbm, cq_ref),
        (ck_hbm, ck_ref),
        (cv_hbm, cv_ref),
        (out_gain_hbm, out_gain_ref),
    ]
    loads = [pltpu.make_async_copy(a, b, load.at[i]) for i, (a, b) in enumerate(loads)]
    for one in loads:
        one.start()

    for one in loads[:2]:
        one.wait()

    pad_rows = jnp.zeros((PAD - here_rows, width), f32)
    tail_rows = PAD - here_rows
    for seq in range(seqs):
        values = tokens_ref[:, seq, :].astype(f32)
        scaled = values * lax.rsqrt(jnp.mean(values * values, axis=-1, keepdims=True) + epsilon)
        spread[seq] = jnp.concatenate([scaled * in_gain_ref[...], pad_rows], axis=0).astype(bf16)

    for one in loads[2:]:
        one.wait()

    block = wk_hbm.shape[0]
    strengths[z, y] = jnp.concatenate(
        [beta_ref[...].astype(f32), jnp.zeros((1, depth - block), f32)], axis=1
    )

    pl.semaphore_wait(barrier, len(friends))

    def z_copy(half, index, offset, device):
        zz = (z + offset) % hops
        one = strengths.at[zz] if half == 2 else (first_half, second_half)[half].at[zz, y]
        return copy(one, one, z_send.at[half, index], z_recv.at[half, index], device)

    def z_launch(half, index, offset, device):
        one = z_copy(half, index, offset, device)
        one.start()
        pending.append(one)

    def offset_of(index):
        return hops - index if index <= far[0] else index - far[0]

    def z_first(half):
        for d in reversed(reach):
            z_launch(half, d, 0, at(d, 0, 0))
            if d in reach_back:
                z_launch(half, far[0] + d, 0, at(hops - d, 0, 0))

    def z_arrived(half, index):
        z_copy(half, index, offset_of(index), me).wait_recv()

    def z_relay(half):
        for further in range(far[0] - REACH):
            if further == 0:
                z_arrived(half, REACH)
            index = far[0] - further
            z_launch(half, index, hops - REACH, at(index - REACH, 0, 0))
        for further in range(far[1] - REACH):
            if further == 0:
                z_arrived(half, far[0] + REACH)
            d = far[1] - further
            z_launch(half, far[0] + d, REACH, at(hops - (d - REACH), 0, 0))

    def y_copy(index, dy, offset, yy, device, back=None):
        one = first_half.at[(z + offset) % hops, yy]
        back = dy if back is None else back
        return copy(one, one, y_send.at[index, dy], y_recv.at[index, back], device)

    def y_fan(index):
        offset = offset_of(index) if index else 0
        for dy in (2, 1, 3):
            one = y_copy(index, dy, offset, y, at(0, dy, 0), seqs - dy)
            one.start()
            pending.append(one)

    def t_slot(yy, xx, cc):
        return rows_buf.at[(yy * chips + xx) * CORES + cc]

    relayed = far[0] > REACH
    tail = copy(tail_out, tail_in, h_send, h_recv, at(1, 0, 0))

    @pl.when(last)
    def _():
        ends = [spread[seq].astype(f32)[here_rows - tail_rows : here_rows] for seq in range(seqs)]
        tail_out[...] = jnp.concatenate(ends, axis=0).astype(bf16)
        tail.start()

    z_first(0)
    for dy in (2, 1, 3):
        one = strengths.at[z, y]
        launch(one, one, g_send.at[dy], g_recv.at[seqs - dy], at(0, dy, 0))
    y_fan(0)

    token_copies = [
        copy(
            spread.at[(y + dy) % seqs],
            t_slot(y, x, core),
            t_send.at[dy * chips + dx],
            t_recv.at[(seqs - dy) % seqs * chips + (chips - dx) % chips],
            at(0, dy, dx),
        )
        for dy, dx in plane
    ]
    token_copies.append(
        copy(spread.at[y], t_slot(y, x, core), c_send.at[0], c_recv.at[0], partner)
    )
    pending.extend(token_copies)

    def send_tokens():
        for one in token_copies:
            one.start()
        rows_buf[(y * chips + x) * CORES + core] = spread[y]

    @pl.when(jnp.logical_not(last))
    def _():
        send_tokens()

    full = PAD + span
    padded = seqs * group * PAD
    row, col = iota((full, padded), 0), iota((full, padded), 1)
    place, inside = col // PAD, col % PAD
    select = (row == PAD + place * here_rows + inside) & (inside < here_rows)
    select = select | ((col - row == padded - PAD) & (inside >= here_rows) & (row < PAD))
    select_buf[...] = jnp.where(select, 1.0, 0.0).astype(bf16)

    order = [2, 1, 3, 0]
    share = span // seqs
    folded = FOLD * here_rows
    batch = chips * folded
    row = iota((batch, 1), 0).astype(f32) + 0.5
    chip_of = jnp.floor(row / folded)
    fold_of = jnp.floor(row / here_rows) - FOLD * chip_of
    inside = row - 0.5 - here_rows * (FOLD * chip_of + fold_of)
    first = (CORES * here_rows * chip_of + inside).astype(jnp.int32)
    col = iota((batch, share), 1)
    for cc in range(CORES):
        owned_buf[cc] = jnp.where(col == first + cc * here_rows, 1.0, 0.0).astype(bf16)

    for dy in (1, 3, 2):
        one = strengths.at[z, (y + dy) % seqs]
        copy(one, one, g_send.at[dy], g_recv.at[dy], me).wait_recv()
    z_first(2)

    @pl.when(last)
    def _():
        tail.wait_recv()
        before = jnp.where(z > 0, tail_in[...].astype(f32), 0.0)
        for seq in range(seqs):
            rows = [
                spread[seq].astype(f32)[:here_rows],
                before[seq * tail_rows : (seq + 1) * tail_rows],
            ]
            spread[seq] = jnp.concatenate(rows, axis=0).astype(bf16)
        send_tokens()

    z_first(1)

    if relayed:
        z_relay(0)
        y_fan(REACH)
        y_fan(far[0] + REACH)
    for d in range(1, REACH if relayed else REACH + 1):
        for index in [d, far[0] + d]:
            if d <= far[index > far[0]]:
                z_arrived(0, index)
                y_fan(index)
    if relayed:
        z_relay(2)
        for d in range(REACH + 1, far[0] + 1):
            for index in [d, far[0] + d]:
                if d <= far[index > far[0]]:
                    z_arrived(0, index)
                    y_fan(index)
    for dy, dx in plane:
        index = dy * chips + dx
        slot = t_slot((y + dy) % seqs, (x + dx) % chips, core)
        copy(slot, slot, t_send.at[0], t_recv.at[index], me).wait_recv()
        launch(slot, slot, c_send.at[index], c_recv.at[index], partner)
    if relayed:
        z_relay(1)
    for d in range(1, far[0] + 1):
        for index in [d, far[0] + d]:
            if d <= far[index > far[0]] and not (relayed and d == REACH):
                z_arrived(2, index)
    for dy, dx in [(0, 0)] + plane:
        index = dy * chips + dx
        slot = t_slot((y + dy) % seqs, (x + dx) % chips, (core + 1) % CORES)
        copy(slot, slot, c_send.at[0], c_recv.at[index], me).wait_recv()
    for index in range(far[0] + far[1] + 1):
        offset = offset_of(index) if index else 0
        for dy in (1, 3, 2):
            y_copy(index, dy, offset, (y + dy) % seqs, me).wait_recv()

    def project(weights):
        pre = dot(rows_buf[...].reshape(padded, width), weights).astype(bf16)
        return dot(select_buf[...], pre)

    devices = hops * seqs
    pick = iota((width, devices), 0) // block == iota((width, devices), 1)
    column = dot(jnp.where(pick, 1.0, 0.0), strengths[...].reshape(devices, depth))
    column = jnp.where(iota((width, depth), 0) % block == iota((width, depth), 1), column, 0.0)
    column = dot(column, jnp.ones((depth, depth), f32)).astype(bf16)
    weights = first_half[...].reshape(width, 2 * depth)
    pre = project(jnp.concatenate([weights, column], axis=1))
    conv_buf[...] = pre[:, : 2 * depth]
    shift = math.log(depth / (4.0 * total_tokens))
    beta = jax.nn.sigmoid(pre[PAD:, 2 * depth :] + shift)
    width_taps = cq_ref.shape[0]

    def conv(part, taps_ref, begin):
        columns = slice(part * depth, (part + 1) * depth)
        total = jnp.zeros((size, depth), f32)
        for tap in range(width_taps):
            first = PAD + begin - (width_taps - 1) + tap
            taps = taps_ref[tap : tap + 1, :].astype(f32)
            total = total + conv_buf[first : first + size, columns] * taps
        return total * jax.nn.sigmoid(total)

    rate = rate_ref[0] / total_tokens
    row, col = iota((size, size), 0), iota((size, size), 1)
    decay = jnp.exp(-rate * jnp.maximum(row - col, 0).astype(f32))
    step = iota((size, depth), 0).astype(f32)
    kept = jnp.exp(-rate * (step + 1.0))
    rest = jnp.exp(-rate * (size - 1.0 - step))
    keys, values, betas = [], [], []
    for chunk in range(CHUNKS):
        begin = chunk * size
        keys.append(l2_normalize(conv(0, ck_ref, begin)))
        values.append(conv(1, cv_ref, begin))
        betas.append(beta[begin : begin + size])
    weighted = [k * b for k, b in zip(keys, betas)]
    lowers = [
        jnp.where(row > col, dot(w, k, NT) * decay, 0.0) for w, k in zip(weighted, keys)
    ]
    inverses = unit_inverses(lowers, row, col)
    both = [
        dot(inv, jnp.concatenate([v * b, w * kept], axis=1))
        for inv, v, b, w in zip(inverses, values, betas, weighted)
    ]
    moved = [dot(k * rest, b, TN) for k, b in zip(keys, both)]
    chunk_maps = [(m[:, :depth], m[:, depth:]) for m in moved]
    chunk_kept = jnp.exp(-rate * jnp.full((1, depth), float(size), f32))
    before, before_kept = [], []
    running, running_kept = chunk_maps[0], chunk_kept
    for chunk in range(1, CHUNKS):
        before.append(running)
        before_kept.append(running_kept)
        running = compose(running, running_kept, chunk_maps[chunk], chunk_kept)
        running_kept = running_kept * chunk_kept
    for part in range(2):
        maps[z, part] = running[part].astype(bf16)

    source = [lambda d: (z + hops - d) % hops, lambda d: (z + d) % hops]

    def m_copy(side, hop, part, offset, device):
        one = maps.at[source[side](offset), part]
        return copy(one, one, m_send.at[side, hop, part], m_recv.at[side, hop, part], device)

    guarded = []

    def useful(side, behind, step):
        if side == 0:
            return (z >= behind) & (z + step < hops)
        first = (z + behind) % hops
        if step == 2:
            return first < far[1]
        return (first < far[1]) & (first < behind + step)

    def m_forward(behind):
        for step in (2, 1):
            for side in range(2):
                if behind + step <= far[side]:
                    device = at(step if side == 0 else hops - step, 0, 0)
                    both_parts = [
                        m_copy(side, behind + step, part, behind, device) for part in range(2)
                    ]
                    needed = useful(side, behind, step)
                    guarded.append((needed, both_parts))

                    @pl.when(needed)
                    def _():
                        for one in both_parts:
                            one.start()

    def m_arrived(hop):
        for side in range(2):
            if hop <= far[side]:
                first = (z + hop) % hops
                needed = z >= hop
                if side == 1:
                    needed = first < far[1]
                    if hop % 2:
                        needed = needed & (first < hop)

                @pl.when(needed)
                def _():
                    for part in range(2):
                        m_copy(side, hop, part, hop, me).wait_recv()

    m_forward(0)

    for d in range(1, far[0] + 1):
        for index in [d, far[0] + d]:
            if d <= far[index > far[0]] and not (relayed and d == REACH):
                z_arrived(1, index)
    for dy in (2, 1, 3):
        one = second_half.at[:, y]
        launch(one, one, q_send.at[dy], q_recv.at[seqs - dy], at(0, dy, 0))

    late_work = {}

    def project_second():
        for dy in (1, 3, 2):
            one = second_half.at[:, (y + dy) % seqs]
            copy(one, one, q_send.at[dy], q_recv.at[dy], me).wait_recv()
        pre = project(second_half[:, :, :, : 2 * depth].reshape(width, 2 * depth))
        full_out = second_half[:, :, :, 2 * depth :].reshape(FOLD, width // FOLD, depth)
        for fold in range(FOLD):
            out_weights[:, fold * depth : (fold + 1) * depth] = full_out[fold]
        conv_buf[:, : depth] = pre[:, :depth]
        gate_pre = pre[PAD:, depth:]
        gate_buf[...] = out_gain_ref[...] * gate_pre * jax.nn.sigmoid(gate_pre)

    def queries_and_scores():
        queries = [
            l2_normalize(conv(0, cq_ref, chunk * size)) * depth ** (-0.5) for chunk in range(CHUNKS)
        ]
        late_work["queries"] = queries
        late_work["scores"] = [
            jnp.where(row >= col, dot(q, k, NT) * decay, 0.0) for q, k in zip(queries, keys)
        ]

    def reads_and_locals():
        for chunk in range(CHUNKS):
            seen = dot(late_work["scores"][chunk], both[chunk])
            read = late_work["queries"][chunk] * kept - seen[:, depth:]
            local = seen[:, :depth]
            if chunk:
                value, erase = before[chunk - 1]
                shifted = dot(read, jnp.concatenate([value, erase], axis=1))
                local = local + shifted[:, :depth]
                read = before_kept[chunk - 1] * read - shifted[:, depth:]
            rows = slice(chunk * size, (chunk + 1) * size)
            reads_buf[rows, :] = read.astype(bf16)
            locals_buf[rows, :] = local

    beside = [project_second, queries_and_scores, reads_and_locals]
    stretch = running_kept
    late, late_kept, early = None, None, jnp.zeros((depth, depth), f32)
    for stage in range(2, far[0] + 2, 2):
        if stage <= far[0]:
            m_arrived(stage)
            m_forward(stage)
        for hop in (stage - 1, stage):
            if hop > far[0]:
                continue
            if hop < stage:
                m_arrived(hop)
            zz = source[0](hop)
            value = jnp.where(z >= hop, maps[zz, 0].astype(f32), 0.0)
            erase = jnp.where(z >= hop, maps[zz, 1].astype(f32), 0.0)
            if late is None:
                late, late_kept = (value, erase), stretch
            else:
                late = compose((value, erase), stretch, late, late_kept)
                late_kept = late_kept * stretch
            if hop <= far[1]:
                zz = source[1](hop)
                new = stretch * early + maps[zz, 0].astype(f32) - dot(maps[zz, 1], early)
                early = jnp.where(z + hop >= hops, new, 0.0)
        if stage >= FIRST_BESIDE and beside:
            beside.pop(0)()
    for one in beside:
        one()
    state = late[0] + late_kept * early - dot(late[1], early)

    state = state.astype(bf16)

    fold_row = fold_of.astype(jnp.int32)

    def products(rows_of, cc):
        rows = dot(owned_buf[cc], rows_of)
        wide = [jnp.where(fold_row == fold, rows, 0.0).astype(bf16) for fold in range(FOLD)]
        return dot(jnp.concatenate(wide, axis=1), out_weights[...], NT).reshape(chips, folded, -1)

    gated = []
    for i, dy in enumerate(order):
        rows = pl.ds(pl.multiple_of((y + dy) % seqs * share, PAD), share)
        out = locals_buf[rows, :] + dot(reads_buf[rows, :], state)
        out = out * lax.rsqrt(jnp.mean(out * out, axis=-1, keepdims=True) + out_epsilon)
        gated.append((out * gate_buf[rows, :]).astype(bf16))
        swap_out[i] = products(gated[i], 1 - core).astype(bf16)
        launch(swap_out.at[i], swap_in.at[i], s_send.at[i], s_recv.at[i], partner)
    for i, dy in enumerate(order):
        mine = products(gated[i], core)
        copy(swap_in.at[i], swap_in.at[i], s_send.at[i], s_recv.at[i], me).wait_recv()
        parts[i] = (mine + swap_in[i].astype(f32)).astype(bf16)
        for dx in (2, 1, 3, 0) if chips == 4 else range(chips):
            if dy or dx:
                launch(
                    parts.at[i, (x + dx) % chips],
                    landed.at[y * chips + x],
                    o_send.at[dy * chips + dx],
                    o_recv.at[(seqs - dy) % seqs * chips + (chips - dx) % chips],
                    at(0, dy, dx),
                )
    landed[y * chips + x] = parts[seqs - 1, x]
    for dy, dx in plane:
        slot = landed.at[(y + dy) % seqs * chips + (x + dx) % chips]
        index = dy * chips + dx
        copy(slot, slot, o_send.at[index], o_recv.at[index], me).wait_recv()
    for seq in range(seqs):
        total = landed[seq * chips].astype(f32)
        for chip in range(1, chips):
            total = total + landed[seq * chips + chip].astype(f32)
        rows = [total[fold * here_rows : (fold + 1) * here_rows] for fold in range(FOLD)]
        out_ref[:, seq, :] = jnp.concatenate(rows, axis=1).astype(bf16)
    for one in pending:
        one.wait_send()

    for needed, both_parts in guarded:

        @pl.when(needed)
        def _():
            for one in both_parts:
                one.wait_send()

    @pl.when(last)
    def _():
        tail.wait_send()


def body(
    tokens,
    in_gain,
    w_query,
    w_key,
    w_value,
    w_gate,
    w_beta,
    conv_query,
    conv_key,
    conv_value,
    decay_rate,
    out_gain,
    w_out,
):
    here_rows, seqs, width = tokens.shape
    depth = w_query.shape[1]
    group, length = lax.axis_size("tp"), lax.axis_size("sp")
    hops = length // seqs
    chips = group // CORES
    owners = seqs * group
    span = owners * here_rows
    block = w_query.shape[0]
    sizes = (depth, seqs, group, hops, here_rows, width)
    anywhere = pl.BlockSpec(memory_space=pl.ANY)
    dma = pltpu.SemaphoreType.DMA
    vmem = pltpu.VMEM
    far = hops // 2 + 1
    return pl.pallas_call(
        functools.partial(mixer_kernel, sizes),
        out_shape=jax.ShapeDtypeStruct(tokens.shape, bf16),
        in_specs=[anywhere] * 10 + [pl.BlockSpec(memory_space=pltpu.SMEM)] + [anywhere] * 2,
        out_specs=pl.BlockSpec(memory_space=vmem),
        scratch_shapes=[
            vmem(tokens.shape, bf16),
            vmem((1, width), f32),
            vmem((1, block), bf16),
            vmem(conv_query.shape, bf16),
            vmem(conv_query.shape, bf16),
            vmem(conv_query.shape, bf16),
            vmem((1, depth), f32),
            vmem((hops, seqs, block, 2 * depth), bf16),
            vmem((hops, seqs, block, 3 * depth), bf16),
            vmem((hops, seqs, 1, depth), f32),
            vmem((seqs, PAD, width), bf16),
            vmem((PAD, width), bf16),
            vmem((PAD, width), bf16),
            vmem((PAD + span, owners * PAD), bf16),
            vmem((CORES, chips * FOLD * here_rows, span // seqs), bf16),
            vmem((span, depth), bf16),
            vmem((span, depth), f32),
            vmem((span, depth), f32),
            vmem((width // FOLD, FOLD * depth), bf16),
            vmem((owners, PAD, width), bf16),
            vmem((PAD + span, 2 * depth), f32),
            vmem((hops, 2, depth, depth), bf16),
            vmem((seqs, chips, FOLD * here_rows, width // FOLD), bf16),
            vmem((seqs, chips, FOLD * here_rows, width // FOLD), bf16),
            vmem((seqs, chips, FOLD * here_rows, width // FOLD), bf16),
            vmem((seqs * chips, FOLD * here_rows, width // FOLD), bf16),
            dma((12,)),
            dma((3, hops)),
            dma((3, hops)),
            dma((hops, seqs)),
            dma((hops, seqs)),
            dma((seqs,)),
            dma((seqs,)),
            dma((seqs,)),
            dma((seqs,)),
            dma((seqs * chips,)),
            dma((seqs * chips,)),
            dma((seqs * chips,)),
            dma((seqs * chips,)),
            dma,
            dma,
            dma((2, far, 2)),
            dma((2, far, 2)),
            dma((seqs,)),
            dma((seqs,)),
            dma((seqs * chips,)),
            dma((seqs * chips,)),
        ],
        compiler_params=pltpu.CompilerParams(
            collective_id=0, has_side_effects=True, vmem_limit_bytes=56 * 1024 * 1024
        ),
    )(
        tokens,
        in_gain[None],
        w_query,
        w_key,
        w_value,
        w_gate,
        w_beta.T,
        conv_query,
        conv_key,
        conv_value,
        decay_rate,
        out_gain[None],
        w_out.T,
    )


def solution(mesh):
    placed = (
        P(("sp", "tp"), None, None),
        P(),
        P("sp", "tp"),
        P("sp", "tp"),
        P("sp", "tp"),
        P("sp", "tp"),
        P("sp", "tp"),
        P(None, "tp"),
        P(None, "tp"),
        P(None, "tp"),
        P("tp"),
        P(),
        P("tp", "sp"),
    )
    return jax.shard_map(
        body, mesh=mesh, in_specs=placed, out_specs=P(("sp", "tp"), None, None), check_vma=False
    )
```

```python
import functools
import math

import jax
import jax.numpy as jnp
from jax import lax
from jax.experimental import pallas as pl
from jax.experimental.pallas import tpu as pltpu
from jax.sharding import PartitionSpec as P

MESH = pl.DeviceIdType.MESH
PAD = 16
CHUNKS = 3
CORES = 2
REACH = 4
FIRST_BESIDE = 4
FOLD = 4
PIECES = 2
epsilon = 1e-06
out_epsilon = 1e-10
f32 = jnp.float32
bf16 = jnp.bfloat16
NN, NT, TN = ((1,), (0,)), ((1,), (1,)), ((0,), (0,))


def dot(a, b, dims=NN):
    return lax.dot_general(
        a.astype(bf16), b.astype(bf16), (dims, ((), ())), preferred_element_type=f32
    )


def iota(shape, axis):
    return lax.broadcasted_iota(jnp.int32, shape, axis)


def l2_normalize(array):
    return array * lax.rsqrt(jnp.sum(array * array, axis=-1, keepdims=True) + epsilon)


def unit_inverses(lowers, row, col):
    size = row.shape[0]
    near = ((row >> 1) == (col >> 1)) & (row != col)
    eye = jnp.where(row == col, 1.0, 0.0)
    inverses = [eye - jnp.where(near, lower, 0.0) for lower in lowers]
    level = 1
    while (1 << level) < size:
        mask = ((row >> (level + 1)) == (col >> (level + 1))) & ((row >> level) != (col >> level))
        inner = [dot(jnp.where(mask, l, 0.0), v) for l, v in zip(lowers, inverses)]
        inverses = [v - dot(v, w) for v, w in zip(inverses, inner)]
        level += 1
    return inverses


def compose(first, kept_first, second, kept_second):
    depth = first[0].shape[0]
    cross = dot(second[1], jnp.concatenate(first, axis=1))
    value = kept_second * first[0] + second[0] - cross[:, :depth]
    erase = kept_second * first[1] + kept_first * second[1] - cross[:, depth:]
    return value, erase


def mixer_kernel(
    sizes,
    tokens_hbm,
    in_gain_hbm,
    wq_hbm,
    wk_hbm,
    wv_hbm,
    wg_hbm,
    wb_hbm,
    cq_hbm,
    ck_hbm,
    cv_hbm,
    rate_ref,
    out_gain_hbm,
    wo_hbm,
    out_ref,
    tokens_ref,
    in_gain_ref,
    beta_ref,
    cq_ref,
    ck_ref,
    cv_ref,
    out_gain_ref,
    first_half,
    second_half,
    strengths,
    spread,
    tail_out,
    tail_in,
    select_buf,
    owned_buf,
    reads_buf,
    locals_buf,
    gate_buf,
    column_buf,
    beta_buf,
    out_weights,
    rows_buf,
    conv_buf,
    maps,
    swap_out,
    swap_in,
    parts,
    landed,
    load,
    z_send,
    z_recv,
    y_send,
    y_recv,
    g_send,
    g_recv,
    q_send,
    q_recv,
    t_send,
    t_recv,
    c_send,
    c_recv,
    h_send,
    h_recv,
    m_send,
    m_recv,
    s_send,
    s_recv,
    o_send,
    o_recv,
):
    depth, seqs, group, hops, here_rows, width = sizes
    chips = group // CORES
    total_tokens = hops * seqs * group * here_rows
    span = seqs * group * here_rows
    size = span // CHUNKS
    sp, tp = lax.axis_index("sp"), lax.axis_index("tp")
    z, y = sp // seqs, sp % seqs
    x, core = tp // CORES, tp % CORES
    far = [hops // 2, (hops - 1) // 2]
    last = (y == seqs - 1) & (tp == group - 1)
    pending = []

    def at(dz, dy, dx, dc=0):
        return {
            "sp": (z + dz) % hops * seqs + (y + dy) % seqs,
            "tp": (x + dx) % chips * CORES + (core + dc) % CORES,
        }

    def copy(src, dst, send, recv, device):
        return pltpu.make_async_remote_copy(
            src_ref=src,
            dst_ref=dst,
            send_sem=send,
            recv_sem=recv,
            device_id=device,
            device_id_type=MESH,
        )

    me = {"sp": sp, "tp": tp}
    partner = at(0, 0, 0, 1)

    def launch(*args):
        one = copy(*args)
        one.start()
        pending.append(one)

    barrier = pltpu.get_barrier_semaphore()
    plane = [(dy, dx) for dy in range(seqs) for dx in range(chips) if dy or dx]
    reach = [d for d in range(1, REACH + 1) if d <= far[0]]
    reach_back = [d for d in range(1, REACH + 1) if d <= far[1]]
    friends = [partner] + [at(0, dy, dx) for dy, dx in plane]
    friends += [at(d, 0, 0) for d in reach] + [at(hops - d, 0, 0) for d in reach]
    for device in friends:
        pl.semaphore_signal(barrier, inc=1, device_id=device, device_id_type=MESH)

    def own(half, part):
        return (first_half, second_half)[half].at[z, y, :, pl.ds(part * depth, depth)]

    loads = [
        (tokens_hbm, tokens_ref),
        (in_gain_hbm, in_gain_ref),
        (wk_hbm, own(0, 0)),
        (wv_hbm, own(0, 1)),
        (wb_hbm, beta_ref),
        (wq_hbm, own(1, 0)),
        (wg_hbm, own(1, 1)),
        (wo_hbm, own(1, 2)),
        (cq_hbm, cq_ref),
        (ck_hbm, ck_ref),
        (cv_hbm, cv_ref),
        (out_gain_hbm, out_gain_ref),
    ]
    loads = [pltpu.make_async_copy(a, b, load.at[i]) for i, (a, b) in enumerate(loads)]
    for one in loads:
        one.start()

    for one in loads[:2]:
        one.wait()

    pad_rows = jnp.zeros((PAD - here_rows, width), f32)
    tail_rows = PAD - here_rows
    for seq in range(seqs):
        values = tokens_ref[:, seq, :].astype(f32)
        scaled = values * lax.rsqrt(jnp.mean(values * values, axis=-1, keepdims=True) + epsilon)
        spread[seq] = jnp.concatenate([scaled * in_gain_ref[...], pad_rows], axis=0).astype(bf16)

    for one in loads[2:]:
        one.wait()

    block = wk_hbm.shape[0]
    strengths[z, y] = jnp.concatenate(
        [beta_ref[...].astype(f32), jnp.zeros((1, depth - block), f32)], axis=1
    )

    pl.semaphore_wait(barrier, len(friends))

    def z_copy(half, index, offset, device):
        zz = (z + offset) % hops
        one = strengths.at[zz] if half == 2 else (first_half, second_half)[half].at[zz, y]
        return copy(one, one, z_send.at[half, index], z_recv.at[half, index], device)

    def z_launch(half, index, offset, device):
        one = z_copy(half, index, offset, device)
        one.start()
        pending.append(one)

    def offset_of(index):
        return hops - index if index <= far[0] else index - far[0]

    def z_first(half):
        for d in reversed(reach):
            z_launch(half, d, 0, at(d, 0, 0))
            if d in reach_back:
                z_launch(half, far[0] + d, 0, at(hops - d, 0, 0))

    def z_arrived(half, index):
        z_copy(half, index, offset_of(index), me).wait_recv()

    def z_relay(half):
        for further in range(far[0] - REACH):
            if further == 0:
                z_arrived(half, REACH)
            index = far[0] - further
            z_launch(half, index, hops - REACH, at(index - REACH, 0, 0))
        for further in range(far[1] - REACH):
            if further == 0:
                z_arrived(half, far[0] + REACH)
            d = far[1] - further
            z_launch(half, far[0] + d, REACH, at(hops - (d - REACH), 0, 0))

    def y_copy(index, dy, offset, yy, device, back=None):
        one = first_half.at[(z + offset) % hops, yy]
        back = dy if back is None else back
        return copy(one, one, y_send.at[index, dy], y_recv.at[index, back], device)

    def y_fan(index):
        offset = offset_of(index) if index else 0
        for dy in (2, 1, 3):
            one = y_copy(index, dy, offset, y, at(0, dy, 0), seqs - dy)
            one.start()
            pending.append(one)

    def t_slot(yy, xx, cc):
        return rows_buf.at[(yy * chips + xx) * CORES + cc]

    relayed = far[0] > REACH
    tail = copy(tail_out, tail_in, h_send, h_recv, at(1, 0, 0))

    @pl.when(last)
    def _():
        ends = [spread[seq].astype(f32)[here_rows - tail_rows : here_rows] for seq in range(seqs)]
        tail_out[...] = jnp.concatenate(ends, axis=0).astype(bf16)
        tail.start()

    z_first(0)
    for dy in (2, 1, 3):
        one = strengths.at[z, y]
        launch(one, one, g_send.at[dy], g_recv.at[seqs - dy], at(0, dy, 0))
    y_fan(0)

    token_copies = [
        copy(
            spread.at[(y + dy) % seqs],
            t_slot(y, x, core),
            t_send.at[dy * chips + dx],
            t_recv.at[(seqs - dy) % seqs * chips + (chips - dx) % chips],
            at(0, dy, dx),
        )
        for dy, dx in plane
    ]
    token_copies.append(
        copy(spread.at[y], t_slot(y, x, core), c_send.at[0], c_recv.at[0], partner)
    )
    pending.extend(token_copies)

    def send_tokens():
        for one in token_copies:
            one.start()
        rows_buf[(y * chips + x) * CORES + core] = spread[y]

    @pl.when(jnp.logical_not(last))
    def _():
        send_tokens()

    full = PAD + span
    padded = seqs * group * PAD
    row, col = iota((full, padded), 0), iota((full, padded), 1)
    place, inside = col // PAD, col % PAD
    select = (row == PAD + place * here_rows + inside) & (inside < here_rows)
    select = select | ((col - row == padded - PAD) & (inside >= here_rows) & (row < PAD))
    select_buf[...] = jnp.where(select, 1.0, 0.0).astype(bf16)

    order = [2, 1, 3, 0]
    share = span // seqs
    folded = FOLD * here_rows
    batch = chips * folded
    row = iota((batch, 1), 0).astype(f32) + 0.5
    chip_of = jnp.floor(row / folded)
    fold_of = jnp.floor(row / here_rows) - FOLD * chip_of
    inside = row - 0.5 - here_rows * (FOLD * chip_of + fold_of)
    first = (CORES * here_rows * chip_of + inside).astype(jnp.int32)
    col = iota((batch, share), 1)
    for cc in range(CORES):
        owned_buf[cc] = jnp.where(col == first + cc * here_rows, 1.0, 0.0).astype(bf16)

    for dy in (1, 3, 2):
        one = strengths.at[z, (y + dy) % seqs]
        copy(one, one, g_send.at[dy], g_recv.at[dy], me).wait_recv()
    z_first(2)

    @pl.when(last)
    def _():
        tail.wait_recv()
        before = jnp.where(z > 0, tail_in[...].astype(f32), 0.0)
        for seq in range(seqs):
            rows = [
                spread[seq].astype(f32)[:here_rows],
                before[seq * tail_rows : (seq + 1) * tail_rows],
            ]
            spread[seq] = jnp.concatenate(rows, axis=0).astype(bf16)
        send_tokens()

    z_first(1)

    if relayed:
        z_relay(0)
        y_fan(REACH)
        y_fan(far[0] + REACH)
    for d in range(1, REACH if relayed else REACH + 1):
        for index in [d, far[0] + d]:
            if d <= far[index > far[0]]:
                z_arrived(0, index)
                y_fan(index)
    if relayed:
        z_relay(2)
        for d in range(REACH + 1, far[0] + 1):
            for index in [d, far[0] + d]:
                if d <= far[index > far[0]]:
                    z_arrived(0, index)
                    y_fan(index)
    for dy, dx in plane:
        index = dy * chips + dx
        slot = t_slot((y + dy) % seqs, (x + dx) % chips, core)
        copy(slot, slot, t_send.at[0], t_recv.at[index], me).wait_recv()
        launch(slot, slot, c_send.at[index], c_recv.at[index], partner)
    if relayed:
        z_relay(1)
    for d in range(1, far[0] + 1):
        for index in [d, far[0] + d]:
            if d <= far[index > far[0]] and not (relayed and d == REACH):
                z_arrived(2, index)
    devices = hops * seqs
    pick = iota((width, devices), 0) // block == iota((width, devices), 1)
    column = dot(jnp.where(pick, 1.0, 0.0), strengths[...].reshape(devices, depth))
    column = jnp.where(iota((width, depth), 0) % block == iota((width, depth), 1), column, 0.0)
    column_buf[...] = dot(column, jnp.ones((depth, depth), f32)).astype(bf16)

    for dy, dx in [(0, 0)] + plane:
        index = dy * chips + dx
        slot = t_slot((y + dy) % seqs, (x + dx) % chips, (core + 1) % CORES)
        copy(slot, slot, c_send.at[0], c_recv.at[index], me).wait_recv()
    def project(weights):
        pre = dot(rows_buf[...].reshape(padded, width), weights).astype(bf16)
        return dot(select_buf[...], pre)

    shift = math.log(depth / (4.0 * total_tokens))
    beta_buf[...] = jax.nn.sigmoid(project(column_buf[...])[PAD:] + shift)

    for index in range(far[0] + far[1] + 1):
        offset = offset_of(index) if index else 0
        for dy in (1, 3, 2):
            y_copy(index, dy, offset, (y + dy) % seqs, me).wait_recv()

    pre = project(first_half[...].reshape(width, 2 * depth))
    conv_buf[...] = pre
    width_taps = cq_ref.shape[0]

    def conv(part, taps_ref, begin):
        columns = slice(part * depth, (part + 1) * depth)
        total = jnp.zeros((size, depth), f32)
        for tap in range(width_taps):
            first = PAD + begin - (width_taps - 1) + tap
            taps = taps_ref[tap : tap + 1, :].astype(f32)
            total = total + conv_buf[first : first + size, columns] * taps
        return total * jax.nn.sigmoid(total)

    rate = rate_ref[0] / total_tokens
    row, col = iota((size, size), 0), iota((size, size), 1)
    decay = jnp.exp(-rate * jnp.maximum(row - col, 0).astype(f32))
    step = iota((size, depth), 0).astype(f32)
    kept = jnp.exp(-rate * (step + 1.0))
    rest = jnp.exp(-rate * (size - 1.0 - step))
    keys, values, betas = [], [], []
    for chunk in range(CHUNKS):
        begin = chunk * size
        keys.append(l2_normalize(conv(0, ck_ref, begin)))
        values.append(conv(1, cv_ref, begin))
        betas.append(beta_buf[begin : begin + size, :])
    weighted = [k * b for k, b in zip(keys, betas)]
    lowers = [
        jnp.where(row > col, dot(w, k, NT) * decay, 0.0) for w, k in zip(weighted, keys)
    ]
    inverses = unit_inverses(lowers, row, col)
    both = [
        dot(inv, jnp.concatenate([v * b, w * kept], axis=1))
        for inv, v, b, w in zip(inverses, values, betas, weighted)
    ]
    moved = [dot(k * rest, b, TN) for k, b in zip(keys, both)]
    chunk_maps = [(m[:, :depth], m[:, depth:]) for m in moved]
    chunk_kept = jnp.exp(-rate * jnp.full((1, depth), float(size), f32))
    before, before_kept = [], []
    running, running_kept = chunk_maps[0], chunk_kept
    for chunk in range(1, CHUNKS):
        before.append(running)
        before_kept.append(running_kept)
        running = compose(running, running_kept, chunk_maps[chunk], chunk_kept)
        running_kept = running_kept * chunk_kept
    for part in range(2):
        maps[z, part] = running[part].astype(bf16)

    source = [lambda d: (z + hops - d) % hops, lambda d: (z + d) % hops]

    def m_copy(side, hop, piece, offset, device):
        rows = depth * 2 // PIECES
        part, begin = piece * rows // depth, piece * rows % depth
        one = maps.at[source[side](offset), part, pl.ds(begin, rows)]
        return copy(one, one, m_send.at[side, hop, piece], m_recv.at[side, hop, piece], device)

    guarded = []

    def useful(side, behind, step):
        if side == 0:
            return (z >= behind) & (z + step < hops)
        first = (z + behind) % hops
        if step == 2:
            return first < far[1]
        return (first < far[1]) & (first < behind + step)

    def m_forward(side, behind, step, piece):
        if behind + step <= far[side]:
            device = at(step if side == 0 else hops - step, 0, 0)
            one = m_copy(side, behind + step, piece, behind, device)
            needed = useful(side, behind, step)
            guarded.append((needed, one))
            pl.when(needed)(one.start)

    def m_arrived(side, hop, piece):
        if hop <= far[side]:
            first = (z + hop) % hops
            needed = z >= hop
            if side == 1:
                needed = first < far[1]
                if hop % 2:
                    needed = needed & (first < hop)
            pl.when(needed)(m_copy(side, hop, piece, hop, me).wait_recv)

    def m_stage(behind):
        for piece in range(PIECES):
            for side in range(2):
                if behind:
                    m_arrived(side, behind, piece)
                m_forward(side, behind, 2, piece)
        for piece in range(PIECES):
            for side in range(2):
                m_forward(side, behind, 1, piece)

    m_stage(0)

    for d in range(1, far[0] + 1):
        for index in [d, far[0] + d]:
            if d <= far[index > far[0]] and not (relayed and d == REACH):
                z_arrived(1, index)
    finished = list(pending)
    pending.clear()
    for dy in (2, 1, 3):
        one = second_half.at[:, y]
        launch(one, one, q_send.at[dy], q_recv.at[seqs - dy], at(0, dy, 0))

    late_work = {}

    def project_second():
        for dy in (1, 3, 2):
            one = second_half.at[:, (y + dy) % seqs]
            copy(one, one, q_send.at[dy], q_recv.at[dy], me).wait_recv()
        pre = project(second_half[:, :, :, : 2 * depth].reshape(width, 2 * depth))
        full_out = second_half[:, :, :, 2 * depth :].reshape(FOLD, width // FOLD, depth)
        for fold in range(FOLD):
            out_weights[:, fold * depth : (fold + 1) * depth] = full_out[fold]
        conv_buf[:, : depth] = pre[:, :depth]
        gate_pre = pre[PAD:, depth:]
        gate_buf[...] = out_gain_ref[...] * gate_pre * jax.nn.sigmoid(gate_pre)

    def queries_and_scores():
        queries = [
            l2_normalize(conv(0, cq_ref, chunk * size)) * depth ** (-0.5) for chunk in range(CHUNKS)
        ]
        late_work["queries"] = queries
        late_work["scores"] = [
            jnp.where(row >= col, dot(q, k, NT) * decay, 0.0) for q, k in zip(queries, keys)
        ]

    def reads_and_locals():
        for chunk in range(CHUNKS):
            seen = dot(late_work["scores"][chunk], both[chunk])
            read = late_work["queries"][chunk] * kept - seen[:, depth:]
            local = seen[:, :depth]
            if chunk:
                value, erase = before[chunk - 1]
                shifted = dot(read, jnp.concatenate([value, erase], axis=1))
                local = local + shifted[:, :depth]
                read = before_kept[chunk - 1] * read - shifted[:, depth:]
            rows = slice(chunk * size, (chunk + 1) * size)
            reads_buf[rows, :] = read.astype(bf16)
            locals_buf[rows, :] = local

    beside = [project_second, queries_and_scores, reads_and_locals]
    stretch = running_kept
    late, late_kept, early = None, None, jnp.zeros((depth, depth), f32)
    for stage in range(2, far[0] + 2, 2):
        if stage < far[0]:
            m_stage(stage)
        for hop in (stage - 1, stage):
            if hop > far[0]:
                continue
            if hop < stage or stage >= far[0]:
                for piece in range(PIECES):
                    for side in range(2):
                        m_arrived(side, hop, piece)
            zz = source[0](hop)
            value = jnp.where(z >= hop, maps[zz, 0].astype(f32), 0.0)
            erase = jnp.where(z >= hop, maps[zz, 1].astype(f32), 0.0)
            if late is None:
                late, late_kept = (value, erase), stretch
            else:
                late = compose((value, erase), stretch, late, late_kept)
                late_kept = late_kept * stretch
            if hop <= far[1]:
                zz = source[1](hop)
                new = stretch * early + maps[zz, 0].astype(f32) - dot(maps[zz, 1], early)
                early = jnp.where(z + hop >= hops, new, 0.0)
        if stage == FIRST_BESIDE:
            for one in finished:
                one.wait_send()
        if stage >= FIRST_BESIDE:
            for _ in range(min(len(beside), 1 if stage == FIRST_BESIDE else 2)):
                beside.pop(0)()
    for one in beside:
        one()
    state = late[0] + late_kept * early - dot(late[1], early)

    state = state.astype(bf16)

    fold_row = fold_of.astype(jnp.int32)

    def products(rows_of, cc):
        rows = dot(owned_buf[cc], rows_of)
        wide = [jnp.where(fold_row == fold, rows, 0.0).astype(bf16) for fold in range(FOLD)]
        return dot(jnp.concatenate(wide, axis=1), out_weights[...], NT).reshape(chips, folded, -1)

    gated = []
    for i, dy in enumerate(order):
        rows = pl.ds(pl.multiple_of((y + dy) % seqs * share, PAD), share)
        out = locals_buf[rows, :] + dot(reads_buf[rows, :], state)
        out = out * lax.rsqrt(jnp.mean(out * out, axis=-1, keepdims=True) + out_epsilon)
        gated.append((out * gate_buf[rows, :]).astype(bf16))
        swap_out[i] = products(gated[i], 1 - core).astype(bf16)
        launch(swap_out.at[i], swap_in.at[i], s_send.at[i], s_recv.at[i], partner)
    for i, dy in enumerate(order):
        mine = products(gated[i], core)
        copy(swap_in.at[i], swap_in.at[i], s_send.at[i], s_recv.at[i], me).wait_recv()
        parts[i] = (mine + swap_in[i].astype(f32)).astype(bf16)
        for dx in (2, 1, 3, 0) if chips == 4 else range(chips):
            if dy or dx:
                launch(
                    parts.at[i, (x + dx) % chips],
                    landed.at[y * chips + x],
                    o_send.at[dy * chips + dx],
                    o_recv.at[(seqs - dy) % seqs * chips + (chips - dx) % chips],
                    at(0, dy, dx),
                )
    landed[y * chips + x] = parts[seqs - 1, x]
    for dy, dx in plane:
        slot = landed.at[(y + dy) % seqs * chips + (x + dx) % chips]
        index = dy * chips + dx
        copy(slot, slot, o_send.at[index], o_recv.at[index], me).wait_recv()
    for seq in range(seqs):
        total = landed[seq * chips].astype(f32)
        for chip in range(1, chips):
            total = total + landed[seq * chips + chip].astype(f32)
        rows = [total[fold * here_rows : (fold + 1) * here_rows] for fold in range(FOLD)]
        out_ref[:, seq, :] = jnp.concatenate(rows, axis=1).astype(bf16)
    for one in pending:
        one.wait_send()

    for needed, one in guarded:
        pl.when(needed)(one.wait_send)

    @pl.when(last)
    def _():
        tail.wait_send()


def body(
    tokens,
    in_gain,
    w_query,
    w_key,
    w_value,
    w_gate,
    w_beta,
    conv_query,
    conv_key,
    conv_value,
    decay_rate,
    out_gain,
    w_out,
):
    here_rows, seqs, width = tokens.shape
    depth = w_query.shape[1]
    group, length = lax.axis_size("tp"), lax.axis_size("sp")
    hops = length // seqs
    chips = group // CORES
    owners = seqs * group
    span = owners * here_rows
    block = w_query.shape[0]
    sizes = (depth, seqs, group, hops, here_rows, width)
    anywhere = pl.BlockSpec(memory_space=pl.ANY)
    dma = pltpu.SemaphoreType.DMA
    vmem = pltpu.VMEM
    far = hops // 2 + 1
    return pl.pallas_call(
        functools.partial(mixer_kernel, sizes),
        out_shape=jax.ShapeDtypeStruct(tokens.shape, bf16),
        in_specs=[anywhere] * 10 + [pl.BlockSpec(memory_space=pltpu.SMEM)] + [anywhere] * 2,
        out_specs=pl.BlockSpec(memory_space=vmem),
        scratch_shapes=[
            vmem(tokens.shape, bf16),
            vmem((1, width), f32),
            vmem((1, block), bf16),
            vmem(conv_query.shape, bf16),
            vmem(conv_query.shape, bf16),
            vmem(conv_query.shape, bf16),
            vmem((1, depth), f32),
            vmem((hops, seqs, block, 2 * depth), bf16),
            vmem((hops, seqs, block, 3 * depth), bf16),
            vmem((hops, seqs, 1, depth), f32),
            vmem((seqs, PAD, width), bf16),
            vmem((PAD, width), bf16),
            vmem((PAD, width), bf16),
            vmem((PAD + span, owners * PAD), bf16),
            vmem((CORES, chips * FOLD * here_rows, span // seqs), bf16),
            vmem((span, depth), bf16),
            vmem((span, depth), f32),
            vmem((span, depth), f32),
            vmem((width, depth), bf16),
            vmem((span, depth), f32),
            vmem((width // FOLD, FOLD * depth), bf16),
            vmem((owners, PAD, width), bf16),
            vmem((PAD + span, 2 * depth), f32),
            vmem((hops, 2, depth, depth), bf16),
            vmem((seqs, chips, FOLD * here_rows, width // FOLD), bf16),
            vmem((seqs, chips, FOLD * here_rows, width // FOLD), bf16),
            vmem((seqs, chips, FOLD * here_rows, width // FOLD), bf16),
            vmem((seqs * chips, FOLD * here_rows, width // FOLD), bf16),
            dma((12,)),
            dma((3, hops)),
            dma((3, hops)),
            dma((hops, seqs)),
            dma((hops, seqs)),
            dma((seqs,)),
            dma((seqs,)),
            dma((seqs,)),
            dma((seqs,)),
            dma((seqs * chips,)),
            dma((seqs * chips,)),
            dma((seqs * chips,)),
            dma((seqs * chips,)),
            dma,
            dma,
            dma((2, far, PIECES)),
            dma((2, far, PIECES)),
            dma((seqs,)),
            dma((seqs,)),
            dma((seqs * chips,)),
            dma((seqs * chips,)),
        ],
        compiler_params=pltpu.CompilerParams(
            collective_id=0, has_side_effects=True, vmem_limit_bytes=56 * 1024 * 1024
        ),
    )(
        tokens,
        in_gain[None],
        w_query,
        w_key,
        w_value,
        w_gate,
        w_beta.T,
        conv_query,
        conv_key,
        conv_value,
        decay_rate,
        out_gain[None],
        w_out.T,
    )


def solution(mesh):
    placed = (
        P(("sp", "tp"), None, None),
        P(),
        P("sp", "tp"),
        P("sp", "tp"),
        P("sp", "tp"),
        P("sp", "tp"),
        P("sp", "tp"),
        P(None, "tp"),
        P(None, "tp"),
        P(None, "tp"),
        P("tp"),
        P(),
        P("tp", "sp"),
    )
    return jax.shard_map(
        body, mesh=mesh, in_specs=placed, out_specs=P(("sp", "tp"), None, None), check_vma=False
    )
```

```python
import functools
import math

import jax
import jax.numpy as jnp
from jax import lax
from jax.experimental import pallas as pl
from jax.experimental.pallas import tpu as pltpu
from jax.sharding import PartitionSpec as P

MESH = pl.DeviceIdType.MESH
PAD = 16
CHUNKS = 3
CORES = 2
REACH = 4
FIRST_BESIDE = 4
FOLD = 4
PIECES = 2
epsilon = 1e-06
out_epsilon = 1e-10
f32 = jnp.float32
bf16 = jnp.bfloat16
NN, NT, TN = ((1,), (0,)), ((1,), (1,)), ((0,), (0,))


def dot(a, b, dims=NN):
    return lax.dot_general(
        a.astype(bf16), b.astype(bf16), (dims, ((), ())), preferred_element_type=f32
    )


def iota(shape, axis):
    return lax.broadcasted_iota(jnp.int32, shape, axis)


def l2_normalize(array):
    return array * lax.rsqrt(jnp.sum(array * array, axis=-1, keepdims=True) + epsilon)


def unit_inverses(lowers, row, col):
    size = row.shape[0]
    near = ((row >> 1) == (col >> 1)) & (row != col)
    eye = jnp.where(row == col, 1.0, 0.0)
    inverses = [eye - jnp.where(near, lower, 0.0) for lower in lowers]
    level = 1
    while (1 << level) < size:
        mask = ((row >> (level + 1)) == (col >> (level + 1))) & ((row >> level) != (col >> level))
        inner = [dot(jnp.where(mask, l, 0.0), v) for l, v in zip(lowers, inverses)]
        inverses = [v - dot(v, w) for v, w in zip(inverses, inner)]
        level += 1
    return inverses


def compose(first, kept_first, second, kept_second):
    depth = first[0].shape[0]
    cross = dot(second[1], jnp.concatenate(first, axis=1))
    value = kept_second * first[0] + second[0] - cross[:, :depth]
    erase = kept_second * first[1] + kept_first * second[1] - cross[:, depth:]
    return value, erase


def mixer_kernel(
    sizes,
    tokens_hbm,
    in_gain_hbm,
    wq_hbm,
    wk_hbm,
    wv_hbm,
    wg_hbm,
    wb_hbm,
    cq_hbm,
    ck_hbm,
    cv_hbm,
    rate_ref,
    out_gain_hbm,
    wo_hbm,
    out_ref,
    tokens_ref,
    in_gain_ref,
    beta_ref,
    cq_ref,
    ck_ref,
    cv_ref,
    out_gain_ref,
    first_half,
    second_half,
    strengths,
    spread,
    tail_out,
    tail_in,
    select_buf,
    owned_buf,
    reads_buf,
    locals_buf,
    gate_buf,
    column_buf,
    beta_buf,
    out_weights,
    rows_buf,
    conv_buf,
    maps,
    swap_out,
    swap_in,
    parts,
    landed,
    load,
    z_send,
    z_recv,
    y_send,
    y_recv,
    g_send,
    g_recv,
    q_send,
    q_recv,
    t_send,
    t_recv,
    c_send,
    c_recv,
    h_send,
    h_recv,
    m_send,
    m_recv,
    s_send,
    s_recv,
    o_send,
    o_recv,
):
    depth, seqs, group, hops, here_rows, width = sizes
    chips = group // CORES
    total_tokens = hops * seqs * group * here_rows
    span = seqs * group * here_rows
    size = span // CHUNKS
    sp, tp = lax.axis_index("sp"), lax.axis_index("tp")
    z, y = sp // seqs, sp % seqs
    x, core = tp // CORES, tp % CORES
    far = [hops // 2, (hops - 1) // 2]
    last = (y == seqs - 1) & (tp == group - 1)
    pending = []

    def at(dz, dy, dx, dc=0):
        return {
            "sp": (z + dz) % hops * seqs + (y + dy) % seqs,
            "tp": (x + dx) % chips * CORES + (core + dc) % CORES,
        }

    def copy(src, dst, send, recv, device):
        return pltpu.make_async_remote_copy(
            src_ref=src,
            dst_ref=dst,
            send_sem=send,
            recv_sem=recv,
            device_id=device,
            device_id_type=MESH,
        )

    me = {"sp": sp, "tp": tp}
    partner = at(0, 0, 0, 1)

    def launch(*args):
        one = copy(*args)
        one.start()
        pending.append(one)

    barrier = pltpu.get_barrier_semaphore()
    plane = [(dy, dx) for dy in range(seqs) for dx in range(chips) if dy or dx]
    reach = [d for d in range(1, REACH + 1) if d <= far[0]]
    reach_back = [d for d in range(1, REACH + 1) if d <= far[1]]
    friends = [partner] + [at(0, dy, dx) for dy, dx in plane]
    friends += [at(d, 0, 0) for d in reach] + [at(hops - d, 0, 0) for d in reach]
    for device in friends:
        pl.semaphore_signal(barrier, inc=1, device_id=device, device_id_type=MESH)

    def own(half, part):
        return (first_half, second_half)[half].at[z, y, :, pl.ds(part * depth, depth)]

    loads = [
        (tokens_hbm, tokens_ref),
        (in_gain_hbm, in_gain_ref),
        (wk_hbm, own(0, 0)),
        (wv_hbm, own(0, 1)),
        (wb_hbm, beta_ref),
        (wq_hbm, own(1, 0)),
        (wg_hbm, own(1, 1)),
        (wo_hbm, own(1, 2)),
        (cq_hbm, cq_ref),
        (ck_hbm, ck_ref),
        (cv_hbm, cv_ref),
        (out_gain_hbm, out_gain_ref),
    ]
    loads = [pltpu.make_async_copy(a, b, load.at[i]) for i, (a, b) in enumerate(loads)]
    for one in loads:
        one.start()

    for one in loads[:2]:
        one.wait()

    pad_rows = jnp.zeros((PAD - here_rows, width), f32)
    tail_rows = PAD - here_rows
    for seq in range(seqs):
        values = tokens_ref[:, seq, :].astype(f32)
        scaled = values * lax.rsqrt(jnp.mean(values * values, axis=-1, keepdims=True) + epsilon)
        spread[seq] = jnp.concatenate([scaled * in_gain_ref[...], pad_rows], axis=0).astype(bf16)

    for one in loads[2:]:
        one.wait()

    block = wk_hbm.shape[0]
    strengths[z, y] = jnp.concatenate(
        [beta_ref[...].astype(f32), jnp.zeros((1, depth - block), f32)], axis=1
    )

    pl.semaphore_wait(barrier, len(friends))

    def z_copy(half, index, offset, device):
        zz = (z + offset) % hops
        one = strengths.at[zz] if half == 2 else (first_half, second_half)[half].at[zz, y]
        return copy(one, one, z_send.at[half, index], z_recv.at[half, index], device)

    def z_launch(half, index, offset, device):
        one = z_copy(half, index, offset, device)
        one.start()
        pending.append(one)

    def offset_of(index):
        return hops - index if index <= far[0] else index - far[0]

    def z_first(half):
        for d in reversed(reach):
            z_launch(half, d, 0, at(d, 0, 0))
            if d in reach_back:
                z_launch(half, far[0] + d, 0, at(hops - d, 0, 0))

    def z_arrived(half, index):
        z_copy(half, index, offset_of(index), me).wait_recv()

    def z_relay(half):
        for further in range(far[0] - REACH):
            if further == 0:
                z_arrived(half, REACH)
            index = far[0] - further
            z_launch(half, index, hops - REACH, at(index - REACH, 0, 0))
        for further in range(far[1] - REACH):
            if further == 0:
                z_arrived(half, far[0] + REACH)
            d = far[1] - further
            z_launch(half, far[0] + d, REACH, at(hops - (d - REACH), 0, 0))

    def y_copy(index, dy, offset, yy, device, back=None):
        one = first_half.at[(z + offset) % hops, yy]
        back = dy if back is None else back
        return copy(one, one, y_send.at[index, dy], y_recv.at[index, back], device)

    def y_fan(index):
        offset = offset_of(index) if index else 0
        for dy in (2, 1, 3):
            one = y_copy(index, dy, offset, y, at(0, dy, 0), seqs - dy)
            one.start()
            pending.append(one)

    def t_slot(yy, xx, cc):
        return rows_buf.at[(yy * chips + xx) * CORES + cc]

    relayed = far[0] > REACH
    tail = copy(tail_out, tail_in, h_send, h_recv, at(1, 0, 0))

    @pl.when(last)
    def _():
        ends = [spread[seq].astype(f32)[here_rows - tail_rows : here_rows] for seq in range(seqs)]
        tail_out[...] = jnp.concatenate(ends, axis=0).astype(bf16)
        tail.start()

    z_first(0)
    for dy in (2, 1, 3):
        one = strengths.at[z, y]
        launch(one, one, g_send.at[dy], g_recv.at[seqs - dy], at(0, dy, 0))
    token_copies = [
        copy(
            spread.at[(y + dy) % seqs],
            t_slot(y, x, core),
            t_send.at[dy * chips + dx],
            t_recv.at[(seqs - dy) % seqs * chips + (chips - dx) % chips],
            at(0, dy, dx),
        )
        for dy, dx in plane
    ]
    token_copies.append(
        copy(spread.at[y], t_slot(y, x, core), c_send.at[0], c_recv.at[0], partner)
    )
    pending.extend(token_copies)

    def send_tokens():
        for one in token_copies:
            one.start()
        rows_buf[(y * chips + x) * CORES + core] = spread[y]

    @pl.when(jnp.logical_not(last))
    def _():
        send_tokens()

    y_fan(0)

    full = PAD + span
    padded = seqs * group * PAD
    row, col = iota((full, padded), 0), iota((full, padded), 1)
    place, inside = col // PAD, col % PAD
    select = (row == PAD + place * here_rows + inside) & (inside < here_rows)
    select = select | ((col - row == padded - PAD) & (inside >= here_rows) & (row < PAD))
    select_buf[...] = jnp.where(select, 1.0, 0.0).astype(bf16)

    order = [2, 1, 3, 0]
    share = span // seqs
    folded = FOLD * here_rows
    batch = chips * folded
    row = iota((batch, 1), 0).astype(f32) + 0.5
    chip_of = jnp.floor(row / folded)
    fold_of = jnp.floor(row / here_rows) - FOLD * chip_of
    inside = row - 0.5 - here_rows * (FOLD * chip_of + fold_of)
    first = (CORES * here_rows * chip_of + inside).astype(jnp.int32)
    col = iota((batch, share), 1)
    for cc in range(CORES):
        owned_buf[cc] = jnp.where(col == first + cc * here_rows, 1.0, 0.0).astype(bf16)

    for dy in (1, 3, 2):
        one = strengths.at[z, (y + dy) % seqs]
        copy(one, one, g_send.at[dy], g_recv.at[dy], me).wait_recv()
    z_first(2)

    @pl.when(last)
    def _():
        tail.wait_recv()
        before = jnp.where(z > 0, tail_in[...].astype(f32), 0.0)
        for seq in range(seqs):
            rows = [
                spread[seq].astype(f32)[:here_rows],
                before[seq * tail_rows : (seq + 1) * tail_rows],
            ]
            spread[seq] = jnp.concatenate(rows, axis=0).astype(bf16)
        send_tokens()

    z_first(1)

    if relayed:
        z_relay(0)
        y_fan(REACH)
        y_fan(far[0] + REACH)
    for d in range(1, REACH if relayed else REACH + 1):
        for index in [d, far[0] + d]:
            if d <= far[index > far[0]]:
                z_arrived(0, index)
                y_fan(index)
    if relayed:
        z_relay(2)
        for d in range(REACH + 1, far[0] + 1):
            for index in [d, far[0] + d]:
                if d <= far[index > far[0]]:
                    z_arrived(0, index)
                    y_fan(index)
    for dy, dx in sorted(plane, key=lambda p: min(p[0], seqs - p[0]) + min(p[1], chips - p[1])):
        index = dy * chips + dx
        slot = t_slot((y + dy) % seqs, (x + dx) % chips, core)
        copy(slot, slot, t_send.at[0], t_recv.at[index], me).wait_recv()
        launch(slot, slot, c_send.at[index], c_recv.at[index], partner)
    if relayed:
        z_relay(1)
    for d in range(1, far[0] + 1):
        for index in [d, far[0] + d]:
            if d <= far[index > far[0]] and not (relayed and d == REACH):
                z_arrived(2, index)
    devices = hops * seqs
    pick = iota((width, devices), 0) // block == iota((width, devices), 1)
    column = dot(jnp.where(pick, 1.0, 0.0), strengths[...].reshape(devices, depth))
    column = jnp.where(iota((width, depth), 0) % block == iota((width, depth), 1), column, 0.0)
    column_buf[...] = dot(column, jnp.ones((depth, depth), f32)).astype(bf16)

    for dy, dx in [(0, 0)] + plane:
        index = dy * chips + dx
        slot = t_slot((y + dy) % seqs, (x + dx) % chips, (core + 1) % CORES)
        copy(slot, slot, c_send.at[0], c_recv.at[index], me).wait_recv()
    def project(weights):
        pre = dot(rows_buf[...].reshape(padded, width), weights).astype(bf16)
        return dot(select_buf[...], pre)

    shift = math.log(depth / (4.0 * total_tokens))
    beta_buf[...] = jax.nn.sigmoid(project(column_buf[...])[PAD:] + shift)

    for index in range(far[0] + far[1] + 1):
        offset = offset_of(index) if index else 0
        for dy in (1, 3, 2):
            y_copy(index, dy, offset, (y + dy) % seqs, me).wait_recv()

    pre = project(first_half[...].reshape(width, 2 * depth))
    conv_buf[...] = pre
    width_taps = cq_ref.shape[0]

    def conv(part, taps_ref, begin):
        columns = slice(part * depth, (part + 1) * depth)
        total = jnp.zeros((size, depth), f32)
        for tap in range(width_taps):
            first = PAD + begin - (width_taps - 1) + tap
            taps = taps_ref[tap : tap + 1, :].astype(f32)
            total = total + conv_buf[first : first + size, columns] * taps
        return total * jax.nn.sigmoid(total)

    rate = rate_ref[0] / total_tokens
    row, col = iota((size, size), 0), iota((size, size), 1)
    decay = jnp.exp(-rate * jnp.maximum(row - col, 0).astype(f32))
    step = iota((size, depth), 0).astype(f32)
    kept = jnp.exp(-rate * (step + 1.0))
    rest = jnp.exp(-rate * (size - 1.0 - step))
    keys, values, betas = [], [], []
    for chunk in range(CHUNKS):
        begin = chunk * size
        keys.append(l2_normalize(conv(0, ck_ref, begin)))
        values.append(conv(1, cv_ref, begin))
        betas.append(beta_buf[begin : begin + size, :])
    weighted = [k * b for k, b in zip(keys, betas)]
    lowers = [
        jnp.where(row > col, dot(w, k, NT) * decay, 0.0) for w, k in zip(weighted, keys)
    ]
    inverses = unit_inverses(lowers, row, col)
    both = [
        dot(inv, jnp.concatenate([v * b, w * kept], axis=1))
        for inv, v, b, w in zip(inverses, values, betas, weighted)
    ]
    moved = [dot(k * rest, b, TN) for k, b in zip(keys, both)]
    chunk_maps = [(m[:, :depth], m[:, depth:]) for m in moved]
    chunk_kept = jnp.exp(-rate * jnp.full((1, depth), float(size), f32))
    before, before_kept = [], []
    running, running_kept = chunk_maps[0], chunk_kept
    for chunk in range(1, CHUNKS):
        before.append(running)
        before_kept.append(running_kept)
        running = compose(running, running_kept, chunk_maps[chunk], chunk_kept)
        running_kept = running_kept * chunk_kept
    for part in range(2):
        maps[z, part] = running[part].astype(bf16)

    source = [lambda d: (z + hops - d) % hops, lambda d: (z + d) % hops]

    def m_copy(side, hop, piece, offset, device):
        rows = depth * 2 // PIECES
        part, begin = piece * rows // depth, piece * rows % depth
        one = maps.at[source[side](offset), part, pl.ds(begin, rows)]
        return copy(one, one, m_send.at[side, hop, piece], m_recv.at[side, hop, piece], device)

    guarded = []

    def useful(side, behind, step):
        if side == 0:
            return (z >= behind) & (z + step < hops)
        first = (z + behind) % hops
        if step == 2:
            return first < far[1]
        return (first < far[1]) & (first < behind + step)

    def m_forward(side, behind, step, piece):
        if behind + step <= far[side]:
            device = at(step if side == 0 else hops - step, 0, 0)
            one = m_copy(side, behind + step, piece, behind, device)
            needed = useful(side, behind, step)
            guarded.append((needed, one))
            pl.when(needed)(one.start)

    def m_arrived(side, hop, piece):
        if hop <= far[side]:
            first = (z + hop) % hops
            needed = z >= hop
            if side == 1:
                needed = first < far[1]
                if hop % 2:
                    needed = needed & (first < hop)
            pl.when(needed)(m_copy(side, hop, piece, hop, me).wait_recv)

    def m_stage(behind):
        for piece in range(PIECES):
            for side in range(2):
                if behind:
                    m_arrived(side, behind, piece)
                m_forward(side, behind, 2, piece)
        for piece in range(PIECES):
            for side in range(2):
                m_forward(side, behind, 1, piece)

    m_stage(0)

    for d in range(1, far[0] + 1):
        for index in [d, far[0] + d]:
            if d <= far[index > far[0]] and not (relayed and d == REACH):
                z_arrived(1, index)
    finished = list(pending)
    pending.clear()
    for dy in (2, 1, 3):
        one = second_half.at[:, y]
        launch(one, one, q_send.at[dy], q_recv.at[seqs - dy], at(0, dy, 0))

    late_work = {}

    def project_second():
        for dy in (1, 3, 2):
            one = second_half.at[:, (y + dy) % seqs]
            copy(one, one, q_send.at[dy], q_recv.at[dy], me).wait_recv()
        pre = project(second_half[:, :, :, : 2 * depth].reshape(width, 2 * depth))
        full_out = second_half[:, :, :, 2 * depth :].reshape(FOLD, width // FOLD, depth)
        for fold in range(FOLD):
            out_weights[:, fold * depth : (fold + 1) * depth] = full_out[fold]
        conv_buf[:, : depth] = pre[:, :depth]
        gate_pre = pre[PAD:, depth:]
        gate_buf[...] = out_gain_ref[...] * gate_pre * jax.nn.sigmoid(gate_pre)

    def queries_and_scores():
        queries = [
            l2_normalize(conv(0, cq_ref, chunk * size)) * depth ** (-0.5) for chunk in range(CHUNKS)
        ]
        late_work["queries"] = queries
        late_work["scores"] = [
            jnp.where(row >= col, dot(q, k, NT) * decay, 0.0) for q, k in zip(queries, keys)
        ]

    def reads_and_locals():
        for chunk in range(CHUNKS):
            seen = dot(late_work["scores"][chunk], both[chunk])
            read = late_work["queries"][chunk] * kept - seen[:, depth:]
            local = seen[:, :depth]
            if chunk:
                value, erase = before[chunk - 1]
                shifted = dot(read, jnp.concatenate([value, erase], axis=1))
                local = local + shifted[:, :depth]
                read = before_kept[chunk - 1] * read - shifted[:, depth:]
            rows = slice(chunk * size, (chunk + 1) * size)
            reads_buf[rows, :] = read.astype(bf16)
            locals_buf[rows, :] = local

    beside = [project_second, queries_and_scores, reads_and_locals]
    stretch = running_kept
    late, late_kept, early = None, None, jnp.zeros((depth, depth), f32)
    for stage in range(2, far[0] + 2, 2):
        if stage < far[0]:
            m_stage(stage)
        for hop in (stage - 1, stage):
            if hop > far[0]:
                continue
            if hop < stage or stage >= far[0]:
                for piece in range(PIECES):
                    for side in range(2):
                        m_arrived(side, hop, piece)
            zz = source[0](hop)
            value = jnp.where(z >= hop, maps[zz, 0].astype(f32), 0.0)
            erase = jnp.where(z >= hop, maps[zz, 1].astype(f32), 0.0)
            if late is None:
                late, late_kept = (value, erase), stretch
            else:
                late = compose((value, erase), stretch, late, late_kept)
                late_kept = late_kept * stretch
            if hop <= far[1]:
                zz = source[1](hop)
                new = stretch * early + maps[zz, 0].astype(f32) - dot(maps[zz, 1], early)
                early = jnp.where(z + hop >= hops, new, 0.0)
        if stage == FIRST_BESIDE:
            for one in finished:
                one.wait_send()
        if stage >= FIRST_BESIDE:
            for _ in range(min(len(beside), 1 if stage == FIRST_BESIDE else 2)):
                beside.pop(0)()
    for one in beside:
        one()
    state = late[0] + late_kept * early - dot(late[1], early)

    state = state.astype(bf16)

    fold_row = fold_of.astype(jnp.int32)

    def products(rows_of, cc):
        rows = dot(owned_buf[cc], rows_of)
        wide = [jnp.where(fold_row == fold, rows, 0.0).astype(bf16) for fold in range(FOLD)]
        return dot(jnp.concatenate(wide, axis=1), out_weights[...], NT).reshape(chips, folded, -1)

    gated = []
    for i, dy in enumerate(order):
        rows = pl.ds(pl.multiple_of((y + dy) % seqs * share, PAD), share)
        out = locals_buf[rows, :] + dot(reads_buf[rows, :], state)
        out = out * lax.rsqrt(jnp.mean(out * out, axis=-1, keepdims=True) + out_epsilon)
        gated.append((out * gate_buf[rows, :]).astype(bf16))
        swap_out[i] = products(gated[i], 1 - core).astype(bf16)
        launch(swap_out.at[i], swap_in.at[i], s_send.at[i], s_recv.at[i], partner)
    for i, dy in enumerate(order):
        mine = products(gated[i], core)
        copy(swap_in.at[i], swap_in.at[i], s_send.at[i], s_recv.at[i], me).wait_recv()
        parts[i] = (mine + swap_in[i].astype(f32)).astype(bf16)
        for dx in (2, 1, 3, 0) if chips == 4 else range(chips):
            if dy or dx:
                launch(
                    parts.at[i, (x + dx) % chips],
                    landed.at[y * chips + x],
                    o_send.at[dy * chips + dx],
                    o_recv.at[(seqs - dy) % seqs * chips + (chips - dx) % chips],
                    at(0, dy, dx),
                )
    landed[y * chips + x] = parts[seqs - 1, x]
    for dy, dx in plane:
        slot = landed.at[(y + dy) % seqs * chips + (x + dx) % chips]
        index = dy * chips + dx
        copy(slot, slot, o_send.at[index], o_recv.at[index], me).wait_recv()
    for seq in range(seqs):
        total = landed[seq * chips].astype(f32)
        for chip in range(1, chips):
            total = total + landed[seq * chips + chip].astype(f32)
        rows = [total[fold * here_rows : (fold + 1) * here_rows] for fold in range(FOLD)]
        out_ref[:, seq, :] = jnp.concatenate(rows, axis=1).astype(bf16)
    for one in pending:
        one.wait_send()

    for needed, one in guarded:
        pl.when(needed)(one.wait_send)

    @pl.when(last)
    def _():
        tail.wait_send()


def body(
    tokens,
    in_gain,
    w_query,
    w_key,
    w_value,
    w_gate,
    w_beta,
    conv_query,
    conv_key,
    conv_value,
    decay_rate,
    out_gain,
    w_out,
):
    here_rows, seqs, width = tokens.shape
    depth = w_query.shape[1]
    group, length = lax.axis_size("tp"), lax.axis_size("sp")
    hops = length // seqs
    chips = group // CORES
    owners = seqs * group
    span = owners * here_rows
    block = w_query.shape[0]
    sizes = (depth, seqs, group, hops, here_rows, width)
    anywhere = pl.BlockSpec(memory_space=pl.ANY)
    dma = pltpu.SemaphoreType.DMA
    vmem = pltpu.VMEM
    far = hops // 2 + 1
    return pl.pallas_call(
        functools.partial(mixer_kernel, sizes),
        out_shape=jax.ShapeDtypeStruct(tokens.shape, bf16),
        in_specs=[anywhere] * 10 + [pl.BlockSpec(memory_space=pltpu.SMEM)] + [anywhere] * 2,
        out_specs=pl.BlockSpec(memory_space=vmem),
        scratch_shapes=[
            vmem(tokens.shape, bf16),
            vmem((1, width), f32),
            vmem((1, block), bf16),
            vmem(conv_query.shape, bf16),
            vmem(conv_query.shape, bf16),
            vmem(conv_query.shape, bf16),
            vmem((1, depth), f32),
            vmem((hops, seqs, block, 2 * depth), bf16),
            vmem((hops, seqs, block, 3 * depth), bf16),
            vmem((hops, seqs, 1, depth), f32),
            vmem((seqs, PAD, width), bf16),
            vmem((PAD, width), bf16),
            vmem((PAD, width), bf16),
            vmem((PAD + span, owners * PAD), bf16),
            vmem((CORES, chips * FOLD * here_rows, span // seqs), bf16),
            vmem((span, depth), bf16),
            vmem((span, depth), f32),
            vmem((span, depth), f32),
            vmem((width, depth), bf16),
            vmem((span, depth), f32),
            vmem((width // FOLD, FOLD * depth), bf16),
            vmem((owners, PAD, width), bf16),
            vmem((PAD + span, 2 * depth), f32),
            vmem((hops, 2, depth, depth), bf16),
            vmem((seqs, chips, FOLD * here_rows, width // FOLD), bf16),
            vmem((seqs, chips, FOLD * here_rows, width // FOLD), bf16),
            vmem((seqs, chips, FOLD * here_rows, width // FOLD), bf16),
            vmem((seqs * chips, FOLD * here_rows, width // FOLD), bf16),
            dma((12,)),
            dma((3, hops)),
            dma((3, hops)),
            dma((hops, seqs)),
            dma((hops, seqs)),
            dma((seqs,)),
            dma((seqs,)),
            dma((seqs,)),
            dma((seqs,)),
            dma((seqs * chips,)),
            dma((seqs * chips,)),
            dma((seqs * chips,)),
            dma((seqs * chips,)),
            dma,
            dma,
            dma((2, far, PIECES)),
            dma((2, far, PIECES)),
            dma((seqs,)),
            dma((seqs,)),
            dma((seqs * chips,)),
            dma((seqs * chips,)),
        ],
        compiler_params=pltpu.CompilerParams(
            collective_id=0, has_side_effects=True, vmem_limit_bytes=56 * 1024 * 1024
        ),
    )(
        tokens,
        in_gain[None],
        w_query,
        w_key,
        w_value,
        w_gate,
        w_beta.T,
        conv_query,
        conv_key,
        conv_value,
        decay_rate,
        out_gain[None],
        w_out.T,
    )


def solution(mesh):
    placed = (
        P(("sp", "tp"), None, None),
        P(),
        P("sp", "tp"),
        P("sp", "tp"),
        P("sp", "tp"),
        P("sp", "tp"),
        P("sp", "tp"),
        P(None, "tp"),
        P(None, "tp"),
        P(None, "tp"),
        P("tp"),
        P(),
        P("tp", "sp"),
    )
    return jax.shard_map(
        body, mesh=mesh, in_specs=placed, out_specs=P(("sp", "tp"), None, None), check_vma=False
    )
```

```python
import functools
import math

import jax
import jax.numpy as jnp
from jax import lax
from jax.experimental import pallas as pl
from jax.experimental.pallas import tpu as pltpu
from jax.sharding import PartitionSpec as P

MESH = pl.DeviceIdType.MESH
PAD = 16
CHUNKS = 4
CORES = 2
REACH = 4
FIRST_BESIDE = 4
FOLD = 4
PIECES = 2
epsilon = 1e-06
out_epsilon = 1e-10
f32 = jnp.float32
bf16 = jnp.bfloat16
NN, NT, TN = ((1,), (0,)), ((1,), (1,)), ((0,), (0,))


def dot(a, b, dims=NN):
    return lax.dot_general(
        a.astype(bf16), b.astype(bf16), (dims, ((), ())), preferred_element_type=f32
    )


def iota(shape, axis):
    return lax.broadcasted_iota(jnp.int32, shape, axis)


def l2_normalize(array):
    return array * lax.rsqrt(jnp.sum(array * array, axis=-1, keepdims=True) + epsilon)


def unit_inverses(lowers, row, col):
    size = row.shape[0]
    near = ((row >> 1) == (col >> 1)) & (row != col)
    eye = jnp.where(row == col, 1.0, 0.0)
    inverses = [eye - jnp.where(near, lower, 0.0) for lower in lowers]
    level = 1
    while (1 << level) < size:
        mask = ((row >> (level + 1)) == (col >> (level + 1))) & ((row >> level) != (col >> level))
        inner = [dot(jnp.where(mask, l, 0.0), v) for l, v in zip(lowers, inverses)]
        inverses = [v - dot(v, w) for v, w in zip(inverses, inner)]
        level += 1
    return inverses


def compose(first, kept_first, second, kept_second):
    depth = first[0].shape[0]
    cross = dot(second[1], jnp.concatenate(first, axis=1))
    value = kept_second * first[0] + second[0] - cross[:, :depth]
    erase = kept_second * first[1] + kept_first * second[1] - cross[:, depth:]
    return value, erase


def mixer_kernel(
    sizes,
    tokens_hbm,
    in_gain_hbm,
    wq_hbm,
    wk_hbm,
    wv_hbm,
    wg_hbm,
    wb_hbm,
    cq_hbm,
    ck_hbm,
    cv_hbm,
    rate_ref,
    out_gain_hbm,
    wo_hbm,
    out_ref,
    tokens_ref,
    in_gain_ref,
    beta_ref,
    cq_ref,
    ck_ref,
    cv_ref,
    out_gain_ref,
    first_half,
    second_half,
    strengths,
    spread,
    tail_out,
    tail_in,
    select_buf,
    owned_buf,
    reads_buf,
    locals_buf,
    gate_buf,
    column_buf,
    beta_buf,
    out_weights,
    rows_buf,
    conv_buf,
    maps,
    swap_out,
    swap_in,
    parts,
    landed,
    load,
    z_send,
    z_recv,
    y_send,
    y_recv,
    g_send,
    g_recv,
    q_send,
    q_recv,
    t_send,
    t_recv,
    c_send,
    c_recv,
    h_send,
    h_recv,
    m_send,
    m_recv,
    s_send,
    s_recv,
    o_send,
    o_recv,
):
    depth, seqs, group, hops, here_rows, width = sizes
    chips = group // CORES
    total_tokens = hops * seqs * group * here_rows
    span = seqs * group * here_rows
    size = span // CHUNKS
    sp, tp = lax.axis_index("sp"), lax.axis_index("tp")
    z, y = sp // seqs, sp % seqs
    x, core = tp // CORES, tp % CORES
    far = [hops // 2, (hops - 1) // 2]
    last = (y == seqs - 1) & (tp == group - 1)
    pending = []

    def at(dz, dy, dx, dc=0):
        return {
            "sp": (z + dz) % hops * seqs + (y + dy) % seqs,
            "tp": (x + dx) % chips * CORES + (core + dc) % CORES,
        }

    def copy(src, dst, send, recv, device):
        return pltpu.make_async_remote_copy(
            src_ref=src,
            dst_ref=dst,
            send_sem=send,
            recv_sem=recv,
            device_id=device,
            device_id_type=MESH,
        )

    me = {"sp": sp, "tp": tp}
    partner = at(0, 0, 0, 1)

    def launch(*args):
        one = copy(*args)
        one.start()
        pending.append(one)

    barrier = pltpu.get_barrier_semaphore()
    plane = [(dy, dx) for dy in range(seqs) for dx in range(chips) if dy or dx]
    reach = [d for d in range(1, REACH + 1) if d <= far[0]]
    reach_back = [d for d in range(1, REACH + 1) if d <= far[1]]
    friends = [partner] + [at(0, dy, dx) for dy, dx in plane]
    friends += [at(d, 0, 0) for d in reach] + [at(hops - d, 0, 0) for d in reach]
    for device in friends:
        pl.semaphore_signal(barrier, inc=1, device_id=device, device_id_type=MESH)

    def own(half, part):
        return (first_half, second_half)[half].at[z, y, :, pl.ds(part * depth, depth)]

    loads = [
        (tokens_hbm, tokens_ref),
        (in_gain_hbm, in_gain_ref),
        (wk_hbm, own(0, 0)),
        (wv_hbm, own(0, 1)),
        (wb_hbm, beta_ref),
        (wq_hbm, own(1, 0)),
        (wg_hbm, own(1, 1)),
        (wo_hbm, own(1, 2)),
        (cq_hbm, cq_ref),
        (ck_hbm, ck_ref),
        (cv_hbm, cv_ref),
        (out_gain_hbm, out_gain_ref),
    ]
    loads = [pltpu.make_async_copy(a, b, load.at[i]) for i, (a, b) in enumerate(loads)]
    for one in loads:
        one.start()

    for one in loads[:2]:
        one.wait()

    pad_rows = jnp.zeros((PAD - here_rows, width), f32)
    tail_rows = PAD - here_rows
    for seq in range(seqs):
        values = tokens_ref[:, seq, :].astype(f32)
        scaled = values * lax.rsqrt(jnp.mean(values * values, axis=-1, keepdims=True) + epsilon)
        spread[seq] = jnp.concatenate([scaled * in_gain_ref[...], pad_rows], axis=0).astype(bf16)

    for one in loads[2:]:
        one.wait()

    block = wk_hbm.shape[0]
    strengths[z, y] = jnp.concatenate(
        [beta_ref[...].astype(f32), jnp.zeros((1, depth - block), f32)], axis=1
    )

    pl.semaphore_wait(barrier, len(friends))

    def z_copy(half, index, offset, device):
        zz = (z + offset) % hops
        one = strengths.at[zz] if half == 2 else (first_half, second_half)[half].at[zz, y]
        return copy(one, one, z_send.at[half, index], z_recv.at[half, index], device)

    def z_launch(half, index, offset, device):
        one = z_copy(half, index, offset, device)
        one.start()
        pending.append(one)

    def offset_of(index):
        return hops - index if index <= far[0] else index - far[0]

    def z_first(half):
        for d in reversed(reach):
            z_launch(half, d, 0, at(d, 0, 0))
            if d in reach_back:
                z_launch(half, far[0] + d, 0, at(hops - d, 0, 0))

    def z_arrived(half, index):
        z_copy(half, index, offset_of(index), me).wait_recv()

    def z_relay(half):
        for further in range(far[0] - REACH):
            if further == 0:
                z_arrived(half, REACH)
            index = far[0] - further
            z_launch(half, index, hops - REACH, at(index - REACH, 0, 0))
        for further in range(far[1] - REACH):
            if further == 0:
                z_arrived(half, far[0] + REACH)
            d = far[1] - further
            z_launch(half, far[0] + d, REACH, at(hops - (d - REACH), 0, 0))

    def y_copy(index, dy, offset, yy, device, back=None):
        one = first_half.at[(z + offset) % hops, yy]
        back = dy if back is None else back
        return copy(one, one, y_send.at[index, dy], y_recv.at[index, back], device)

    def y_fan(index):
        offset = offset_of(index) if index else 0
        for dy in (2, 1, 3):
            one = y_copy(index, dy, offset, y, at(0, dy, 0), seqs - dy)
            one.start()
            pending.append(one)

    def t_slot(yy, xx, cc):
        return rows_buf.at[(yy * chips + xx) * CORES + cc]

    relayed = far[0] > REACH
    tail = copy(tail_out, tail_in, h_send, h_recv, at(1, 0, 0))

    @pl.when(last)
    def _():
        ends = [spread[seq].astype(f32)[here_rows - tail_rows : here_rows] for seq in range(seqs)]
        tail_out[...] = jnp.concatenate(ends, axis=0).astype(bf16)
        tail.start()

    z_first(0)
    for dy in (2, 1, 3):
        one = strengths.at[z, y]
        launch(one, one, g_send.at[dy], g_recv.at[seqs - dy], at(0, dy, 0))
    token_copies = [
        copy(
            spread.at[(y + dy) % seqs],
            t_slot(y, x, core),
            t_send.at[dy * chips + dx],
            t_recv.at[(seqs - dy) % seqs * chips + (chips - dx) % chips],
            at(0, dy, dx),
        )
        for dy, dx in plane
    ]
    token_copies.append(
        copy(spread.at[y], t_slot(y, x, core), c_send.at[0], c_recv.at[0], partner)
    )
    pending.extend(token_copies)

    def send_tokens():
        for one in token_copies:
            one.start()
        rows_buf[(y * chips + x) * CORES + core] = spread[y]

    @pl.when(jnp.logical_not(last))
    def _():
        send_tokens()

    y_fan(0)

    full = PAD + span
    padded = seqs * group * PAD
    row, col = iota((full, padded), 0), iota((full, padded), 1)
    place, inside = col // PAD, col % PAD
    select = (row == PAD + place * here_rows + inside) & (inside < here_rows)
    select = select | ((col - row == padded - PAD) & (inside >= here_rows) & (row < PAD))
    select_buf[...] = jnp.where(select, 1.0, 0.0).astype(bf16)

    order = [2, 1, 3, 0]
    share = span // seqs
    folded = FOLD * here_rows
    batch = chips * folded
    row = iota((batch, 1), 0).astype(f32) + 0.5
    chip_of = jnp.floor(row / folded)
    fold_of = jnp.floor(row / here_rows) - FOLD * chip_of
    inside = row - 0.5 - here_rows * (FOLD * chip_of + fold_of)
    first = (CORES * here_rows * chip_of + inside).astype(jnp.int32)
    col = iota((batch, share), 1)
    for cc in range(CORES):
        owned_buf[cc] = jnp.where(col == first + cc * here_rows, 1.0, 0.0).astype(bf16)

    for dy in (1, 3, 2):
        one = strengths.at[z, (y + dy) % seqs]
        copy(one, one, g_send.at[dy], g_recv.at[dy], me).wait_recv()
    z_first(2)

    @pl.when(last)
    def _():
        tail.wait_recv()
        before = jnp.where(z > 0, tail_in[...].astype(f32), 0.0)
        for seq in range(seqs):
            rows = [
                spread[seq].astype(f32)[:here_rows],
                before[seq * tail_rows : (seq + 1) * tail_rows],
            ]
            spread[seq] = jnp.concatenate(rows, axis=0).astype(bf16)
        send_tokens()

    z_first(1)

    if relayed:
        z_relay(0)
        y_fan(REACH)
        y_fan(far[0] + REACH)
    for d in range(1, REACH if relayed else REACH + 1):
        for index in [d, far[0] + d]:
            if d <= far[index > far[0]]:
                z_arrived(0, index)
                y_fan(index)
    if relayed:
        z_relay(2)
        for d in range(REACH + 1, far[0] + 1):
            for index in [d, far[0] + d]:
                if d <= far[index > far[0]]:
                    z_arrived(0, index)
                    y_fan(index)
    for dy, dx in sorted(plane, key=lambda p: min(p[0], seqs - p[0]) + min(p[1], chips - p[1])):
        index = dy * chips + dx
        slot = t_slot((y + dy) % seqs, (x + dx) % chips, core)
        copy(slot, slot, t_send.at[0], t_recv.at[index], me).wait_recv()
        launch(slot, slot, c_send.at[index], c_recv.at[index], partner)
    if relayed:
        z_relay(1)
    for d in range(1, far[0] + 1):
        for index in [d, far[0] + d]:
            if d <= far[index > far[0]] and not (relayed and d == REACH):
                z_arrived(2, index)
    devices = hops * seqs
    pick = iota((width, devices), 0) // block == iota((width, devices), 1)
    column = dot(jnp.where(pick, 1.0, 0.0), strengths[...].reshape(devices, depth))
    column = jnp.where(iota((width, depth), 0) % block == iota((width, depth), 1), column, 0.0)
    column_buf[...] = dot(column, jnp.ones((depth, depth), f32)).astype(bf16)

    for dy, dx in [(0, 0)] + plane:
        index = dy * chips + dx
        slot = t_slot((y + dy) % seqs, (x + dx) % chips, (core + 1) % CORES)
        copy(slot, slot, c_send.at[0], c_recv.at[index], me).wait_recv()
    def project(weights):
        pre = dot(rows_buf[...].reshape(padded, width), weights).astype(bf16)
        return dot(select_buf[...], pre)

    shift = math.log(depth / (4.0 * total_tokens))
    beta_buf[...] = jax.nn.sigmoid(project(column_buf[...])[PAD:] + shift)

    for index in range(far[0] + far[1] + 1):
        offset = offset_of(index) if index else 0
        for dy in (1, 3, 2):
            y_copy(index, dy, offset, (y + dy) % seqs, me).wait_recv()

    pre = project(first_half[...].reshape(width, 2 * depth))
    conv_buf[...] = pre
    width_taps = cq_ref.shape[0]

    def conv(part, taps_ref, begin):
        columns = slice(part * depth, (part + 1) * depth)
        total = jnp.zeros((size, depth), f32)
        for tap in range(width_taps):
            first = PAD + begin - (width_taps - 1) + tap
            taps = taps_ref[tap : tap + 1, :].astype(f32)
            total = total + conv_buf[first : first + size, columns] * taps
        return total * jax.nn.sigmoid(total)

    rate = rate_ref[0] / total_tokens
    row, col = iota((size, size), 0), iota((size, size), 1)
    decay = jnp.exp(-rate * jnp.maximum(row - col, 0).astype(f32))
    step = iota((size, depth), 0).astype(f32)
    kept = jnp.exp(-rate * (step + 1.0))
    rest = jnp.exp(-rate * (size - 1.0 - step))
    keys, values, betas = [], [], []
    for chunk in range(CHUNKS):
        begin = chunk * size
        keys.append(l2_normalize(conv(0, ck_ref, begin)))
        values.append(conv(1, cv_ref, begin))
        betas.append(beta_buf[begin : begin + size, :])
    weighted = [k * b for k, b in zip(keys, betas)]
    lowers = [
        jnp.where(row > col, dot(w, k, NT) * decay, 0.0) for w, k in zip(weighted, keys)
    ]
    inverses = unit_inverses(lowers, row, col)
    both = [
        dot(inv, jnp.concatenate([v * b, w * kept], axis=1))
        for inv, v, b, w in zip(inverses, values, betas, weighted)
    ]
    moved = [dot(k * rest, b, TN) for k, b in zip(keys, both)]
    chunk_maps = [(m[:, :depth], m[:, depth:]) for m in moved]
    chunk_kept = jnp.exp(-rate * jnp.full((1, depth), float(size), f32))
    kept_two = chunk_kept * chunk_kept
    front = compose(chunk_maps[0], chunk_kept, chunk_maps[1], chunk_kept)
    back = compose(chunk_maps[2], chunk_kept, chunk_maps[3], chunk_kept)
    running = compose(front, kept_two, back, kept_two)
    running_kept = kept_two * kept_two
    for part in range(2):
        maps[z, part] = running[part].astype(bf16)

    source = [lambda d: (z + hops - d) % hops, lambda d: (z + d) % hops]

    def m_copy(side, hop, piece, offset, device):
        rows = depth * 2 // PIECES
        part, begin = piece * rows // depth, piece * rows % depth
        one = maps.at[source[side](offset), part, pl.ds(begin, rows)]
        return copy(one, one, m_send.at[side, hop, piece], m_recv.at[side, hop, piece], device)

    guarded = []

    def useful(side, behind, step):
        if side == 0:
            return (z >= behind) & (z + step < hops)
        first = (z + behind) % hops
        if step == 2:
            return first < far[1]
        return (first < far[1]) & (first < behind + step)

    def m_forward(side, behind, step, piece):
        if behind + step <= far[side]:
            device = at(step if side == 0 else hops - step, 0, 0)
            one = m_copy(side, behind + step, piece, behind, device)
            needed = useful(side, behind, step)
            guarded.append((needed, one))
            pl.when(needed)(one.start)

    def m_arrived(side, hop, piece):
        if hop <= far[side]:
            first = (z + hop) % hops
            needed = z >= hop
            if side == 1:
                needed = first < far[1]
                if hop % 2:
                    needed = needed & (first < hop)
            pl.when(needed)(m_copy(side, hop, piece, hop, me).wait_recv)

    def m_stage(behind):
        for piece in range(PIECES):
            for side in range(2):
                if behind:
                    m_arrived(side, behind, piece)
                m_forward(side, behind, 2, piece)
        for piece in range(PIECES):
            for side in range(2):
                m_forward(side, behind, 1, piece)

    m_stage(0)
    third = compose(front, kept_two, chunk_maps[2], chunk_kept)
    before = [chunk_maps[0], front, third]
    before_kept = [chunk_kept, kept_two, kept_two * chunk_kept]

    for d in range(1, far[0] + 1):
        for index in [d, far[0] + d]:
            if d <= far[index > far[0]] and not (relayed and d == REACH):
                z_arrived(1, index)
    finished = list(pending)
    pending.clear()
    for dy in (2, 1, 3):
        one = second_half.at[:, y]
        launch(one, one, q_send.at[dy], q_recv.at[seqs - dy], at(0, dy, 0))

    late_work = {}

    def project_second():
        for dy in (1, 3, 2):
            one = second_half.at[:, (y + dy) % seqs]
            copy(one, one, q_send.at[dy], q_recv.at[dy], me).wait_recv()
        pre = project(second_half[:, :, :, : 2 * depth].reshape(width, 2 * depth))
        full_out = second_half[:, :, :, 2 * depth :].reshape(FOLD, width // FOLD, depth)
        for fold in range(FOLD):
            out_weights[:, fold * depth : (fold + 1) * depth] = full_out[fold]
        conv_buf[:, : depth] = pre[:, :depth]
        gate_pre = pre[PAD:, depth:]
        gate_buf[...] = out_gain_ref[...] * gate_pre * jax.nn.sigmoid(gate_pre)

    def queries_and_scores():
        queries = [
            l2_normalize(conv(0, cq_ref, chunk * size)) * depth ** (-0.5) for chunk in range(CHUNKS)
        ]
        late_work["queries"] = queries
        late_work["scores"] = [
            jnp.where(row >= col, dot(q, k, NT) * decay, 0.0) for q, k in zip(queries, keys)
        ]

    def reads_and_locals():
        for chunk in range(CHUNKS):
            seen = dot(late_work["scores"][chunk], both[chunk])
            read = late_work["queries"][chunk] * kept - seen[:, depth:]
            local = seen[:, :depth]
            if chunk:
                value, erase = before[chunk - 1]
                shifted = dot(read, jnp.concatenate([value, erase], axis=1))
                local = local + shifted[:, :depth]
                read = before_kept[chunk - 1] * read - shifted[:, depth:]
            rows = slice(chunk * size, (chunk + 1) * size)
            reads_buf[rows, :] = read.astype(bf16)
            locals_buf[rows, :] = local

    beside = [project_second, queries_and_scores, reads_and_locals]
    stretch = running_kept
    late, late_kept, early = None, None, jnp.zeros((depth, depth), f32)
    for stage in range(2, far[0] + 2, 2):
        if stage < far[0]:
            m_stage(stage)
        for hop in (stage - 1, stage):
            if hop > far[0]:
                continue
            if hop < stage or stage >= far[0]:
                for piece in range(PIECES):
                    for side in range(2):
                        m_arrived(side, hop, piece)
            zz = source[0](hop)
            value = jnp.where(z >= hop, maps[zz, 0].astype(f32), 0.0)
            erase = jnp.where(z >= hop, maps[zz, 1].astype(f32), 0.0)
            if late is None:
                late, late_kept = (value, erase), stretch
            else:
                late = compose((value, erase), stretch, late, late_kept)
                late_kept = late_kept * stretch
            if hop <= far[1]:
                zz = source[1](hop)
                new = stretch * early + maps[zz, 0].astype(f32) - dot(maps[zz, 1], early)
                early = jnp.where(z + hop >= hops, new, 0.0)
        if stage == FIRST_BESIDE:
            for one in finished:
                one.wait_send()
        if stage >= FIRST_BESIDE:
            for _ in range(min(len(beside), 1 if stage == FIRST_BESIDE else 2)):
                beside.pop(0)()
    for one in beside:
        one()
    state = late[0] + late_kept * early - dot(late[1], early)

    state = state.astype(bf16)

    fold_row = fold_of.astype(jnp.int32)

    def products(rows_of, cc):
        rows = dot(owned_buf[cc], rows_of)
        wide = [jnp.where(fold_row == fold, rows, 0.0).astype(bf16) for fold in range(FOLD)]
        return dot(jnp.concatenate(wide, axis=1), out_weights[...], NT).reshape(chips, folded, -1)

    gated = []
    for i, dy in enumerate(order):
        rows = pl.ds(pl.multiple_of((y + dy) % seqs * share, PAD), share)
        out = locals_buf[rows, :] + dot(reads_buf[rows, :], state)
        out = out * lax.rsqrt(jnp.mean(out * out, axis=-1, keepdims=True) + out_epsilon)
        gated.append((out * gate_buf[rows, :]).astype(bf16))
        swap_out[i] = products(gated[i], 1 - core).astype(bf16)
        launch(swap_out.at[i], swap_in.at[i], s_send.at[i], s_recv.at[i], partner)
    for i, dy in enumerate(order):
        mine = products(gated[i], core)
        copy(swap_in.at[i], swap_in.at[i], s_send.at[i], s_recv.at[i], me).wait_recv()
        parts[i] = (mine + swap_in[i].astype(f32)).astype(bf16)
        for dx in (2, 1, 3, 0) if chips == 4 else range(chips):
            if dy or dx:
                launch(
                    parts.at[i, (x + dx) % chips],
                    landed.at[y * chips + x],
                    o_send.at[dy * chips + dx],
                    o_recv.at[(seqs - dy) % seqs * chips + (chips - dx) % chips],
                    at(0, dy, dx),
                )
    landed[y * chips + x] = parts[seqs - 1, x]
    for dy, dx in plane:
        slot = landed.at[(y + dy) % seqs * chips + (x + dx) % chips]
        index = dy * chips + dx
        copy(slot, slot, o_send.at[index], o_recv.at[index], me).wait_recv()
    for seq in range(seqs):
        total = landed[seq * chips].astype(f32)
        for chip in range(1, chips):
            total = total + landed[seq * chips + chip].astype(f32)
        rows = [total[fold * here_rows : (fold + 1) * here_rows] for fold in range(FOLD)]
        out_ref[:, seq, :] = jnp.concatenate(rows, axis=1).astype(bf16)
    for one in pending:
        one.wait_send()

    for needed, one in guarded:
        pl.when(needed)(one.wait_send)

    @pl.when(last)
    def _():
        tail.wait_send()


def body(
    tokens,
    in_gain,
    w_query,
    w_key,
    w_value,
    w_gate,
    w_beta,
    conv_query,
    conv_key,
    conv_value,
    decay_rate,
    out_gain,
    w_out,
):
    here_rows, seqs, width = tokens.shape
    depth = w_query.shape[1]
    group, length = lax.axis_size("tp"), lax.axis_size("sp")
    hops = length // seqs
    chips = group // CORES
    owners = seqs * group
    span = owners * here_rows
    block = w_query.shape[0]
    sizes = (depth, seqs, group, hops, here_rows, width)
    anywhere = pl.BlockSpec(memory_space=pl.ANY)
    dma = pltpu.SemaphoreType.DMA
    vmem = pltpu.VMEM
    far = hops // 2 + 1
    return pl.pallas_call(
        functools.partial(mixer_kernel, sizes),
        out_shape=jax.ShapeDtypeStruct(tokens.shape, bf16),
        in_specs=[anywhere] * 10 + [pl.BlockSpec(memory_space=pltpu.SMEM)] + [anywhere] * 2,
        out_specs=pl.BlockSpec(memory_space=vmem),
        scratch_shapes=[
            vmem(tokens.shape, bf16),
            vmem((1, width), f32),
            vmem((1, block), bf16),
            vmem(conv_query.shape, bf16),
            vmem(conv_query.shape, bf16),
            vmem(conv_query.shape, bf16),
            vmem((1, depth), f32),
            vmem((hops, seqs, block, 2 * depth), bf16),
            vmem((hops, seqs, block, 3 * depth), bf16),
            vmem((hops, seqs, 1, depth), f32),
            vmem((seqs, PAD, width), bf16),
            vmem((PAD, width), bf16),
            vmem((PAD, width), bf16),
            vmem((PAD + span, owners * PAD), bf16),
            vmem((CORES, chips * FOLD * here_rows, span // seqs), bf16),
            vmem((span, depth), bf16),
            vmem((span, depth), f32),
            vmem((span, depth), f32),
            vmem((width, depth), bf16),
            vmem((span, depth), f32),
            vmem((width // FOLD, FOLD * depth), bf16),
            vmem((owners, PAD, width), bf16),
            vmem((PAD + span, 2 * depth), f32),
            vmem((hops, 2, depth, depth), bf16),
            vmem((seqs, chips, FOLD * here_rows, width // FOLD), bf16),
            vmem((seqs, chips, FOLD * here_rows, width // FOLD), bf16),
            vmem((seqs, chips, FOLD * here_rows, width // FOLD), bf16),
            vmem((seqs * chips, FOLD * here_rows, width // FOLD), bf16),
            dma((12,)),
            dma((3, hops)),
            dma((3, hops)),
            dma((hops, seqs)),
            dma((hops, seqs)),
            dma((seqs,)),
            dma((seqs,)),
            dma((seqs,)),
            dma((seqs,)),
            dma((seqs * chips,)),
            dma((seqs * chips,)),
            dma((seqs * chips,)),
            dma((seqs * chips,)),
            dma,
            dma,
            dma((2, far, PIECES)),
            dma((2, far, PIECES)),
            dma((seqs,)),
            dma((seqs,)),
            dma((seqs * chips,)),
            dma((seqs * chips,)),
        ],
        compiler_params=pltpu.CompilerParams(
            collective_id=0, has_side_effects=True, vmem_limit_bytes=56 * 1024 * 1024
        ),
    )(
        tokens,
        in_gain[None],
        w_query,
        w_key,
        w_value,
        w_gate,
        w_beta.T,
        conv_query,
        conv_key,
        conv_value,
        decay_rate,
        out_gain[None],
        w_out.T,
    )


def solution(mesh):
    placed = (
        P(("sp", "tp"), None, None),
        P(),
        P("sp", "tp"),
        P("sp", "tp"),
        P("sp", "tp"),
        P("sp", "tp"),
        P("sp", "tp"),
        P(None, "tp"),
        P(None, "tp"),
        P(None, "tp"),
        P("tp"),
        P(),
        P("tp", "sp"),
    )
    return jax.shard_map(
        body, mesh=mesh, in_specs=placed, out_specs=P(("sp", "tp"), None, None), check_vma=False
    )
```
